32 devices in a mesh: sp: 4 (over x, core), tp: 8 (over z, y).
Axes of the slice: x: 2, y: 2, z: 4, core: 2. Of those that a mesh axis runs over, the one named last changes fastest.
Arguments:
- latent: bfloat16 [512, 4096], P('sp', 'tp'), may hold values from -60 to 60
- context: bfloat16 [64, 4096], P('sp', 'tp'), may hold values from -6 to 6
- conditioning: bfloat16 [4096], P('sp'), may hold values from -6 to 6
- context_prompt_vector: bfloat16 [4096], P('sp'), may hold values from -6 to 6
- shift_matrix: bfloat16 [4096, 4096], P('tp', 'sp'), may hold values from -0.09375 to 0.09375
- scale_matrix: bfloat16 [4096, 4096], P('tp', 'sp'), may hold values from -0.09375 to 0.09375
- residual_gate_matrix: bfloat16 [4096, 4096], P('tp', 'sp'), may hold values from -0.09375 to 0.09375
- query_matrix: bfloat16 [2048, 4096], P('tp'), may hold values from -0.09375 to 0.09375
- key_matrix: bfloat16 [2048, 4096], P('tp'), may hold values from -0.09375 to 0.09375
- value_matrix: bfloat16 [4096, 4096], P('tp'), may hold values from -0.09375 to 0.09375
- gate_matrix: bfloat16 [4096, 4096], P('tp'), may hold values from -0.09375 to 0.09375
- decay_down_factor: bfloat16 [2, 4096, 16], replicated, may hold values from -0.09375 to 0.09375
- decay_up_factor: bfloat16 [2, 16, 2048], replicated, may hold values from -1.5 to 1.5
- decay_key_bias: float32 [2, 2048], replicated, may hold values from -0.5 to 7
- spike_log_decay: float32 [2, 512, 16], P(None, 'sp'), may hold values from -2.8 to 0
- output_gain: float32 [4096], P('tp'), may hold values from 0.1 to 1.9
- output_matrix: bfloat16 [4096, 4096], P('tp'), may hold values from -0.375 to 0.375
Outputs:
- mixed: bfloat16 [512, 4096], P('sp', 'tp')
The draws below stay inside these ranges and needn't reach their ends.
All inputs are finite; a program needn't handle non-finite values.
Results may differ from the reference program's by a relative error of at most 0.013.
Values may be sent and summed in bfloat16 or wider, within the bound.
No kernel may reach another device: no remote copies, remote signals or barrier semaphores. Data moves between devices by JAX's collectives and lax.ppermute only.
A program may use at most 64 MiB of HBM per device.

```python
import math
import jax
import jax.numpy as jnp
from jax import lax

D = 4096
HEADS = 16
DK = 128
DV = 256
DECAY_RANK = 16
BLK = 64
VGROUP = 64
SEQ = 512
CTX = 64


def draw_latent(key, part):
    key_one, key_two = jax.random.split(key, 2)
    normal_part = jnp.clip(jax.random.normal(key_one, (SEQ, D), jnp.float32), -5.0, 5.0)
    column_rise = jnp.exp(jnp.linspace(math.log(0.6), math.log(2.0), D))
    jitter = jax.random.uniform(key_two, (1, D), jnp.float32, 0.7, 1.4)
    return (normal_part * column_rise * jitter).astype(jnp.bfloat16)


def draw_decay_key_bias(key, part):
    key_one, key_two, key_three = jax.random.split(key, 3)
    fast_share = 0.5
    fast_heads = jax.random.bernoulli(key_one, fast_share, (2, HEADS, 1))
    fast_rates = jax.random.uniform(key_two, (2, HEADS, DK), jnp.float32, -0.5, 1.5)
    slow_rates = jax.random.uniform(key_three, (2, HEADS, DK), jnp.float32, 5.0, 7.0)
    return jnp.where(fast_heads, fast_rates, slow_rates).reshape(2, HEADS * DK)


def draw_spike_log_decay(key, part):
    key_one, key_two = jax.random.split(key, 2)
    spots = jax.random.randint(key_one, (2, HEADS, 4), 0, SEQ)
    depths = jnp.log(jax.random.uniform(key_two, (2, HEADS, 4), jnp.float32, 0.5, 0.8))
    positions = jnp.arange(SEQ, dtype=jnp.int32)
    hits = (positions[None, None, None, :] == spots[:, :, :, None]).astype(jnp.float32)
    summed = jnp.sum(hits * depths[:, :, :, None], axis=2)
    return jnp.transpose(summed, (0, 2, 1))


def level_of(rng, dims, cuts, least, top_value):
    factor_of, own = 1.0, jax.random.fold_in(rng, 6)
    for position, blocks in cuts:
        heights = jnp.exp(jax.random.uniform(jax.random.fold_in(own, position), (blocks,), jnp.float32, least / len(cuts), top_value / len(cuts)))
        factor_of = factor_of * jnp.repeat(heights, dims[position] // blocks).reshape([-1 if axis == position else 1 for axis in range(len(dims))])
    return factor_of


def centred(own_key, shape, deviation, reach, shards=(), held_as=jnp.bfloat16):
    entries = jax.random.normal(own_key, shape, jnp.float32) * deviation
    if len(shards) > 0:
        entries = level_of(own_key, shape, shards, -0.22, 0.18) * entries
    return jnp.clip(entries, min=-reach, max=reach).astype(held_as)


def setup_inputs(seed: int = 0) -> dict:
    splits = jax.random.split(jax.random.key(seed), 18)
    latent = draw_latent(jax.random.fold_in(splits[17], 71), 0)
    context = centred(splits[1], (CTX, D), 1.0, 6.0, ((0, 4), (1, 8)))
    conditioning = centred(splits[2], (D,), 1.0, 6.0, ((0, 4),))
    context_prompt_vector = centred(splits[3], (D,), 1.0, 6.0, ((0, 4),))
    shift_matrix = centred(splits[4], (D, D), D ** -0.5, 0.09375, ((0, 8), (1, 4)))
    scale_matrix = centred(splits[5], (D, D), D ** -0.5, 0.09375, ((0, 8), (1, 4)))
    residual_gate_matrix = centred(splits[6], (D, D), D ** -0.5, 0.09375, ((0, 8), (1, 4)))
    query_matrix = centred(splits[7], (HEADS * DK, D), D ** -0.5, 0.09375, ((0, 8),))
    key_matrix = centred(splits[8], (HEADS * DK, D), D ** -0.5, 0.09375, ((0, 8),))
    value_matrix = centred(splits[9], (HEADS * DV, D), D ** -0.5, 0.09375, ((0, 8),))
    gate_matrix = centred(splits[10], (HEADS * DV, D), D ** -0.5, 0.09375, ((0, 8),))
    decay_down_factor = centred(splits[11], (2, D, DECAY_RANK), D ** -0.5, 0.09375)
    decay_up_factor = centred(splits[12], (2, DECAY_RANK, HEADS * DK), DECAY_RANK ** -0.5, 1.5)
    decay_key_bias = draw_decay_key_bias(jax.random.fold_in(splits[17], 71), 0)
    spike_log_decay = draw_spike_log_decay(jax.random.fold_in(splits[17], 71), 0)
    output_gain = jnp.clip(1.0 + 0.18 * jax.random.normal(splits[15], (HEADS * DV,), jnp.float32), 0.1, 1.9)
    output_matrix = centred(splits[16], (D, HEADS * DV), (HEADS * DV // 16) ** -0.5, 0.375, ((0, 8),))
    return {"latent": latent, "context": context, "conditioning": conditioning, "context_prompt_vector": context_prompt_vector, "shift_matrix": shift_matrix, "scale_matrix": scale_matrix, "residual_gate_matrix": residual_gate_matrix, "query_matrix": query_matrix, "key_matrix": key_matrix, "value_matrix": value_matrix, "gate_matrix": gate_matrix, "decay_down_factor": decay_down_factor, "decay_up_factor": decay_up_factor, "decay_key_bias": decay_key_bias, "spike_log_decay": spike_log_decay, "output_gain": output_gain, "output_matrix": output_matrix}


epsilon = 1e-05
gate_norm = 16.0
precise = lax.Precision.HIGHEST

def linear(rows, weight):
    return lax.dot_general(rows, weight, (((1,), (1,)), ((), ())), preferred_element_type=jnp.float32)

def modulated(rows, shift_vec, scale_vec):
    rows_f = rows.astype(jnp.float32)
    mean_val = lax.optimization_barrier(jnp.mean(rows_f, axis=-1, keepdims=True))
    variance = lax.optimization_barrier(jnp.mean(rows_f * rows_f, axis=-1, keepdims=True)) - mean_val * mean_val
    return ((rows_f - mean_val) * lax.rsqrt(variance + epsilon) * (1.0 + scale_vec) + shift_vec).astype(jnp.bfloat16)

def reverse_rows(array):
    return jnp.flip(array, axis=0)

def end_state(key_rows, value_rows, log_decay):
    cumulative = jnp.cumsum(log_decay, axis=0)
    totals = cumulative[-1]
    weighted = key_rows * jnp.exp(totals - cumulative)
    return (jnp.exp(totals), jnp.einsum('nhd,nhe->hde', weighted, value_rows, precision=precise))

def blockwise(queries, key_rows, value_rows, log_decay, carried, block_len):
    length, head_count, _ = queries.shape
    value_width = value_rows.shape[-1]
    blocks = length // block_len

    def shaped(array):
        return array.reshape(blocks, block_len, head_count, array.shape[-1])
    triangle = jnp.tril(jnp.ones((block_len, block_len), jnp.float32))

    def advance(state_now, inputs):
        block_q, block_k, block_v, block_a = inputs
        cumulative = jnp.cumsum(block_a, axis=0)
        block_end = cumulative[-1]
        query_dec = block_q * jnp.exp(cumulative)
        scores = jnp.einsum('ihd,jhd->hij', query_dec, block_k * jnp.exp(-cumulative), precision=precise) * triangle
        result = jnp.einsum('hij,jhe->ihe', scores, block_v, precision=precise)
        result = result + jnp.einsum('ihd,hde->ihe', query_dec, state_now, precision=precise)
        state_next = state_now * jnp.exp(block_end)[:, :, None] + jnp.einsum('jhd,jhe->hde', block_k * jnp.exp(block_end - cumulative), block_v, precision=precise)
        return (state_next, result)
    _, outputs = lax.scan(advance, carried, (shaped(queries), shaped(key_rows), shaped(value_rows), shaped(log_decay)))
    return outputs.reshape(length, head_count, value_width)

def reference(latent, context, conditioning, context_prompt_vector, shift_matrix, scale_matrix, residual_gate_matrix, query_matrix, key_matrix, value_matrix, gate_matrix, decay_down_factor, decay_up_factor, decay_key_bias, spike_log_decay, output_gain, output_matrix):
    conds = jax.nn.silu(jnp.stack([conditioning, context_prompt_vector]).astype(jnp.float32)).astype(jnp.bfloat16)
    shifts = linear(conds, shift_matrix)
    scales = linear(conds, scale_matrix)
    gates = linear(conds, residual_gate_matrix)
    latent_normalized = modulated(latent, shifts[0], scales[0])
    normed_ctx = modulated(context, shifts[1], scales[1])

    def project(rows, weight):
        stored = lax.optimization_barrier(linear(rows, weight).astype(jnp.bfloat16))
        return stored.astype(jnp.float32)

    def split_heads(rows, width):
        return rows.reshape(rows.shape[0], HEADS, width)
    queries = split_heads(project(latent_normalized, query_matrix), DK) * DK ** (-0.5)
    key_rows = split_heads(project(latent_normalized, key_matrix), DK)
    value_rows = split_heads(project(latent_normalized, value_matrix), DV)
    gate_rows = project(latent_normalized, gate_matrix)
    ctx_keys = split_heads(project(normed_ctx, key_matrix), DK)
    ctx_values = split_heads(project(normed_ctx, value_matrix), DV)

    def per_head_decay(rows, direction):
        low_rows = jnp.dot(rows, decay_down_factor[direction], preferred_element_type=jnp.float32)
        pre_act = jnp.dot(low_rows, decay_up_factor[direction].astype(jnp.float32), precision=precise) + decay_key_bias[direction]
        return split_heads(jax.nn.log_sigmoid(pre_act) / gate_norm, DK)
    latent_forward = per_head_decay(latent_normalized, 0) + spike_log_decay[0][:, :, None]
    latent_backward = per_head_decay(latent_normalized, 1) + spike_log_decay[1][:, :, None]
    ctx_fwd = per_head_decay(normed_ctx, 0)
    ctx_bwd = per_head_decay(normed_ctx, 1)
    start_fwd = end_state(ctx_keys, ctx_values, ctx_fwd)[1]
    start_bwd = end_state(reverse_rows(ctx_keys), reverse_rows(ctx_values), reverse_rows(ctx_bwd))[1]
    out_fwd = blockwise(queries, key_rows, value_rows, latent_forward, start_fwd, BLK)
    out_bwd = reverse_rows(blockwise(reverse_rows(queries), reverse_rows(key_rows), reverse_rows(value_rows), reverse_rows(latent_backward), start_bwd, BLK))
    grouped = (out_fwd + out_bwd).reshape(SEQ, HEADS * DV // VGROUP, VGROUP)
    grouped = grouped * lax.rsqrt(lax.optimization_barrier(jnp.mean(grouped * grouped, axis=-1, keepdims=True)) + epsilon)
    heads_out = (grouped.reshape(SEQ, HEADS * DV) * output_gain * jax.nn.silu(gate_rows)).astype(jnp.bfloat16)
    branch = linear(heads_out, output_matrix)
    return (latent.astype(jnp.float32) + gates[0] * branch).astype(jnp.bfloat16)
```

```python
import functools

import jax
import jax.numpy as jnp
from jax import lax
from jax.experimental import pallas as pl
from jax.experimental.pallas import tpu as pltpu
from jax.sharding import PartitionSpec as P


D = 4096
HEADS = 16
DK = 128
DECAY_RANK = 16
BLK = 64
VGROUP = 64


epsilon = 1e-05
gate_norm = 16.0
precise = lax.Precision.HIGHEST


def for_sending(value):

    def short(part):
        return part.astype(jnp.bfloat16) if part.dtype == jnp.float32 else part

    return jax.tree.map(short, value)


def from_partner(value, axis, distance):
    return lax.ppermute(value, axis, [(i, i ^ 1 << distance) for i in range(lax.axis_size(axis))])


def carried_in(value, axis, combine, identity, reverse):
    peers, index = (lax.axis_size(axis), lax.axis_index(axis))
    everything = jax.tree.map(
        lambda part, kind: lax.all_gather(part.astype(kind), axis),
        value,
        (jnp.bfloat16, jnp.bfloat16),
    )
    start = jax.tree.map(
        lambda part, zero: jnp.broadcast_to(jnp.asarray(zero, part.dtype), part.shape),
        value,
        identity,
    )

    def turn(k, before):
        at = peers - 1 - k if reverse else k
        reached = at > index if reverse else at < index
        new = combine(
            before, jax.tree.map(lambda part, own: part[at].astype(own.dtype), everything, value)
        )
        return jax.tree.map(lambda a, b: jnp.where(reached, a, b), new, before)

    return lax.fori_loop(0, peers, turn, start)


def linear(rows, weight):
    return lax.dot_general(
        rows, weight, (((1,), (1,)), ((), ())), preferred_element_type=jnp.float32
    )


def modulated(rows, row_sum, row_squares, shift_vec, scale_vec):
    rows_f = rows.astype(jnp.float32)
    mean_val = row_sum / D
    variance = row_squares / D - mean_val * mean_val
    return (
        (rows_f - mean_val) * lax.rsqrt(variance + epsilon) * (1.0 + scale_vec) + shift_vec
    ).astype(jnp.bfloat16)


def reverse_rows(array):
    return jnp.flip(array, axis=0)


def end_state(key_rows, value_rows, log_decay):
    cumulative = jnp.cumsum(log_decay, axis=0)
    totals = cumulative[-1]
    weighted = key_rows * jnp.exp(totals - cumulative)
    return (jnp.exp(totals), jnp.einsum("nhd,nhe->hde", weighted, value_rows, precision=precise))


def combine(earlier, later):
    return (earlier[0] * later[0], later[0][..., None] * earlier[1] + later[1])


def blockwise(queries, key_rows, value_rows, log_decay, carried, block_len):
    length, head_count, _ = queries.shape
    value_width = value_rows.shape[-1]
    blocks = length // block_len

    def shaped(array):
        return array.reshape(blocks, block_len, head_count, array.shape[-1])

    triangle = jnp.tril(jnp.ones((block_len, block_len), jnp.float32))

    def advance(state_now, inputs):
        block_q, block_k, block_v, block_a = inputs
        cumulative = jnp.cumsum(block_a, axis=0)
        block_end = cumulative[-1]
        query_dec = block_q * jnp.exp(cumulative)
        scores = (
            jnp.einsum("ihd,jhd->hij", query_dec, block_k * jnp.exp(-cumulative), precision=precise)
            * triangle
        )
        result = jnp.einsum("hij,jhe->ihe", scores, block_v, precision=precise)
        result = result + jnp.einsum("ihd,hde->ihe", query_dec, state_now, precision=precise)
        state_next = state_now * jnp.exp(block_end)[:, :, None] + jnp.einsum(
            "jhd,jhe->hde", block_k * jnp.exp(block_end - cumulative), block_v, precision=precise
        )
        return (state_next, result)

    _, outputs = lax.scan(
        advance, carried, (shaped(queries), shaped(key_rows), shaped(value_rows), shaped(log_decay))
    )
    return outputs.reshape(length, head_count, value_width)


def head_channels(pieces, per_head, tp_index):
    for bit_number in range(per_head.bit_length() - 1):
        partner = from_partner(
            (for_sending(pieces[0]), for_sending(pieces[1]), for_sending(pieces[2])),
            "tp",
            bit_number,
        )
        upper = tp_index // (1 << bit_number) % 2 == 1
        pieces = tuple(
            (
                jnp.where(
                    upper,
                    jnp.concatenate([theirs, mine], axis=1),
                    jnp.concatenate([mine, theirs], axis=1),
                )
                for mine, theirs in zip(pieces, partner)
            )
        )
    return pieces


def context_totals(fwd_growth, fwd_state, bwd_growth, bwd_state, identity):

    def absorb(carried, piece):
        return (combine(carried, piece), None)

    total_fwd, _ = lax.scan(absorb, identity, (fwd_growth, fwd_state))
    total_bwd, _ = lax.scan(absorb, identity, (bwd_growth, bwd_state), reverse=True)
    return (total_fwd, total_bwd)


def stored(array):
    return lax.optimization_barrier(array.astype(jnp.bfloat16))


def local_general(
    latent,
    context,
    conditioning,
    context_prompt_vector,
    shift_matrix,
    scale_matrix,
    residual_gate_matrix,
    query_matrix,
    key_matrix,
    value_matrix,
    gate_matrix,
    decay_down_factor,
    decay_up_factor,
    decay_key_bias,
    spike_log_decay,
    output_gain,
    output_matrix,
):
    tp_count = lax.axis_size("tp")
    tp_index = lax.axis_index("tp")
    per_head = max(tp_count // HEADS, 1)
    heads_per_shard = max(HEADS // tp_count, 1)
    leading_head = tp_index // per_head * heads_per_shard
    tok_rows = latent.shape[0]
    conds = jax.nn.silu(
        jnp.stack([conditioning, context_prompt_vector]).astype(jnp.float32)
    ).astype(jnp.bfloat16)
    shifts, scales, gates = lax.psum(
        (
            linear(conds, shift_matrix),
            linear(conds, scale_matrix),
            linear(conds, residual_gate_matrix),
        ),
        "sp",
    )
    down_both = jnp.concatenate([decay_down_factor[0].T, decay_down_factor[1].T], axis=0)
    lat_weights = (query_matrix, key_matrix, value_matrix, gate_matrix, down_both)
    ctx_weights = (key_matrix, value_matrix, down_both)
    lat_f = latent.astype(jnp.float32)
    ctx_f = context.astype(jnp.float32)
    lat_sum, lat_squares, ctx_sum, ctx_squares = lax.psum(
        (
            jnp.sum(lat_f, axis=1, keepdims=True),
            jnp.sum(lat_f * lat_f, axis=1, keepdims=True),
            jnp.sum(ctx_f, axis=1, keepdims=True),
            jnp.sum(ctx_f * ctx_f, axis=1, keepdims=True),
        ),
        "tp",
    )
    latent_normalized = modulated(latent, lat_sum, lat_squares, shifts[0], scales[0])
    normed_ctx = modulated(context, ctx_sum, ctx_squares, shifts[1], scales[1])
    lat_piece = lax.all_gather(latent_normalized, "tp", axis=1, tiled=True)
    ctx_piece = lax.all_gather(normed_ctx, "tp", axis=1, tiled=True)
    lat_new = tuple((linear(lat_piece, weight) for weight in lat_weights))
    ctx_new = tuple((linear(ctx_piece, weight) for weight in ctx_weights))
    query_part, key_part, value_part, gate_part, low_rank_part = lat_new
    ctx_key_part, ctx_value_part, ctx_low = ctx_new
    query_full, key_full, ctx_key_full = head_channels(
        (stored(query_part), stored(key_part), stored(ctx_key_part)), per_head, tp_index
    )

    def split_heads(rows, width):
        return rows.astype(jnp.float32).reshape(rows.shape[0], heads_per_shard, width)

    value_cols = value_part.shape[1] // heads_per_shard
    queries = split_heads(query_full, DK) * DK ** (-0.5)
    key_rows = split_heads(key_full, DK)
    ctx_keys = split_heads(ctx_key_full, DK)
    values_lat = split_heads(stored(value_part), value_cols)
    values_ctx = split_heads(stored(ctx_value_part), value_cols)
    gate_rows = stored(gate_part).astype(jnp.float32)

    def per_head_decay(low_rows, direction):
        up_part = lax.dynamic_slice_in_dim(
            decay_up_factor[direction], leading_head * DK, heads_per_shard * DK, 1
        ).astype(jnp.float32)
        bias_part = lax.dynamic_slice_in_dim(
            decay_key_bias[direction], leading_head * DK, heads_per_shard * DK, 0
        )
        pre_act = jnp.dot(low_rows, up_part, precision=precise) + bias_part
        return (jax.nn.log_sigmoid(pre_act) / gate_norm).reshape(
            low_rows.shape[0], heads_per_shard, DK
        )

    decay_spikes = lax.dynamic_slice_in_dim(spike_log_decay, leading_head, heads_per_shard, 2)
    latent_forward = per_head_decay(low_rank_part[:, :DECAY_RANK], 0) + decay_spikes[0][:, :, None]
    latent_backward = per_head_decay(low_rank_part[:, DECAY_RANK:], 1) + decay_spikes[1][:, :, None]
    ctx_fwd = per_head_decay(ctx_low[:, :DECAY_RANK], 0)
    ctx_bwd = per_head_decay(ctx_low[:, DECAY_RANK:], 1)
    cf_growth, cf_state = end_state(ctx_keys, values_ctx, ctx_fwd)
    cb_growth, cb_state = end_state(
        reverse_rows(ctx_keys), reverse_rows(values_ctx), reverse_rows(ctx_bwd)
    )
    lf_growth, lf_state = end_state(key_rows, values_lat, latent_forward)
    lb_growth, lb_state = end_state(
        reverse_rows(key_rows), reverse_rows(values_lat), reverse_rows(latent_backward)
    )
    identity = (
        jnp.ones((heads_per_shard, DK), jnp.float32),
        jnp.zeros((heads_per_shard, DK, value_cols), jnp.float32),
    )
    ctx_gathered = (
        lax.all_gather(cf_growth[None].astype(jnp.bfloat16), "sp", axis=0, tiled=True).astype(
            jnp.float32
        ),
        lax.all_gather(cf_state[None].astype(jnp.bfloat16), "sp", axis=0, tiled=True).astype(
            jnp.float32
        ),
        lax.all_gather(cb_growth[None].astype(jnp.bfloat16), "sp", axis=0, tiled=True).astype(
            jnp.float32
        ),
        lax.all_gather(cb_state[None].astype(jnp.bfloat16), "sp", axis=0, tiled=True).astype(
            jnp.float32
        ),
    )
    total_fwd, total_bwd = context_totals(
        ctx_gathered[0], ctx_gathered[1], ctx_gathered[2], ctx_gathered[3], identity
    )
    prefix = carried_in((lf_growth, lf_state), "sp", combine, identity, False)
    suffix = carried_in((lb_growth, lb_state), "sp", combine, identity, True)
    start_fwd = combine(total_fwd, prefix)[1]
    start_bwd = combine(total_bwd, suffix)[1]
    zero_state = jnp.zeros((heads_per_shard, DK, value_cols), jnp.float32)

    def direction_out(query_rows, key_list, value_list, log_decay, start_state):
        local_part = blockwise(query_rows, key_list, value_list, log_decay, zero_state, BLK)
        reach = query_rows * jnp.exp(jnp.cumsum(log_decay, axis=0))
        return local_part + jnp.einsum("nhd,hde->nhe", reach, start_state, precision=precise)

    out_fwd = direction_out(queries, key_rows, values_lat, latent_forward, start_fwd)
    out_bwd = reverse_rows(
        direction_out(
            reverse_rows(queries),
            reverse_rows(key_rows),
            reverse_rows(values_lat),
            reverse_rows(latent_backward),
            start_bwd,
        )
    )
    grouped = (out_fwd + out_bwd).reshape(tok_rows, -1, VGROUP)
    grouped = grouped * lax.rsqrt(jnp.mean(grouped * grouped, axis=-1, keepdims=True) + epsilon)
    heads_out = (grouped.reshape(tok_rows, -1) * output_gain * jax.nn.silu(gate_rows)).astype(
        jnp.bfloat16
    )
    branch = linear(lax.all_gather(heads_out, "tp", axis=1, tiled=True), output_matrix)
    return (latent.astype(jnp.float32) + gates[0] * branch).astype(jnp.bfloat16)


VMEM_SPEC = pl.BlockSpec(memory_space=pltpu.VMEM)
SMEM_SPEC = pl.BlockSpec(memory_space=pltpu.SMEM)
ANY_SPEC = pl.BlockSpec(memory_space=pl.ANY)
NT = (((1,), (1,)), ((), ()))
NN = (((1,), (0,)), ((), ()))
TN = (((0,), (0,)), ((), ()))
f32 = jnp.float32
bf16 = jnp.bfloat16


def matmul(a, b, dims=NN):
    return lax.dot_general(a, b, dims, preferred_element_type=f32)


def halves(value):
    high = value.astype(bf16)
    return (high, (value - high.astype(f32)).astype(bf16))


def exchange(value, axis, distance):
    return lax.ppermute(value, axis, [(i, i ^ distance) for i in range(lax.axis_size(axis))])


def gathered_pieces(value, axis):
    count = lax.axis_size(axis)
    pieces = {0: value, 1: exchange(value, axis, 1)}
    for k in range(2, count, 2):
        pieces[k] = exchange(value, axis, k)
    for k in range(2, count, 2):
        pieces[k + 1] = exchange(pieces[k], axis, 1)
    return [pieces[k] for k in range(count)]


def call(kernel, out_shapes, in_specs, args, flops, traffic, scratch=()):
    single = not isinstance(out_shapes, (tuple, list))
    return pl.pallas_call(
        kernel,
        out_shape=out_shapes,
        in_specs=in_specs,
        out_specs=VMEM_SPEC if single else [VMEM_SPEC] * len(out_shapes),
        scratch_shapes=list(scratch),
        cost_estimate=pl.CostEstimate(flops=flops, bytes_accessed=traffic, transcendentals=0),
    )(*args)


def modulation_kernel(cond_ref, prompt_ref, shift_ref, scale_ref, gate_ref, out_ref):
    row = lax.broadcasted_iota(jnp.int32, (8, cond_ref.shape[1]), 0)
    both = jnp.where(row % 2 == 0, cond_ref[...].astype(f32), prompt_ref[...].astype(f32))
    conds = (both * jax.nn.sigmoid(both)).astype(bf16)
    row_out = lax.broadcasted_iota(jnp.int32, out_ref.shape, 0)
    shifts = matmul(conds, shift_ref[...], NT)
    scales = matmul(conds, scale_ref[...], NT)
    gates = matmul(conds, gate_ref[...], NT)
    out_ref[...] = jnp.where(row_out < 2, shifts, jnp.where(row_out < 4, scales, gates))


def block_masks(total, tokens, wanted):
    i = lax.broadcasted_iota(jnp.int32, (total, total), 0)
    j = lax.broadcasted_iota(jnp.int32, (total, total), 1)
    last = tokens // BLK
    bi = jnp.minimum(lax.shift_right_logical(i, BLK.bit_length() - 1), last)
    bj = jnp.minimum(lax.shift_right_logical(j, BLK.bit_length() - 1), last)
    return wanted(i, j, bi, bj)


def project_kernel(count, tokens, heads, *refs):
    place = refs[0]
    pieces = refs[1 : 1 + count]
    mods = refs[1 + count : 1 + count + count // 2]
    key_hbm, value_hbm, down, up, bias, spikes = refs[1 + count + count // 2 : 7 + count + count // 2]
    normed, keys, values, cum_f, cum_b, payload, key_w, value_w, sems = refs[7 + count + count // 2 :]
    key_copy = pltpu.make_async_copy(key_hbm, key_w, sems.at[0])
    value_copy = pltpu.make_async_copy(value_hbm, value_w, sems.at[1])
    key_copy.start()
    value_copy.start()
    tp = place[0]
    total, width = pieces[0].shape
    lanes = 128
    sums = jnp.zeros((total, lanes), f32)
    squares = jnp.zeros((total, lanes), f32)
    for piece in pieces:
        for c in range(width // lanes):
            x = piece[:, c * lanes : (c + 1) * lanes].astype(f32)
            sums = sums + x
            squares = squares + x * x
    features = width * count
    mean = jnp.sum(sums, axis=1, keepdims=True) / features
    variance = jnp.sum(squares, axis=1, keepdims=True) / features - mean * mean
    inverse = lax.rsqrt(variance + epsilon)
    for k, piece in enumerate(pieces):
        base = 8 * (k % 2)
        mod = mods[k // 2][base : base + 8, :]
        column = pl.multiple_of(lax.bitwise_xor(tp, k) * width, width)
        x = piece[...].astype(f32)
        scaled = (x - mean) * inverse
        ahead = scaled[:tokens] * (1.0 + mod[2:3]) + mod[0:1]
        context = scaled[tokens:] * (1.0 + mod[3:4]) + mod[1:2]
        normed[:tokens, pl.ds(column, width)] = ahead.astype(bf16)
        normed[tokens:, pl.ds(column, width)] = context.astype(bf16)
    low_high, low_low = halves(matmul(normed[...], down[...], NT))
    pre = matmul(low_high, up[...]) + matmul(low_low, up[...]) + bias[...]
    decay = (jnp.minimum(pre, 0.0) - jnp.log1p(jnp.exp(-jnp.abs(pre)))) * (1.0 / gate_norm)
    marks = [
        decay[:tokens, c * DK : (c + 1) * DK] + spikes[:, c : c + 1] for c in range(2 * heads)
    ]
    decay = jnp.concatenate([jnp.concatenate(marks, axis=1), decay[tokens:]], axis=0)
    ones = jnp.ones((total, total), f32)
    zeros = jnp.zeros((total, total), f32)
    lower = block_masks(
        total, tokens, lambda i, j, bi, bj: jnp.where((bi == bj) & (i >= j), ones, zeros)
    ).astype(bf16)
    upper = block_masks(
        total, tokens, lambda i, j, bi, bj: jnp.where((bi == bj) & (i <= j), ones, zeros)
    ).astype(bf16)
    half = heads * DK
    high, low = halves(decay)
    cf = matmul(lower, high[:, :half]) + matmul(lower, low[:, :half])
    cb = matmul(upper, high[:, half:]) + matmul(upper, low[:, half:])
    cum_f[...] = cf[:tokens]
    cum_b[...] = cb[:tokens]
    key_copy.wait()
    key_all = matmul(normed[...], key_w[...], NT).astype(bf16)
    keys[...] = key_all[:tokens]
    value_copy.wait()
    value_all = matmul(normed[...], value_w[...], NT).astype(bf16)
    values[...] = value_all[:tokens]
    wide = value_all.shape[1] // heads
    blocks = tokens // BLK
    size = heads * wide
    growth = [[], [], [], []]
    ctx = total - tokens
    start = 2 * size + growth_rows(heads)
    for h in range(heads):
        own = slice(h * DK, (h + 1) * DK)
        kh = key_all[:, own].astype(f32)
        vh = value_all[:tokens, h * wide : (h + 1) * wide]
        cfh, cbh = (cf[:, own], cb[:, own])
        ends_f = [cfh[(b + 1) * BLK - 1 : (b + 1) * BLK] for b in range(blocks)]
        ends_b = [cbh[b * BLK : b * BLK + 1] for b in range(blocks)]
        weighted_f, weighted_b = ([], [])
        for b in range(blocks):
            rows = slice(b * BLK, (b + 1) * BLK)
            weighted_f.append(kh[rows] * jnp.exp(sum(ends_f[b + 1 :], ends_f[b]) - cfh[rows]))
            weighted_b.append(kh[rows] * jnp.exp(sum(ends_b[:b], ends_b[b]) - cbh[rows]))
        kf = jnp.concatenate(weighted_f, axis=0).astype(bf16)
        kb = jnp.concatenate(weighted_b, axis=0).astype(bf16)
        payload[h * wide : (h + 1) * wide, :] = matmul(vh, kf, TN).astype(bf16)
        payload[size + h * wide : size + (h + 1) * wide, :] = matmul(vh, kb, TN).astype(bf16)
        growth[0].append(jnp.exp(sum(ends_f[1:], ends_f[0])))
        growth[1].append(jnp.exp(sum(ends_b[1:], ends_b[0])))
        end_f, end_b = (cfh[total - 1 : total], cbh[tokens : tokens + 1])
        growth[2].append(jnp.exp(end_f))
        growth[3].append(jnp.exp(end_b))
        at = start + h * ctx
        payload[at : at + ctx, :] = (kh[tokens:] * jnp.exp(end_f - cfh[tokens:])).astype(bf16)
        at = at + heads * ctx
        payload[at : at + ctx, :] = (kh[tokens:] * jnp.exp(end_b - cbh[tokens:])).astype(bf16)
    for c in range(size // DK):
        at = start + (2 * heads + c) * ctx
        payload[at : at + ctx, :] = value_all[tokens:, c * DK : (c + 1) * DK]
    payload[2 * size : start, :] = growth_block(growth, heads)


def growth_rows(heads):
    return -(-4 * heads // 16) * 16


def growth_block(growth, heads):
    rows = [row for kind in growth for row in kind]
    blank = jnp.zeros((growth_rows(heads) - len(rows), DK), f32)
    return jnp.concatenate([*rows, blank], axis=0).astype(bf16)


def growth_of(ref, at, kind, h, heads):
    block = ref[at : at + growth_rows(heads), :].astype(f32)
    return block[kind * heads + h : kind * heads + h + 1]


def within_kernel(
    heads,
    normed,
    query_hbm,
    gate_hbm,
    keys,
    values,
    cum_f,
    cum_b,
    gain,
    inside,
    reach_f,
    reach_b,
    gated,
    query_w,
    gate_w,
    sems,
):
    query_copy = pltpu.make_async_copy(query_hbm, query_w, sems.at[0])
    gate_copy = pltpu.make_async_copy(gate_hbm, gate_w, sems.at[1])
    query_copy.start()
    gate_copy.start()
    tokens = keys.shape[0]
    rows_in = normed[:tokens, :]
    query_copy.wait()
    query_all = matmul(rows_in, query_w[...], NT).astype(bf16).astype(f32) * DK ** (-0.5)
    wide = values.shape[1] // heads
    blocks = tokens // BLK

    def choose(i, j, bi, bj):
        same = bi == bj
        return (same & (i >= j), same & (i <= j), bi > bj, bi < bj)

    forward, backward, later, sooner = block_masks(tokens, tokens, choose)
    for h in range(heads):
        own = slice(h * DK, (h + 1) * DK)
        qh = query_all[:, own]
        kh = keys[:, own].astype(f32)
        cf, cb = (cum_f[:, own], cum_b[:, own])
        ends_f = [cf[(b + 1) * BLK - 1 : (b + 1) * BLK] for b in range(blocks)]
        ends_b = [cb[b * BLK : b * BLK + 1] for b in range(blocks)]
        spread = (BLK, DK)
        end_f = jnp.concatenate([jnp.broadcast_to(e, spread) for e in ends_f], axis=0)
        end_b = jnp.concatenate([jnp.broadcast_to(e, spread) for e in ends_b], axis=0)
        qf, qb = (qh * jnp.exp(cf), qh * jnp.exp(cb))
        qf_b, qb_b = (qf.astype(bf16), qb.astype(bf16))
        scores = (
            jnp.where(forward, matmul(qf_b, (kh * jnp.exp(-cf)).astype(bf16), NT), 0.0)
            + jnp.where(backward, matmul(qb_b, (kh * jnp.exp(-cb)).astype(bf16), NT), 0.0)
            + jnp.where(later, matmul(qf_b, (kh * jnp.exp(end_f - cf)).astype(bf16), NT), 0.0)
            + jnp.where(sooner, matmul(qb_b, (kh * jnp.exp(end_b - cb)).astype(bf16), NT), 0.0)
        )
        vh = values[:, h * wide : (h + 1) * wide]
        inside[:, h * wide : (h + 1) * wide] = matmul(scores.astype(bf16), vh)
        for b in range(blocks):
            rows = slice(b * BLK, (b + 1) * BLK)
            before = sum(ends_f[:b], jnp.zeros_like(ends_f[0]))
            after = sum(ends_b[b + 1 :], jnp.zeros_like(ends_b[0]))
            reach_f[rows, own] = (qf[rows] * jnp.exp(before)).astype(bf16)
            reach_b[rows, own] = (qb[rows] * jnp.exp(after)).astype(bf16)
    gate_copy.wait()
    gates = matmul(rows_in, gate_w[...], NT).astype(bf16).astype(f32)
    gated[...] = gains_of(gates, gain[...])


def gains_of(gates, gain):
    return gates * jax.nn.sigmoid(gates) * gain


def merge_kernel(bit, final, heads, ctx, place, own, partner, out):
    size = (own.shape[0] - growth_rows(heads) - 4 * heads * ctx) // 2
    lift = growth_rows(heads)
    states = 1 if final else 2
    sp = place[1]
    side = lax.bitwise_and(lax.shift_right_logical(sp, bit), 1)
    onward = lax.bitwise_and(lax.shift_right_logical(sp, bit + 1), 1)

    def emit(low, up):
        wide = size // heads

        def forward(at):
            for h in range(heads):
                rows = slice(h * wide, (h + 1) * wide)
                decayed = growth_of(up, 2 * size, 0, h, heads) * low[rows, :].astype(f32)
                out[at + h * wide : at + (h + 1) * wide, :] = (
                    decayed + up[rows, :].astype(f32)
                ).astype(bf16)

        def backward(at):
            for h in range(heads):
                rows = slice(size + h * wide, size + (h + 1) * wide)
                decayed = growth_of(low, 2 * size, 1, h, heads) * up[rows, :].astype(f32)
                out[at + h * wide : at + (h + 1) * wide, :] = (
                    decayed + low[rows, :].astype(f32)
                ).astype(bf16)

        if final:
            pl.when(onward == 0)(lambda: forward(0))
            pl.when(onward == 1)(lambda: backward(0))
        else:
            forward(0)
            backward(size)
        out[states * size : states * size + lift, :] = (
            low[2 * size : 2 * size + lift, :].astype(f32)
            * up[2 * size : 2 * size + lift, :].astype(f32)
        ).astype(bf16)
        base_in, base_out = (2 * size + lift, states * size + lift)
        for section in range(4 * heads):
            before = low[base_in + section * ctx : base_in + (section + 1) * ctx, :]
            after = up[base_in + section * ctx : base_in + (section + 1) * ctx, :]
            if section < heads:
                before = before.astype(f32) * growth_of(up, 2 * size, 2, section, heads)
            elif section < 2 * heads:
                after = after.astype(f32) * growth_of(low, 2 * size, 3, section - heads, heads)
            at = base_out + 2 * section * ctx
            out[at : at + ctx, :] = before.astype(bf16)
            out[at + ctx : at + 2 * ctx, :] = after.astype(bf16)

    pl.when(side == 0)(lambda: emit(own, partner))
    pl.when(side == 1)(lambda: emit(partner, own))


def finish_kernel(steps, heads, ctx, *refs):
    place, own = refs[:2]
    partners = refs[2 : 2 + steps]
    inside, reach_f, reach_b, gated, out, start_f, start_b, grow_f, grow_b = refs[2 + steps :]
    sp = place[1]
    size = start_f.shape[0]
    wide = size // heads
    start_f[...] = jnp.zeros(start_f.shape, f32)
    start_b[...] = jnp.zeros(start_b.shape, f32)
    grow_f[...] = jnp.ones(grow_f.shape, f32)
    grow_b[...] = jnp.ones(grow_b.shape, f32)

    def take(start, grow, partner, at, kind, states):
        for h in range(heads):
            rows = slice(h * wide, (h + 1) * wide)
            one = slice(h, h + 1)
            theirs = partner[at + h * wide : at + (h + 1) * wide, :].astype(f32)
            start[rows, :] = start[rows, :] + grow[one, :] * theirs
            grow[one, :] = grow[one, :] * growth_of(partner, states * size, kind, h, heads)

    for step in range(steps):
        side = lax.bitwise_and(lax.shift_right_logical(sp, step), 1)
        states = 1 if step == steps - 1 and steps > 1 else 2
        partner = partners[step]
        back = size if states == 2 else 0
        pl.when(side == 1)(functools.partial(take, start_f, grow_f, partner, 0, 0, states))
        pl.when(side == 0)(functools.partial(take, start_b, grow_b, partner, back, 1, states))

    states = 1 if steps > 1 else 2
    lift = growth_rows(heads)
    base = states * size + lift
    rows_each = ctx << (steps - 1)

    def context(low, up):
        def part(ref, section):
            return ref[base + section * rows_each : base + (section + 1) * rows_each, :]

        for h in range(heads):
            rows = slice(h * wide, (h + 1) * wide)
            one = slice(h, h + 1)
            grow_up = growth_of(up, states * size, 2, h, heads)
            grow_low = growth_of(low, states * size, 3, h, heads)
            kf = [(part(low, h).astype(f32) * grow_up).astype(bf16), part(up, h)]
            kb = [part(low, heads + h), (part(up, heads + h).astype(f32) * grow_low).astype(bf16)]
            first = 2 * heads + h * (wide // DK)
            for c in range(wide // DK):
                vs = jnp.concatenate([part(low, first + c), part(up, first + c)], axis=0)
                at = slice(h * wide + c * DK, h * wide + (c + 1) * DK)
                start_f[at, :] += grow_f[one, :] * matmul(vs, jnp.concatenate(kf, axis=0), TN)
                start_b[at, :] += grow_b[one, :] * matmul(vs, jnp.concatenate(kb, axis=0), TN)

    side = lax.bitwise_and(lax.shift_right_logical(sp, steps - 1), 1)
    pl.when(side == 0)(lambda: context(own, partners[-1]))
    pl.when(side == 1)(lambda: context(partners[-1], own))
    i = lax.broadcasted_iota(jnp.int32, (DK, DK), 0)
    j = lax.broadcasted_iota(jnp.int32, (DK, DK), 1)
    shift = VGROUP.bit_length() - 1
    alike = lax.shift_right_logical(i, shift) == lax.shift_right_logical(j, shift)
    averaging = jnp.where(alike, 1.0 / VGROUP, 0.0).astype(bf16)
    for h in range(heads):
        own_rows = slice(h * wide, (h + 1) * wide)
        lanes = slice(h * DK, (h + 1) * DK)
        result = (
            inside[:, own_rows]
            + matmul(reach_f[:, lanes], start_f[own_rows, :].astype(bf16), NT)
            + matmul(reach_b[:, lanes], start_b[own_rows, :].astype(bf16), NT)
        )
        for c in range(wide // DK):
            x = result[:, c * DK : (c + 1) * DK]
            high, low = halves(x * x)
            power = matmul(high, averaging) + matmul(low, averaging)
            at = slice(h * wide + c * DK, h * wide + (c + 1) * DK)
            out[:, at] = (x * lax.rsqrt(power + epsilon) * gated[:, at]).astype(bf16)


def output_kernel(count, *refs):
    place = refs[0]
    pieces = refs[1 : 1 + count]
    weight, latent, mod, out = refs[1 + count :]
    tp = place[0]
    width = pieces[0].shape[1]
    branch = jnp.zeros(out.shape, f32)
    for k, piece in enumerate(pieces):
        column = pl.multiple_of(lax.bitwise_xor(tp, k) * width, width)
        branch = branch + matmul(piece[...], weight[:, pl.ds(column, width)], NT)
    out[...] = (latent[...].astype(f32) + mod[4:5, :] * branch).astype(bf16)


def local_direct(
    latent,
    context,
    conditioning,
    context_prompt_vector,
    shift_matrix,
    scale_matrix,
    residual_gate_matrix,
    query_matrix,
    key_matrix,
    value_matrix,
    gate_matrix,
    decay_down_factor,
    decay_up_factor,
    decay_key_bias,
    spike_log_decay,
    output_gain,
    output_matrix,
):
    tp_count, sp_count = (lax.axis_size("tp"), lax.axis_size("sp"))
    tp_index, sp_index = (lax.axis_index("tp"), lax.axis_index("sp"))
    heads = HEADS // tp_count
    tokens, width = latent.shape
    ctx = context.shape[0]
    total = tokens + ctx
    features = width * tp_count
    steps = sp_count.bit_length() - 1
    place = jnp.stack([tp_index, sp_index]).astype(jnp.int32)
    shape = jax.ShapeDtypeStruct

    pieces = gathered_pieces(jnp.concatenate([latent, context], axis=0), "tp")
    inner = conditioning.shape[0]
    mod = call(
        modulation_kernel,
        shape((8, width), f32),
        [VMEM_SPEC] * 5,
        (
            conditioning[None],
            context_prompt_vector[None],
            shift_matrix,
            scale_matrix,
            residual_gate_matrix,
        ),
        6 * 8 * width * inner,
        6 * width * inner,
    )
    for bit in range(steps):
        mod = mod + exchange(mod, "sp", 1 << bit)
    mod_pair = jnp.concatenate([mod, exchange(mod, "tp", 1)], axis=0)
    mods = [mod_pair] + [exchange(mod_pair, "tp", k) for k in range(2, tp_count, 2)]

    half = heads * DK
    own_up = lax.dynamic_slice_in_dim(decay_up_factor, tp_index * half, half, 2)
    blank = jnp.zeros((DECAY_RANK, half), bf16)
    up = jnp.concatenate(
        [
            jnp.concatenate([own_up[0], blank], axis=1),
            jnp.concatenate([blank, own_up[1]], axis=1),
        ],
        axis=0,
    )
    bias = lax.dynamic_slice_in_dim(decay_key_bias, tp_index * half, half, 1).reshape(1, 2 * half)
    spikes = lax.dynamic_slice_in_dim(spike_log_decay, tp_index * heads, heads, 2)
    spikes = jnp.transpose(spikes, (1, 0, 2)).reshape(tokens, 2 * heads)
    down = jnp.transpose(decay_down_factor, (0, 2, 1)).reshape(2 * DECAY_RANK, features)

    vdim = value_matrix.shape[0]
    lift = growth_rows(heads)
    normed, keys, values, cum_f, cum_b, payload = call(
        functools.partial(project_kernel, tp_count, tokens, heads),
        [
            shape((total, features), bf16),
            shape((tokens, half), bf16),
            shape((tokens, vdim), bf16),
            shape((tokens, half), f32),
            shape((tokens, half), f32),
            shape((2 * vdim + lift + 4 * heads * ctx, DK), bf16),
        ],
        [SMEM_SPEC] + [VMEM_SPEC] * (tp_count + tp_count // 2) + [ANY_SPEC] * 2 + [VMEM_SPEC] * 4,
        (place, *pieces, *mods, key_matrix, value_matrix, down, up, bias, spikes),
        2 * total * features * (half + vdim),
        2 * features * (half + vdim),
        [
            pltpu.VMEM(key_matrix.shape, bf16),
            pltpu.VMEM(value_matrix.shape, bf16),
            pltpu.SemaphoreType.DMA((2,)),
        ],
    )
    partners = [exchange(payload, "sp", 1)]
    rows = ctx
    for bit in range(steps - 1):
        final = bit == steps - 2
        states = 1 if final else 2
        payload = call(
            functools.partial(merge_kernel, bit, final, heads, rows),
            shape((states * vdim + lift + 8 * heads * rows, DK), bf16),
            [SMEM_SPEC, VMEM_SPEC, VMEM_SPEC],
            (place, payload, partners[-1]),
            4 * vdim * DK,
            8 * vdim * DK,
        )
        rows = 2 * rows
        partners.append(exchange(payload, "sp", 2 << bit))
    inside, reach_f, reach_b, gated = call(
        functools.partial(within_kernel, heads),
        [
            shape((tokens, vdim), f32),
            shape((tokens, half), bf16),
            shape((tokens, half), bf16),
            shape((tokens, vdim), f32),
        ],
        [VMEM_SPEC] + [ANY_SPEC] * 2 + [VMEM_SPEC] * 5,
        (
            normed,
            query_matrix,
            gate_matrix,
            keys,
            values,
            cum_f,
            cum_b,
            output_gain[None],
        ),
        2 * tokens * features * (half + vdim),
        2 * features * (half + vdim),
        [
            pltpu.VMEM(query_matrix.shape, bf16),
            pltpu.VMEM(gate_matrix.shape, bf16),
            pltpu.SemaphoreType.DMA((2,)),
        ],
    )
    heads_out = call(
        functools.partial(finish_kernel, steps, heads, ctx),
        shape((tokens, vdim), bf16),
        [SMEM_SPEC] + [VMEM_SPEC] * (5 + steps),
        (place, payload, *partners, inside, reach_f, reach_b, gated),
        8 * tokens * vdim * DK,
        8 * tokens * vdim,
        [
            pltpu.VMEM((vdim, DK), f32),
            pltpu.VMEM((vdim, DK), f32),
            pltpu.VMEM((8 * -(-heads // 8), DK), f32),
            pltpu.VMEM((8 * -(-heads // 8), DK), f32),
        ],
    )
    branches = gathered_pieces(heads_out, "tp")
    return call(
        functools.partial(output_kernel, tp_count),
        shape((tokens, width), bf16),
        [SMEM_SPEC] + [VMEM_SPEC] * (tp_count + 3),
        (place, *branches, output_matrix, latent, mod),
        2 * tokens * width * vdim * tp_count,
        2 * width * vdim * tp_count,
    )


def solution(mesh):
    placed = (
        P("sp", "tp"),
        P("sp", "tp"),
        P("sp"),
        P("sp"),
        P("tp", "sp"),
        P("tp", "sp"),
        P("tp", "sp"),
        P("tp", None),
        P("tp", None),
        P("tp", None),
        P("tp", None),
        P(),
        P(),
        P(),
        P(None, "sp", None),
        P("tp"),
        P("tp", None),
    )
    tp_count, sp_count = (mesh.shape["tp"], mesh.shape["sp"])
    powers = tp_count & tp_count - 1 == 0 and sp_count & sp_count - 1 == 0
    direct = 2 <= tp_count <= HEADS and sp_count >= 2 and powers
    return jax.shard_map(
        local_direct if direct else local_general, mesh=mesh, in_specs=placed, out_specs=P("sp", "tp"), check_vma=False
    )
```

```python
import functools

import jax
import jax.numpy as jnp
from jax import lax
from jax.experimental import pallas as pl
from jax.experimental.pallas import tpu as pltpu
from jax.sharding import PartitionSpec as P


D = 4096
HEADS = 16
DK = 128
DECAY_RANK = 16
BLK = 64
VGROUP = 64


epsilon = 1e-05
gate_norm = 16.0
precise = lax.Precision.HIGHEST


def for_sending(value):

    def short(part):
        return part.astype(jnp.bfloat16) if part.dtype == jnp.float32 else part

    return jax.tree.map(short, value)


def from_partner(value, axis, distance):
    return lax.ppermute(value, axis, [(i, i ^ 1 << distance) for i in range(lax.axis_size(axis))])


def carried_in(value, axis, combine, identity, reverse):
    peers, index = (lax.axis_size(axis), lax.axis_index(axis))
    everything = jax.tree.map(
        lambda part, kind: lax.all_gather(part.astype(kind), axis),
        value,
        (jnp.bfloat16, jnp.bfloat16),
    )
    start = jax.tree.map(
        lambda part, zero: jnp.broadcast_to(jnp.asarray(zero, part.dtype), part.shape),
        value,
        identity,
    )

    def turn(k, before):
        at = peers - 1 - k if reverse else k
        reached = at > index if reverse else at < index
        new = combine(
            before, jax.tree.map(lambda part, own: part[at].astype(own.dtype), everything, value)
        )
        return jax.tree.map(lambda a, b: jnp.where(reached, a, b), new, before)

    return lax.fori_loop(0, peers, turn, start)


def linear(rows, weight):
    return lax.dot_general(
        rows, weight, (((1,), (1,)), ((), ())), preferred_element_type=jnp.float32
    )


def modulated(rows, row_sum, row_squares, shift_vec, scale_vec):
    rows_f = rows.astype(jnp.float32)
    mean_val = row_sum / D
    variance = row_squares / D - mean_val * mean_val
    return (
        (rows_f - mean_val) * lax.rsqrt(variance + epsilon) * (1.0 + scale_vec) + shift_vec
    ).astype(jnp.bfloat16)


def reverse_rows(array):
    return jnp.flip(array, axis=0)


def end_state(key_rows, value_rows, log_decay):
    cumulative = jnp.cumsum(log_decay, axis=0)
    totals = cumulative[-1]
    weighted = key_rows * jnp.exp(totals - cumulative)
    return (jnp.exp(totals), jnp.einsum("nhd,nhe->hde", weighted, value_rows, precision=precise))


def combine(earlier, later):
    return (earlier[0] * later[0], later[0][..., None] * earlier[1] + later[1])


def blockwise(queries, key_rows, value_rows, log_decay, carried, block_len):
    length, head_count, _ = queries.shape
    value_width = value_rows.shape[-1]
    blocks = length // block_len

    def shaped(array):
        return array.reshape(blocks, block_len, head_count, array.shape[-1])

    triangle = jnp.tril(jnp.ones((block_len, block_len), jnp.float32))

    def advance(state_now, inputs):
        block_q, block_k, block_v, block_a = inputs
        cumulative = jnp.cumsum(block_a, axis=0)
        block_end = cumulative[-1]
        query_dec = block_q * jnp.exp(cumulative)
        scores = (
            jnp.einsum("ihd,jhd->hij", query_dec, block_k * jnp.exp(-cumulative), precision=precise)
            * triangle
        )
        result = jnp.einsum("hij,jhe->ihe", scores, block_v, precision=precise)
        result = result + jnp.einsum("ihd,hde->ihe", query_dec, state_now, precision=precise)
        state_next = state_now * jnp.exp(block_end)[:, :, None] + jnp.einsum(
            "jhd,jhe->hde", block_k * jnp.exp(block_end - cumulative), block_v, precision=precise
        )
        return (state_next, result)

    _, outputs = lax.scan(
        advance, carried, (shaped(queries), shaped(key_rows), shaped(value_rows), shaped(log_decay))
    )
    return outputs.reshape(length, head_count, value_width)


def head_channels(pieces, per_head, tp_index):
    for bit_number in range(per_head.bit_length() - 1):
        partner = from_partner(
            (for_sending(pieces[0]), for_sending(pieces[1]), for_sending(pieces[2])),
            "tp",
            bit_number,
        )
        upper = tp_index // (1 << bit_number) % 2 == 1
        pieces = tuple(
            (
                jnp.where(
                    upper,
                    jnp.concatenate([theirs, mine], axis=1),
                    jnp.concatenate([mine, theirs], axis=1),
                )
                for mine, theirs in zip(pieces, partner)
            )
        )
    return pieces


def context_totals(fwd_growth, fwd_state, bwd_growth, bwd_state, identity):

    def absorb(carried, piece):
        return (combine(carried, piece), None)

    total_fwd, _ = lax.scan(absorb, identity, (fwd_growth, fwd_state))
    total_bwd, _ = lax.scan(absorb, identity, (bwd_growth, bwd_state), reverse=True)
    return (total_fwd, total_bwd)


def stored(array):
    return lax.optimization_barrier(array.astype(jnp.bfloat16))


def local_general(
    latent,
    context,
    conditioning,
    context_prompt_vector,
    shift_matrix,
    scale_matrix,
    residual_gate_matrix,
    query_matrix,
    key_matrix,
    value_matrix,
    gate_matrix,
    decay_down_factor,
    decay_up_factor,
    decay_key_bias,
    spike_log_decay,
    output_gain,
    output_matrix,
):
    tp_count = lax.axis_size("tp")
    tp_index = lax.axis_index("tp")
    per_head = max(tp_count // HEADS, 1)
    heads_per_shard = max(HEADS // tp_count, 1)
    leading_head = tp_index // per_head * heads_per_shard
    tok_rows = latent.shape[0]
    conds = jax.nn.silu(
        jnp.stack([conditioning, context_prompt_vector]).astype(jnp.float32)
    ).astype(jnp.bfloat16)
    shifts, scales, gates = lax.psum(
        (
            linear(conds, shift_matrix),
            linear(conds, scale_matrix),
            linear(conds, residual_gate_matrix),
        ),
        "sp",
    )
    down_both = jnp.concatenate([decay_down_factor[0].T, decay_down_factor[1].T], axis=0)
    lat_weights = (query_matrix, key_matrix, value_matrix, gate_matrix, down_both)
    ctx_weights = (key_matrix, value_matrix, down_both)
    lat_f = latent.astype(jnp.float32)
    ctx_f = context.astype(jnp.float32)
    lat_sum, lat_squares, ctx_sum, ctx_squares = lax.psum(
        (
            jnp.sum(lat_f, axis=1, keepdims=True),
            jnp.sum(lat_f * lat_f, axis=1, keepdims=True),
            jnp.sum(ctx_f, axis=1, keepdims=True),
            jnp.sum(ctx_f * ctx_f, axis=1, keepdims=True),
        ),
        "tp",
    )
    latent_normalized = modulated(latent, lat_sum, lat_squares, shifts[0], scales[0])
    normed_ctx = modulated(context, ctx_sum, ctx_squares, shifts[1], scales[1])
    lat_piece = lax.all_gather(latent_normalized, "tp", axis=1, tiled=True)
    ctx_piece = lax.all_gather(normed_ctx, "tp", axis=1, tiled=True)
    lat_new = tuple((linear(lat_piece, weight) for weight in lat_weights))
    ctx_new = tuple((linear(ctx_piece, weight) for weight in ctx_weights))
    query_part, key_part, value_part, gate_part, low_rank_part = lat_new
    ctx_key_part, ctx_value_part, ctx_low = ctx_new
    query_full, key_full, ctx_key_full = head_channels(
        (stored(query_part), stored(key_part), stored(ctx_key_part)), per_head, tp_index
    )

    def split_heads(rows, width):
        return rows.astype(jnp.float32).reshape(rows.shape[0], heads_per_shard, width)

    value_cols = value_part.shape[1] // heads_per_shard
    queries = split_heads(query_full, DK) * DK ** (-0.5)
    key_rows = split_heads(key_full, DK)
    ctx_keys = split_heads(ctx_key_full, DK)
    values_lat = split_heads(stored(value_part), value_cols)
    values_ctx = split_heads(stored(ctx_value_part), value_cols)
    gate_rows = stored(gate_part).astype(jnp.float32)

    def per_head_decay(low_rows, direction):
        up_part = lax.dynamic_slice_in_dim(
            decay_up_factor[direction], leading_head * DK, heads_per_shard * DK, 1
        ).astype(jnp.float32)
        bias_part = lax.dynamic_slice_in_dim(
            decay_key_bias[direction], leading_head * DK, heads_per_shard * DK, 0
        )
        pre_act = jnp.dot(low_rows, up_part, precision=precise) + bias_part
        return (jax.nn.log_sigmoid(pre_act) / gate_norm).reshape(
            low_rows.shape[0], heads_per_shard, DK
        )

    decay_spikes = lax.dynamic_slice_in_dim(spike_log_decay, leading_head, heads_per_shard, 2)
    latent_forward = per_head_decay(low_rank_part[:, :DECAY_RANK], 0) + decay_spikes[0][:, :, None]
    latent_backward = per_head_decay(low_rank_part[:, DECAY_RANK:], 1) + decay_spikes[1][:, :, None]
    ctx_fwd = per_head_decay(ctx_low[:, :DECAY_RANK], 0)
    ctx_bwd = per_head_decay(ctx_low[:, DECAY_RANK:], 1)
    cf_growth, cf_state = end_state(ctx_keys, values_ctx, ctx_fwd)
    cb_growth, cb_state = end_state(
        reverse_rows(ctx_keys), reverse_rows(values_ctx), reverse_rows(ctx_bwd)
    )
    lf_growth, lf_state = end_state(key_rows, values_lat, latent_forward)
    lb_growth, lb_state = end_state(
        reverse_rows(key_rows), reverse_rows(values_lat), reverse_rows(latent_backward)
    )
    identity = (
        jnp.ones((heads_per_shard, DK), jnp.float32),
        jnp.zeros((heads_per_shard, DK, value_cols), jnp.float32),
    )
    ctx_gathered = (
        lax.all_gather(cf_growth[None].astype(jnp.bfloat16), "sp", axis=0, tiled=True).astype(
            jnp.float32
        ),
        lax.all_gather(cf_state[None].astype(jnp.bfloat16), "sp", axis=0, tiled=True).astype(
            jnp.float32
        ),
        lax.all_gather(cb_growth[None].astype(jnp.bfloat16), "sp", axis=0, tiled=True).astype(
            jnp.float32
        ),
        lax.all_gather(cb_state[None].astype(jnp.bfloat16), "sp", axis=0, tiled=True).astype(
            jnp.float32
        ),
    )
    total_fwd, total_bwd = context_totals(
        ctx_gathered[0], ctx_gathered[1], ctx_gathered[2], ctx_gathered[3], identity
    )
    prefix = carried_in((lf_growth, lf_state), "sp", combine, identity, False)
    suffix = carried_in((lb_growth, lb_state), "sp", combine, identity, True)
    start_fwd = combine(total_fwd, prefix)[1]
    start_bwd = combine(total_bwd, suffix)[1]
    zero_state = jnp.zeros((heads_per_shard, DK, value_cols), jnp.float32)

    def direction_out(query_rows, key_list, value_list, log_decay, start_state):
        local_part = blockwise(query_rows, key_list, value_list, log_decay, zero_state, BLK)
        reach = query_rows * jnp.exp(jnp.cumsum(log_decay, axis=0))
        return local_part + jnp.einsum("nhd,hde->nhe", reach, start_state, precision=precise)

    out_fwd = direction_out(queries, key_rows, values_lat, latent_forward, start_fwd)
    out_bwd = reverse_rows(
        direction_out(
            reverse_rows(queries),
            reverse_rows(key_rows),
            reverse_rows(values_lat),
            reverse_rows(latent_backward),
            start_bwd,
        )
    )
    grouped = (out_fwd + out_bwd).reshape(tok_rows, -1, VGROUP)
    grouped = grouped * lax.rsqrt(jnp.mean(grouped * grouped, axis=-1, keepdims=True) + epsilon)
    heads_out = (grouped.reshape(tok_rows, -1) * output_gain * jax.nn.silu(gate_rows)).astype(
        jnp.bfloat16
    )
    branch = linear(lax.all_gather(heads_out, "tp", axis=1, tiled=True), output_matrix)
    return (latent.astype(jnp.float32) + gates[0] * branch).astype(jnp.bfloat16)


VMEM_SPEC = pl.BlockSpec(memory_space=pltpu.VMEM)
HBM_SPEC = pl.BlockSpec(memory_space=pltpu.HBM)
NT = (((1,), (1,)), ((), ()))
NN = (((1,), (0,)), ((), ()))
TN = (((0,), (0,)), ((), ()))
f32 = jnp.float32
bf16 = jnp.bfloat16


def matmul(a, b, dims=NN):
    return lax.dot_general(a, b, dims, preferred_element_type=f32)


def halves(value):
    high = value.astype(bf16)
    return (high, (value - high.astype(f32)).astype(bf16))


def exchange(value, axis, distance):
    return lax.ppermute(value, axis, [(i, i ^ distance) for i in range(lax.axis_size(axis))])


def gather_plan(count):
    half = count // 2
    direct = dict.fromkeys(k for k in (half, 2, 1, count - 1) if k < count)
    plan = [(k, 0) for k in direct]
    for k in range(3, count):
        if k not in direct:
            plan.append((k, half if k & half else 2 if k == 3 else 0))
    return plan


def gathered_pieces(value, axis):
    pieces = {0: value}
    for k, source in gather_plan(lax.axis_size(axis)):
        pieces[k] = exchange(pieces[source], axis, k ^ source)
    return [pieces[k] for k in sorted(pieces)]


WIDE_GRANT = 63500
SURVEY_FLOPS = 15 * 10**9
SURVEY_BYTES = 40 * 10**6


def call(kernel, out_shapes, in_specs, args, flops, traffic, scratch=(), grant=24 << 10):
    single = not isinstance(out_shapes, (tuple, list))
    return pl.pallas_call(
        kernel,
        out_shape=out_shapes,
        in_specs=in_specs,
        out_specs=VMEM_SPEC if single else [VMEM_SPEC] * len(out_shapes),
        scratch_shapes=list(scratch),
        compiler_params=pltpu.CompilerParams(vmem_limit_bytes=grant << 10),
        cost_estimate=pl.CostEstimate(flops=flops, bytes_accessed=traffic, transcendentals=0),
    )(*args)


def fetch(sources, targets, sems):
    copies = [
        pltpu.make_async_copy(source, target, sems.at[n])
        for n, (source, target) in enumerate(zip(sources, targets))
    ]
    for copy in copies:
        copy.start()
    return copies


def modulation_kernel(*refs):
    sources = refs[:7]
    out, joined = refs[7:9]
    cond_ref, prompt_ref, *weights = refs[9:14]
    tokens = sources[5].shape[0]
    rows = (joined.at[pl.ds(0, tokens)], joined.at[pl.ds(tokens, sources[6].shape[0])])
    copies = fetch(sources, (cond_ref, prompt_ref, *weights, *rows), refs[14])

    def in_one_row(ref):
        block = ref[...].astype(f32)
        return jnp.concatenate([block[r : r + 1] for r in range(block.shape[0])], axis=1)

    copies[0].wait()
    cond = in_one_row(cond_ref)
    copies[1].wait()
    row = lax.broadcasted_iota(jnp.int32, (8, cond.shape[1]), 0)
    both = jnp.where(row % 2 == 0, cond, in_one_row(prompt_ref))
    conds = (both * jax.nn.sigmoid(both)).astype(bf16)
    products = []
    for copy, weight in zip(copies[2:5], weights):
        copy.wait()
        products.append(matmul(conds, weight[...], NT))
    shifts, scales, gates = products
    row_out = lax.broadcasted_iota(jnp.int32, out.shape, 0)
    out[...] = jnp.where(row_out < 2, shifts, jnp.where(row_out < 4, scales, gates))
    copies[5].wait()
    copies[6].wait()


def row_sums(pieces):
    total, width = pieces[0].shape
    sums = jnp.zeros((total, 128), f32)
    squares = jnp.zeros((total, 128), f32)
    for piece in pieces:
        for c in range(width // 128):
            x = piece[:, c * 128 : (c + 1) * 128].astype(f32)
            sums = sums + x
            squares = squares + x * x
    return (sums, squares)


def add_kernel(mine, theirs, *outs):
    total = mine[...] + theirs[...]
    for out in outs:
        out[...] = total[: out.shape[0]]


def join_kernel(*refs):
    at = 0
    for ref in refs[:-1]:
        refs[-1][at : at + ref.shape[0], :] = ref[...]
        at += ref.shape[0]


def survey_kernel(*refs):
    refs[-2][...], refs[-1][...] = row_sums(refs[:-2])


def block_masks(total, tokens, wanted):
    i = lax.broadcasted_iota(jnp.int32, (total, total), 0)
    j = lax.broadcasted_iota(jnp.int32, (total, total), 1)
    last = tokens // BLK
    bi = jnp.minimum(lax.shift_right_logical(i, BLK.bit_length() - 1), last)
    bj = jnp.minimum(lax.shift_right_logical(j, BLK.bit_length() - 1), last)
    return wanted(i, j, bi, bj)


def project_kernel(count, tokens, heads, surveyed, *refs):
    pieces = refs[:count]
    mods = refs[count : count + count.bit_length()]
    refs = refs[count + count.bit_length() :]
    down, key_w, value_w, early_sums, early_squares, spikes = refs[:6]
    normed, keys, values, cum_f, cum_b, payload = refs[8:14]
    up_own, bias_own, sems = refs[14:]
    tp = lax.axis_index("tp")
    half = heads * DK
    first = pl.multiple_of(tp * half, half)
    sources = (refs[6].at[:, :, pl.ds(first, half)], refs[7].at[:, pl.ds(first, half)])
    copies = fetch(sources, (up_own, bias_own), sems)
    total, width = pieces[0].shape
    ctx = total - tokens
    features = width * count

    def mod_row(k, row):
        level = k.bit_length()
        at = 4 * (k - (1 << level >> 1)) + row
        return mods[level][at : at + 1, :]

    sums, squares = row_sums([pieces[k] for k in range(count) if k not in surveyed])
    sums, squares = (sums + early_sums[...], squares + early_squares[...])
    mean = jnp.sum(sums, axis=1, keepdims=True) / features
    variance = jnp.sum(squares, axis=1, keepdims=True) / features - mean * mean
    inverse = lax.rsqrt(variance + epsilon)
    for k, piece in enumerate(pieces):
        column = pl.multiple_of(lax.bitwise_xor(tp, k) * width, width)
        scaled = (piece[...].astype(f32) - mean) * inverse
        ahead = scaled[:tokens] * (1.0 + mod_row(k, 2)) + mod_row(k, 0)
        context = scaled[tokens:] * (1.0 + mod_row(k, 3)) + mod_row(k, 1)
        normed[:tokens, pl.ds(column, width)] = ahead.astype(bf16)
        normed[tokens:, pl.ds(column, width)] = context.astype(bf16)
    low_high, low_low = halves(matmul(normed[...], down[...], NT))
    for copy in copies:
        copy.wait()
    blank = jnp.zeros((DECAY_RANK, half), bf16)
    up = jnp.concatenate(
        [
            jnp.concatenate([up_own[0], blank], axis=1),
            jnp.concatenate([blank, up_own[1]], axis=1),
        ],
        axis=0,
    )
    bias = jnp.concatenate([bias_own[0:1, :], bias_own[1:2, :]], axis=1)
    pre = matmul(low_high, up) + matmul(low_low, up) + bias
    decay = (jnp.minimum(pre, 0.0) - jnp.log1p(jnp.exp(-jnp.abs(pre)))) * (1.0 / gate_norm)
    row = lax.broadcasted_iota(jnp.int32, (spikes.shape[1], half), 0)
    head = lax.shift_right_logical(
        lax.broadcasted_iota(jnp.int32, (spikes.shape[1], half), 1), DK.bit_length() - 1
    )
    wanted = jnp.where(row == head + tp * heads, 1.0, 0.0).astype(bf16)
    marks = []
    for d in range(2):
        spike_high, spike_low = halves(spikes[d])
        added = matmul(spike_high, wanted, TN) + matmul(spike_low, wanted, TN)
        marks.append(decay[:tokens, d * half : (d + 1) * half] + added)
    decay = jnp.concatenate([jnp.concatenate(marks, axis=1), decay[tokens:]], axis=0)
    ones = jnp.ones((total, total), f32)
    zeros = jnp.zeros((total, total), f32)
    lower = block_masks(
        total, tokens, lambda i, j, bi, bj: jnp.where((bi == bj) & (i >= j), ones, zeros)
    ).astype(bf16)
    upper = block_masks(
        total, tokens, lambda i, j, bi, bj: jnp.where((bi == bj) & (i <= j), ones, zeros)
    ).astype(bf16)
    high, low = halves(decay)
    cf = matmul(lower, high[:, :half]) + matmul(lower, low[:, :half])
    cb = matmul(upper, high[:, half:]) + matmul(upper, low[:, half:])
    cum_f[...] = cf[:tokens]
    cum_b[...] = cb[:tokens]
    key_all = matmul(normed[...], key_w[...], NT).astype(bf16)
    keys[...] = key_all[:tokens]
    value_all = matmul(normed[...], value_w[...], NT).astype(bf16)
    values[...] = value_all[:tokens]
    wide = value_all.shape[1] // heads
    blocks = tokens // BLK
    size = heads * wide
    growth = [[], [], [], []]
    start = 2 * size + growth_rows(heads)
    for h in range(heads):
        own = slice(h * DK, (h + 1) * DK)
        kh = key_all[:, own].astype(f32)
        vh = value_all[:tokens, h * wide : (h + 1) * wide]
        cfh, cbh = (cf[:, own], cb[:, own])
        ends_f = [cfh[(b + 1) * BLK - 1 : (b + 1) * BLK] for b in range(blocks)]
        ends_b = [cbh[b * BLK : b * BLK + 1] for b in range(blocks)]
        weighted_f, weighted_b = ([], [])
        for b in range(blocks):
            rows = slice(b * BLK, (b + 1) * BLK)
            weighted_f.append(kh[rows] * jnp.exp(sum(ends_f[b + 1 :], ends_f[b]) - cfh[rows]))
            weighted_b.append(kh[rows] * jnp.exp(sum(ends_b[:b], ends_b[b]) - cbh[rows]))
        kf = jnp.concatenate(weighted_f, axis=0).astype(bf16)
        kb = jnp.concatenate(weighted_b, axis=0).astype(bf16)
        payload[h * wide : (h + 1) * wide, :] = matmul(vh, kf, TN).astype(bf16)
        payload[size + h * wide : size + (h + 1) * wide, :] = matmul(vh, kb, TN).astype(bf16)
        growth[0].append(jnp.exp(sum(ends_f[1:], ends_f[0])))
        growth[1].append(jnp.exp(sum(ends_b[1:], ends_b[0])))
        end_f, end_b = (cfh[total - 1 : total], cbh[tokens : tokens + 1])
        growth[2].append(jnp.exp(end_f))
        growth[3].append(jnp.exp(end_b))
        at = start + h * ctx
        payload[at : at + ctx, :] = (kh[tokens:] * jnp.exp(end_f - cfh[tokens:])).astype(bf16)
        at = at + heads * ctx
        payload[at : at + ctx, :] = (kh[tokens:] * jnp.exp(end_b - cbh[tokens:])).astype(bf16)
    for c in range(size // DK):
        at = start + (2 * heads + c) * ctx
        payload[at : at + ctx, :] = value_all[tokens:, c * DK : (c + 1) * DK]
    payload[2 * size : start, :] = growth_block(growth, heads)


def growth_rows(heads):
    return -(-4 * heads // 16) * 16


def growth_block(growth, heads):
    rows = [row for kind in growth for row in kind]
    blank = jnp.zeros((growth_rows(heads) - len(rows), DK), f32)
    return jnp.concatenate([*rows, blank], axis=0).astype(bf16)


def growth_of(ref, at, kind, h, heads):
    block = ref[at : at + growth_rows(heads), :].astype(f32)
    return block[kind * heads + h : kind * heads + h + 1]


def within_kernel(
    heads,
    normed,
    query_w,
    gate_w,
    keys,
    values,
    cum_f,
    cum_b,
    gain,
    inside,
    reach_f,
    reach_b,
    gated,
):
    tokens = keys.shape[0]
    rows_in = normed[:tokens, :]
    query_all = matmul(rows_in, query_w[...], NT).astype(bf16).astype(f32) * DK ** (-0.5)
    wide = values.shape[1] // heads
    blocks = tokens // BLK

    def choose(i, j, bi, bj):
        same = bi == bj
        return (same & (i >= j), same & (i <= j), bi > bj, bi < bj)

    forward, backward, later, sooner = block_masks(tokens, tokens, choose)
    for h in range(heads):
        own = slice(h * DK, (h + 1) * DK)
        qh = query_all[:, own]
        kh = keys[:, own].astype(f32)
        cf, cb = (cum_f[:, own], cum_b[:, own])
        ends_f = [cf[(b + 1) * BLK - 1 : (b + 1) * BLK] for b in range(blocks)]
        ends_b = [cb[b * BLK : b * BLK + 1] for b in range(blocks)]
        spread = (BLK, DK)
        end_f = jnp.concatenate([jnp.broadcast_to(e, spread) for e in ends_f], axis=0)
        end_b = jnp.concatenate([jnp.broadcast_to(e, spread) for e in ends_b], axis=0)
        qf, qb = (qh * jnp.exp(cf), qh * jnp.exp(cb))
        qf_b, qb_b = (qf.astype(bf16), qb.astype(bf16))
        scores = (
            jnp.where(forward, matmul(qf_b, (kh * jnp.exp(-cf)).astype(bf16), NT), 0.0)
            + jnp.where(backward, matmul(qb_b, (kh * jnp.exp(-cb)).astype(bf16), NT), 0.0)
            + jnp.where(later, matmul(qf_b, (kh * jnp.exp(end_f - cf)).astype(bf16), NT), 0.0)
            + jnp.where(sooner, matmul(qb_b, (kh * jnp.exp(end_b - cb)).astype(bf16), NT), 0.0)
        )
        vh = values[:, h * wide : (h + 1) * wide]
        inside[:, h * wide : (h + 1) * wide] = matmul(scores.astype(bf16), vh)
        for b in range(blocks):
            rows = slice(b * BLK, (b + 1) * BLK)
            before = sum(ends_f[:b], jnp.zeros_like(ends_f[0]))
            after = sum(ends_b[b + 1 :], jnp.zeros_like(ends_b[0]))
            reach_f[rows, own] = (qf[rows] * jnp.exp(before)).astype(bf16)
            reach_b[rows, own] = (qb[rows] * jnp.exp(after)).astype(bf16)
    gates = matmul(rows_in, gate_w[...], NT).astype(bf16).astype(f32)
    gated[...] = gains_of(gates, gain[...])


def gains_of(gates, gain):
    return gates * jax.nn.sigmoid(gates) * gain


def merge_kernel(bit, final, heads, ctx, own, partner, out):
    size = (own.shape[0] - growth_rows(heads) - 4 * heads * ctx) // 2
    lift = growth_rows(heads)
    states = 1 if final else 2
    sp = lax.axis_index("sp")
    side = lax.bitwise_and(lax.shift_right_logical(sp, bit), 1)
    onward = lax.bitwise_and(lax.shift_right_logical(sp, bit + 1), 1)

    def emit(low, up):
        wide = size // heads

        def forward(at):
            for h in range(heads):
                rows = slice(h * wide, (h + 1) * wide)
                decayed = growth_of(up, 2 * size, 0, h, heads) * low[rows, :].astype(f32)
                out[at + h * wide : at + (h + 1) * wide, :] = (
                    decayed + up[rows, :].astype(f32)
                ).astype(bf16)

        def backward(at):
            for h in range(heads):
                rows = slice(size + h * wide, size + (h + 1) * wide)
                decayed = growth_of(low, 2 * size, 1, h, heads) * up[rows, :].astype(f32)
                out[at + h * wide : at + (h + 1) * wide, :] = (
                    decayed + low[rows, :].astype(f32)
                ).astype(bf16)

        if final:
            pl.when(onward == 0)(lambda: forward(0))
            pl.when(onward == 1)(lambda: backward(0))
        else:
            forward(0)
            backward(size)
        out[states * size : states * size + lift, :] = (
            low[2 * size : 2 * size + lift, :].astype(f32)
            * up[2 * size : 2 * size + lift, :].astype(f32)
        ).astype(bf16)
        base_in, base_out = (2 * size + lift, states * size + lift)
        for section in range(4 * heads):
            before = low[base_in + section * ctx : base_in + (section + 1) * ctx, :]
            after = up[base_in + section * ctx : base_in + (section + 1) * ctx, :]
            if section < heads:
                before = before.astype(f32) * growth_of(up, 2 * size, 2, section, heads)
            elif section < 2 * heads:
                after = after.astype(f32) * growth_of(low, 2 * size, 3, section - heads, heads)
            at = base_out + 2 * section * ctx
            out[at : at + ctx, :] = before.astype(bf16)
            out[at + ctx : at + 2 * ctx, :] = after.astype(bf16)

    pl.when(side == 0)(lambda: emit(own, partner))
    pl.when(side == 1)(lambda: emit(partner, own))


def finish_kernel(steps, heads, ctx, *refs):
    own = refs[0]
    partners = refs[1 : 1 + steps]
    inside, reach_f, reach_b, gated, out, start_f, start_b, grow_f, grow_b = refs[1 + steps :]
    sp = lax.axis_index("sp")
    size = start_f.shape[0]
    wide = size // heads
    start_f[...] = jnp.zeros(start_f.shape, f32)
    start_b[...] = jnp.zeros(start_b.shape, f32)
    grow_f[...] = jnp.ones(grow_f.shape, f32)
    grow_b[...] = jnp.ones(grow_b.shape, f32)

    def take(start, grow, partner, at, kind, states):
        for h in range(heads):
            rows = slice(h * wide, (h + 1) * wide)
            one = slice(h, h + 1)
            theirs = partner[at + h * wide : at + (h + 1) * wide, :].astype(f32)
            start[rows, :] = start[rows, :] + grow[one, :] * theirs
            grow[one, :] = grow[one, :] * growth_of(partner, states * size, kind, h, heads)

    for step in range(steps):
        side = lax.bitwise_and(lax.shift_right_logical(sp, step), 1)
        states = 1 if step == steps - 1 and steps > 1 else 2
        partner = partners[step]
        back = size if states == 2 else 0
        pl.when(side == 1)(functools.partial(take, start_f, grow_f, partner, 0, 0, states))
        pl.when(side == 0)(functools.partial(take, start_b, grow_b, partner, back, 1, states))

    states = 1 if steps > 1 else 2
    lift = growth_rows(heads)
    base = states * size + lift
    rows_each = ctx << (steps - 1)

    def context(low, up):
        def part(ref, section):
            return ref[base + section * rows_each : base + (section + 1) * rows_each, :]

        for h in range(heads):
            one = slice(h, h + 1)
            grow_up = growth_of(up, states * size, 2, h, heads)
            grow_low = growth_of(low, states * size, 3, h, heads)
            kf = [(part(low, h).astype(f32) * grow_up).astype(bf16), part(up, h)]
            kb = [part(low, heads + h), (part(up, heads + h).astype(f32) * grow_low).astype(bf16)]
            first = 2 * heads + h * (wide // DK)
            for c in range(wide // DK):
                vs = jnp.concatenate([part(low, first + c), part(up, first + c)], axis=0)
                at = slice(h * wide + c * DK, h * wide + (c + 1) * DK)
                start_f[at, :] += grow_f[one, :] * matmul(vs, jnp.concatenate(kf, axis=0), TN)
                start_b[at, :] += grow_b[one, :] * matmul(vs, jnp.concatenate(kb, axis=0), TN)

    side = lax.bitwise_and(lax.shift_right_logical(sp, steps - 1), 1)
    pl.when(side == 0)(lambda: context(own, partners[-1]))
    pl.when(side == 1)(lambda: context(partners[-1], own))
    i = lax.broadcasted_iota(jnp.int32, (DK, DK), 0)
    j = lax.broadcasted_iota(jnp.int32, (DK, DK), 1)
    shift = VGROUP.bit_length() - 1
    alike = lax.shift_right_logical(i, shift) == lax.shift_right_logical(j, shift)
    averaging = jnp.where(alike, 1.0 / VGROUP, 0.0).astype(bf16)
    for h in range(heads):
        own_rows = slice(h * wide, (h + 1) * wide)
        lanes = slice(h * DK, (h + 1) * DK)
        result = (
            inside[:, own_rows]
            + matmul(reach_f[:, lanes], start_f[own_rows, :].astype(bf16), NT)
            + matmul(reach_b[:, lanes], start_b[own_rows, :].astype(bf16), NT)
        )
        for c in range(wide // DK):
            x = result[:, c * DK : (c + 1) * DK]
            high, low = halves(x * x)
            power = matmul(high, averaging) + matmul(low, averaging)
            at = slice(h * wide + c * DK, h * wide + (c + 1) * DK)
            out[:, at] = (x * lax.rsqrt(power + epsilon) * gated[:, at]).astype(bf16)


def branch_of(order, pieces, weight):
    width = pieces[0].shape[1]
    branch = None
    for k, piece in zip(order, pieces):
        column = pl.multiple_of(lax.bitwise_xor(lax.axis_index("tp"), k) * width, width)
        part = matmul(piece[...], weight[:, pl.ds(column, width)], NT)
        branch = part if branch is None else branch + part
    return branch


def early_kernel(order, *refs):
    weight, out = refs[-2:]
    out[...] = branch_of(order, refs[:-2], weight)


def output_kernel(order, *refs):
    weight, early, latent, mod, out = refs[-5:]
    branch = early[...] + branch_of(order, refs[:-5], weight)
    out[...] = (latent[...].astype(f32) + mod[4:5, :] * branch).astype(bf16)


def local_direct(*args):
    return direct_plan(*args)


def direct_plan(
    latent,
    context,
    conditioning,
    context_prompt_vector,
    shift_matrix,
    scale_matrix,
    residual_gate_matrix,
    query_matrix,
    key_matrix,
    value_matrix,
    gate_matrix,
    decay_down_factor,
    decay_up_factor,
    decay_key_bias,
    spike_log_decay,
    output_gain,
    output_matrix,
):
    tp_count, sp_count = (lax.axis_size("tp"), lax.axis_size("sp"))
    heads = HEADS // tp_count
    tokens, width = latent.shape
    ctx = context.shape[0]
    total = tokens + ctx
    features = width * tp_count
    steps = sp_count.bit_length() - 1
    shape = jax.ShapeDtypeStruct

    inner = conditioning.shape[0]
    rows_in = (inner // 128, 128)
    mod, joined = call(
        modulation_kernel,
        [shape((8, width), f32), shape((total, width), bf16)],
        [HBM_SPEC] * 7,
        (
            conditioning.reshape(rows_in),
            context_prompt_vector.reshape(rows_in),
            shift_matrix,
            scale_matrix,
            residual_gate_matrix,
            latent,
            context,
        ),
        6 * 8 * width * inner,
        6 * width * inner,
        [pltpu.VMEM(rows_in, bf16)] * 2
        + [pltpu.VMEM(shift_matrix.shape, bf16)] * 3
        + [pltpu.SemaphoreType.DMA((7,))],
        WIDE_GRANT,
    )
    pieces = gathered_pieces(joined, "tp")
    for bit in range(steps):
        theirs = exchange(mod, "sp", 1 << bit)
        rows = [8] if bit < steps - 1 else [8, 4]
        sums = call(
            add_kernel,
            [shape((r, width), f32) for r in rows],
            [VMEM_SPEC] * 2,
            (mod, theirs),
            8 * width,
            64 * width,
        )
        mod = sums[0]
    mods = [sums[1]]
    for bit in range(tp_count.bit_length() - 1):
        joint = mods[0]
        if bit > 0:
            joint = call(
                join_kernel,
                shape((4 << bit, width), f32),
                [VMEM_SPEC] * len(mods),
                mods,
                8 * width,
                64 * width,
            )
        mods = mods + [exchange(joint, "tp", 1 << bit)]

    half = heads * DK
    down = jnp.transpose(decay_down_factor, (0, 2, 1)).reshape(2 * DECAY_RANK, features)
    vdim = value_matrix.shape[0]
    lift = growth_rows(heads)
    surveyed = [0] + [k for k, source in gather_plan(tp_count) if source == 0][:3]
    early = call(
        survey_kernel,
        [shape((total, 128), f32)] * 2,
        [VMEM_SPEC] * len(surveyed),
        [pieces[k] for k in surveyed],
        SURVEY_FLOPS,
        SURVEY_BYTES,
    )
    normed, keys, values, cum_f, cum_b, payload = call(
        functools.partial(project_kernel, tp_count, tokens, heads, surveyed),
        [
            shape((total, features), bf16),
            shape((tokens, half), bf16),
            shape((tokens, vdim), bf16),
            shape((tokens, half), f32),
            shape((tokens, half), f32),
            shape((2 * vdim + lift + 4 * heads * ctx, DK), bf16),
        ],
        [VMEM_SPEC] * (tp_count + len(mods) + 6) + [HBM_SPEC] * 2,
        (
            *pieces,
            *mods,
            down,
            key_matrix,
            value_matrix,
            *early,
            jnp.transpose(spike_log_decay, (0, 2, 1)),
            decay_up_factor,
            decay_key_bias,
        ),
        2 * total * features * (half + vdim),
        2 * features * (half + vdim),
        [
            pltpu.VMEM((2, DECAY_RANK, half), bf16),
            pltpu.VMEM((2, half), f32),
            pltpu.SemaphoreType.DMA((2,)),
        ],
    )
    partners = [exchange(payload, "sp", 1)]
    rows = ctx
    for bit in range(steps - 1):
        final = bit == steps - 2
        states = 1 if final else 2
        payload = call(
            functools.partial(merge_kernel, bit, final, heads, rows),
            shape((states * vdim + lift + 8 * heads * rows, DK), bf16),
            [VMEM_SPEC, VMEM_SPEC],
            (payload, partners[-1]),
            4 * vdim * DK,
            8 * vdim * DK,
        )
        rows = 2 * rows
        partners.append(exchange(payload, "sp", 2 << bit))
    inside, reach_f, reach_b, gated = call(
        functools.partial(within_kernel, heads),
        [
            shape((tokens, vdim), f32),
            shape((tokens, half), bf16),
            shape((tokens, half), bf16),
            shape((tokens, vdim), f32),
        ],
        [VMEM_SPEC] * 8,
        (
            normed,
            query_matrix,
            gate_matrix,
            keys,
            values,
            cum_f,
            cum_b,
            output_gain[None],
        ),
        2 * tokens * features * (half + vdim),
        2 * features * (half + vdim),
    )
    heads_out = call(
        functools.partial(finish_kernel, steps, heads, ctx),
        shape((tokens, vdim), bf16),
        [VMEM_SPEC] * (5 + steps),
        (payload, *partners, inside, reach_f, reach_b, gated),
        8 * tokens * vdim * DK,
        8 * tokens * vdim,
        [
            pltpu.VMEM((vdim, DK), f32),
            pltpu.VMEM((vdim, DK), f32),
            pltpu.VMEM((8 * -(-heads // 8), DK), f32),
            pltpu.VMEM((8 * -(-heads // 8), DK), f32),
        ],
    )
    branches = gathered_pieces(heads_out, "tp")
    late = [k for k in range(1, tp_count) if k >= tp_count - 3]
    soon = [k for k in range(tp_count) if k not in late]
    cost = 2 * width * vdim
    early = call(
        functools.partial(early_kernel, soon),
        shape((tokens, width), f32),
        [VMEM_SPEC] * (len(soon) + 1),
        (*(branches[k] for k in soon), output_matrix),
        tokens * cost * len(soon),
        cost * len(soon),
    )
    return call(
        functools.partial(output_kernel, late),
        shape((tokens, width), bf16),
        [VMEM_SPEC] * (len(late) + 4),
        (*(branches[k] for k in late), output_matrix, early, latent, mod),
        tokens * cost * len(late),
        cost * len(late),
    )


def solution(mesh):
    placed = (
        P("sp", "tp"),
        P("sp", "tp"),
        P("sp"),
        P("sp"),
        P("tp", "sp"),
        P("tp", "sp"),
        P("tp", "sp"),
        P("tp", None),
        P("tp", None),
        P("tp", None),
        P("tp", None),
        P(),
        P(),
        P(),
        P(None, "sp", None),
        P("tp"),
        P("tp", None),
    )
    tp_count, sp_count = (mesh.shape["tp"], mesh.shape["sp"])
    powers = tp_count & tp_count - 1 == 0 and sp_count & sp_count - 1 == 0
    direct = 2 <= tp_count <= HEADS and sp_count >= 2 and powers
    return jax.shard_map(
        local_direct if direct else local_general, mesh=mesh, in_specs=placed, out_specs=P("sp", "tp"), check_vma=False
    )
```

```python
import functools

import jax
import jax.numpy as jnp
from jax import lax
from jax.experimental import pallas as pl
from jax.experimental.pallas import tpu as pltpu
from jax.sharding import PartitionSpec as P


D = 4096
HEADS = 16
DK = 128
DECAY_RANK = 16
BLK = 64
VGROUP = 64


epsilon = 1e-05
gate_norm = 16.0
precise = lax.Precision.HIGHEST


def for_sending(value):

    def short(part):
        return part.astype(jnp.bfloat16) if part.dtype == jnp.float32 else part

    return jax.tree.map(short, value)


def from_partner(value, axis, distance):
    return lax.ppermute(value, axis, [(i, i ^ 1 << distance) for i in range(lax.axis_size(axis))])


def carried_in(value, axis, combine, identity, reverse):
    peers, index = (lax.axis_size(axis), lax.axis_index(axis))
    everything = jax.tree.map(
        lambda part, kind: lax.all_gather(part.astype(kind), axis),
        value,
        (jnp.bfloat16, jnp.bfloat16),
    )
    start = jax.tree.map(
        lambda part, zero: jnp.broadcast_to(jnp.asarray(zero, part.dtype), part.shape),
        value,
        identity,
    )

    def turn(k, before):
        at = peers - 1 - k if reverse else k
        reached = at > index if reverse else at < index
        new = combine(
            before, jax.tree.map(lambda part, own: part[at].astype(own.dtype), everything, value)
        )
        return jax.tree.map(lambda a, b: jnp.where(reached, a, b), new, before)

    return lax.fori_loop(0, peers, turn, start)


def linear(rows, weight):
    return lax.dot_general(
        rows, weight, (((1,), (1,)), ((), ())), preferred_element_type=jnp.float32
    )


def modulated(rows, row_sum, row_squares, shift_vec, scale_vec):
    rows_f = rows.astype(jnp.float32)
    mean_val = row_sum / D
    variance = row_squares / D - mean_val * mean_val
    return (
        (rows_f - mean_val) * lax.rsqrt(variance + epsilon) * (1.0 + scale_vec) + shift_vec
    ).astype(jnp.bfloat16)


def reverse_rows(array):
    return jnp.flip(array, axis=0)


def end_state(key_rows, value_rows, log_decay):
    cumulative = jnp.cumsum(log_decay, axis=0)
    totals = cumulative[-1]
    weighted = key_rows * jnp.exp(totals - cumulative)
    return (jnp.exp(totals), jnp.einsum("nhd,nhe->hde", weighted, value_rows, precision=precise))


def combine(earlier, later):
    return (earlier[0] * later[0], later[0][..., None] * earlier[1] + later[1])


def blockwise(queries, key_rows, value_rows, log_decay, carried, block_len):
    length, head_count, _ = queries.shape
    value_width = value_rows.shape[-1]
    blocks = length // block_len

    def shaped(array):
        return array.reshape(blocks, block_len, head_count, array.shape[-1])

    triangle = jnp.tril(jnp.ones((block_len, block_len), jnp.float32))

    def advance(state_now, inputs):
        block_q, block_k, block_v, block_a = inputs
        cumulative = jnp.cumsum(block_a, axis=0)
        block_end = cumulative[-1]
        query_dec = block_q * jnp.exp(cumulative)
        scores = (
            jnp.einsum("ihd,jhd->hij", query_dec, block_k * jnp.exp(-cumulative), precision=precise)
            * triangle
        )
        result = jnp.einsum("hij,jhe->ihe", scores, block_v, precision=precise)
        result = result + jnp.einsum("ihd,hde->ihe", query_dec, state_now, precision=precise)
        state_next = state_now * jnp.exp(block_end)[:, :, None] + jnp.einsum(
            "jhd,jhe->hde", block_k * jnp.exp(block_end - cumulative), block_v, precision=precise
        )
        return (state_next, result)

    _, outputs = lax.scan(
        advance, carried, (shaped(queries), shaped(key_rows), shaped(value_rows), shaped(log_decay))
    )
    return outputs.reshape(length, head_count, value_width)


def head_channels(pieces, per_head, tp_index):
    for bit_number in range(per_head.bit_length() - 1):
        partner = from_partner(
            (for_sending(pieces[0]), for_sending(pieces[1]), for_sending(pieces[2])),
            "tp",
            bit_number,
        )
        upper = tp_index // (1 << bit_number) % 2 == 1
        pieces = tuple(
            (
                jnp.where(
                    upper,
                    jnp.concatenate([theirs, mine], axis=1),
                    jnp.concatenate([mine, theirs], axis=1),
                )
                for mine, theirs in zip(pieces, partner)
            )
        )
    return pieces


def context_totals(fwd_growth, fwd_state, bwd_growth, bwd_state, identity):

    def absorb(carried, piece):
        return (combine(carried, piece), None)

    total_fwd, _ = lax.scan(absorb, identity, (fwd_growth, fwd_state))
    total_bwd, _ = lax.scan(absorb, identity, (bwd_growth, bwd_state), reverse=True)
    return (total_fwd, total_bwd)


def stored(array):
    return lax.optimization_barrier(array.astype(jnp.bfloat16))


def local_general(
    latent,
    context,
    conditioning,
    context_prompt_vector,
    shift_matrix,
    scale_matrix,
    residual_gate_matrix,
    query_matrix,
    key_matrix,
    value_matrix,
    gate_matrix,
    decay_down_factor,
    decay_up_factor,
    decay_key_bias,
    spike_log_decay,
    output_gain,
    output_matrix,
):
    tp_count = lax.axis_size("tp")
    tp_index = lax.axis_index("tp")
    per_head = max(tp_count // HEADS, 1)
    heads_per_shard = max(HEADS // tp_count, 1)
    leading_head = tp_index // per_head * heads_per_shard
    tok_rows = latent.shape[0]
    conds = jax.nn.silu(
        jnp.stack([conditioning, context_prompt_vector]).astype(jnp.float32)
    ).astype(jnp.bfloat16)
    shifts, scales, gates = lax.psum(
        (
            linear(conds, shift_matrix),
            linear(conds, scale_matrix),
            linear(conds, residual_gate_matrix),
        ),
        "sp",
    )
    down_both = jnp.concatenate([decay_down_factor[0].T, decay_down_factor[1].T], axis=0)
    lat_weights = (query_matrix, key_matrix, value_matrix, gate_matrix, down_both)
    ctx_weights = (key_matrix, value_matrix, down_both)
    lat_f = latent.astype(jnp.float32)
    ctx_f = context.astype(jnp.float32)
    lat_sum, lat_squares, ctx_sum, ctx_squares = lax.psum(
        (
            jnp.sum(lat_f, axis=1, keepdims=True),
            jnp.sum(lat_f * lat_f, axis=1, keepdims=True),
            jnp.sum(ctx_f, axis=1, keepdims=True),
            jnp.sum(ctx_f * ctx_f, axis=1, keepdims=True),
        ),
        "tp",
    )
    latent_normalized = modulated(latent, lat_sum, lat_squares, shifts[0], scales[0])
    normed_ctx = modulated(context, ctx_sum, ctx_squares, shifts[1], scales[1])
    lat_piece = lax.all_gather(latent_normalized, "tp", axis=1, tiled=True)
    ctx_piece = lax.all_gather(normed_ctx, "tp", axis=1, tiled=True)
    lat_new = tuple((linear(lat_piece, weight) for weight in lat_weights))
    ctx_new = tuple((linear(ctx_piece, weight) for weight in ctx_weights))
    query_part, key_part, value_part, gate_part, low_rank_part = lat_new
    ctx_key_part, ctx_value_part, ctx_low = ctx_new
    query_full, key_full, ctx_key_full = head_channels(
        (stored(query_part), stored(key_part), stored(ctx_key_part)), per_head, tp_index
    )

    def split_heads(rows, width):
        return rows.astype(jnp.float32).reshape(rows.shape[0], heads_per_shard, width)

    value_cols = value_part.shape[1] // heads_per_shard
    queries = split_heads(query_full, DK) * DK ** (-0.5)
    key_rows = split_heads(key_full, DK)
    ctx_keys = split_heads(ctx_key_full, DK)
    values_lat = split_heads(stored(value_part), value_cols)
    values_ctx = split_heads(stored(ctx_value_part), value_cols)
    gate_rows = stored(gate_part).astype(jnp.float32)

    def per_head_decay(low_rows, direction):
        up_part = lax.dynamic_slice_in_dim(
            decay_up_factor[direction], leading_head * DK, heads_per_shard * DK, 1
        ).astype(jnp.float32)
        bias_part = lax.dynamic_slice_in_dim(
            decay_key_bias[direction], leading_head * DK, heads_per_shard * DK, 0
        )
        pre_act = jnp.dot(low_rows, up_part, precision=precise) + bias_part
        return (jax.nn.log_sigmoid(pre_act) / gate_norm).reshape(
            low_rows.shape[0], heads_per_shard, DK
        )

    decay_spikes = lax.dynamic_slice_in_dim(spike_log_decay, leading_head, heads_per_shard, 2)
    latent_forward = per_head_decay(low_rank_part[:, :DECAY_RANK], 0) + decay_spikes[0][:, :, None]
    latent_backward = per_head_decay(low_rank_part[:, DECAY_RANK:], 1) + decay_spikes[1][:, :, None]
    ctx_fwd = per_head_decay(ctx_low[:, :DECAY_RANK], 0)
    ctx_bwd = per_head_decay(ctx_low[:, DECAY_RANK:], 1)
    cf_growth, cf_state = end_state(ctx_keys, values_ctx, ctx_fwd)
    cb_growth, cb_state = end_state(
        reverse_rows(ctx_keys), reverse_rows(values_ctx), reverse_rows(ctx_bwd)
    )
    lf_growth, lf_state = end_state(key_rows, values_lat, latent_forward)
    lb_growth, lb_state = end_state(
        reverse_rows(key_rows), reverse_rows(values_lat), reverse_rows(latent_backward)
    )
    identity = (
        jnp.ones((heads_per_shard, DK), jnp.float32),
        jnp.zeros((heads_per_shard, DK, value_cols), jnp.float32),
    )
    ctx_gathered = (
        lax.all_gather(cf_growth[None].astype(jnp.bfloat16), "sp", axis=0, tiled=True).astype(
            jnp.float32
        ),
        lax.all_gather(cf_state[None].astype(jnp.bfloat16), "sp", axis=0, tiled=True).astype(
            jnp.float32
        ),
        lax.all_gather(cb_growth[None].astype(jnp.bfloat16), "sp", axis=0, tiled=True).astype(
            jnp.float32
        ),
        lax.all_gather(cb_state[None].astype(jnp.bfloat16), "sp", axis=0, tiled=True).astype(
            jnp.float32
        ),
    )
    total_fwd, total_bwd = context_totals(
        ctx_gathered[0], ctx_gathered[1], ctx_gathered[2], ctx_gathered[3], identity
    )
    prefix = carried_in((lf_growth, lf_state), "sp", combine, identity, False)
    suffix = carried_in((lb_growth, lb_state), "sp", combine, identity, True)
    start_fwd = combine(total_fwd, prefix)[1]
    start_bwd = combine(total_bwd, suffix)[1]
    zero_state = jnp.zeros((heads_per_shard, DK, value_cols), jnp.float32)

    def direction_out(query_rows, key_list, value_list, log_decay, start_state):
        local_part = blockwise(query_rows, key_list, value_list, log_decay, zero_state, BLK)
        reach = query_rows * jnp.exp(jnp.cumsum(log_decay, axis=0))
        return local_part + jnp.einsum("nhd,hde->nhe", reach, start_state, precision=precise)

    out_fwd = direction_out(queries, key_rows, values_lat, latent_forward, start_fwd)
    out_bwd = reverse_rows(
        direction_out(
            reverse_rows(queries),
            reverse_rows(key_rows),
            reverse_rows(values_lat),
            reverse_rows(latent_backward),
            start_bwd,
        )
    )
    grouped = (out_fwd + out_bwd).reshape(tok_rows, -1, VGROUP)
    grouped = grouped * lax.rsqrt(jnp.mean(grouped * grouped, axis=-1, keepdims=True) + epsilon)
    heads_out = (grouped.reshape(tok_rows, -1) * output_gain * jax.nn.silu(gate_rows)).astype(
        jnp.bfloat16
    )
    branch = linear(lax.all_gather(heads_out, "tp", axis=1, tiled=True), output_matrix)
    return (latent.astype(jnp.float32) + gates[0] * branch).astype(jnp.bfloat16)


VMEM_SPEC = pl.BlockSpec(memory_space=pltpu.VMEM)
HBM_SPEC = pl.BlockSpec(memory_space=pltpu.HBM)
NT = (((1,), (1,)), ((), ()))
NN = (((1,), (0,)), ((), ()))
TN = (((0,), (0,)), ((), ()))
f32 = jnp.float32
bf16 = jnp.bfloat16


def matmul(a, b, dims=NN):
    return lax.dot_general(a, b, dims, preferred_element_type=f32)


def halves(value):
    high = value.astype(bf16)
    return (high, (value - high.astype(f32)).astype(bf16))


def exchange(value, axis, distance):
    return lax.ppermute(value, axis, [(i, i ^ distance) for i in range(lax.axis_size(axis))])


def gather_plan(count, label):
    if count == 8:
        return PLANS[label]
    half = count // 2
    direct = dict.fromkeys(k for k in (half, 2, 1, count - 1) if k < count)
    plan = [(k, 0) for k in direct]
    for k in range(3, count):
        if k not in direct:
            plan.append((k, half if k & half else 2 if k == 3 else 0))
    return plan


def gathered_pieces(value, axis, label):
    pieces = {0: value}
    for k, source in gather_plan(lax.axis_size(axis), label):
        pieces[k] = exchange(pieces[source], axis, k ^ source)
    return [pieces[k] for k in sorted(pieces)]


def mod_steps(count):
    return MOD_STEPS if count == 8 else tuple(1 << bit for bit in range(count.bit_length() - 1))


WIDE_GRANT = 60000
STAGE_GRANT = 2 << 10
SURVEY_FLOPS = 15 * 10**9
SURVEY_BYTES = 40 * 10**6
MOD_STEPS = (1, 2, 4)
PLANS = {
    "lat": ((4, 0), (2, 0), (1, 0), (7, 0), (3, 2), (5, 4), (6, 4)),
    "out": ((2, 0), (4, 0), (1, 0), (3, 2), (7, 0), (5, 4), (6, 4)),
}


def call(kernel, out_shapes, in_specs, args, flops, traffic, scratch=(), grant=24 << 10):
    single = not isinstance(out_shapes, (tuple, list))
    return pl.pallas_call(
        kernel,
        out_shape=out_shapes,
        in_specs=in_specs,
        out_specs=VMEM_SPEC if single else [VMEM_SPEC] * len(out_shapes),
        scratch_shapes=list(scratch),
        compiler_params=pltpu.CompilerParams(vmem_limit_bytes=grant << 10),
        cost_estimate=pl.CostEstimate(flops=flops, bytes_accessed=traffic, transcendentals=0),
    )(*args)


def fetch(sources, targets, sems):
    copies = [
        pltpu.make_async_copy(source, target, sems.at[n])
        for n, (source, target) in enumerate(zip(sources, targets))
    ]
    for copy in copies:
        copy.start()
    return copies


def in_one_row(ref):
    block = ref[...].astype(f32)
    return jnp.concatenate([block[r : r + 1] for r in range(block.shape[0])], axis=1)


def modulation_kernel(*refs):
    sources = refs[:6]
    out, joined = refs[6:8]
    cond_ref, prompt_ref, *weights = refs[8:12]
    tokens = sources[4].shape[0]
    rows = (joined.at[pl.ds(0, tokens)], joined.at[pl.ds(tokens, sources[5].shape[0])])
    copies = fetch(sources, (cond_ref, prompt_ref, *weights, *rows), refs[12])
    copies[0].wait()
    cond = in_one_row(cond_ref)
    copies[1].wait()
    row = lax.broadcasted_iota(jnp.int32, (8, cond.shape[1]), 0)
    both = jnp.where(row % 2 == 0, cond, in_one_row(prompt_ref))
    conds = (both * jax.nn.sigmoid(both)).astype(bf16)
    row_out = lax.broadcasted_iota(jnp.int32, out.shape, 0)
    copies[2].wait()
    shifts = matmul(conds, weights[0][...], NT)
    copies[3].wait()
    scales = matmul(conds, weights[1][...], NT)
    out[...] = jnp.where(row_out < 2, shifts, scales)
    copies[4].wait()
    copies[5].wait()


def gate_rows_of(width):
    return -(-2 * (width // DK) // 16) * 16


def split_row(value):
    count = value.shape[1] // DK
    rows = [value[:, c * DK : (c + 1) * DK] for c in range(count)]
    blank = jnp.zeros((gate_rows_of(value.shape[1]) - 2 * count, DK), bf16)
    parts = [halves(row) for row in rows]
    return jnp.concatenate([p[0] for p in parts] + [p[1] for p in parts] + [blank], axis=0)


def joined_row(block, width):
    count = width // DK
    value = block.astype(f32)
    value = value[:count] + value[count : 2 * count]
    return jnp.concatenate([value[c : c + 1] for c in range(count)], axis=1)


def gating_kernel(cond_ref, weight, out):
    cond = in_one_row(cond_ref)
    cond = jnp.broadcast_to(cond, (8, cond.shape[1]))
    conds = (cond * jax.nn.sigmoid(cond)).astype(bf16)
    out[...] = split_row(matmul(conds, weight[...], NT)[:1])


def row_sums(pieces):
    total, width = pieces[0].shape
    sums = jnp.zeros((total, 128), f32)
    squares = jnp.zeros((total, 128), f32)
    for piece in pieces:
        for c in range(width // 128):
            x = piece[:, c * 128 : (c + 1) * 128].astype(f32)
            sums = sums + x
            squares = squares + x * x
    return (sums, squares)


def add_kernel(mine, theirs, *outs):
    total = mine[...] + theirs[...]
    for out in outs:
        out[...] = total[: out.shape[0]]


def join_kernel(*refs):
    at = 0
    for ref in refs[:-1]:
        refs[-1][at : at + ref.shape[0], :] = ref[...]
        at += ref.shape[0]


def stage_kernel(*refs):
    sources = refs[:-2]
    targets, at = ([], 0)
    for source in sources:
        targets.append(refs[-2].at[pl.ds(at, source.shape[0])])
        at += source.shape[0]
    for copy in fetch(sources, targets, refs[-1]):
        copy.wait()


def survey_kernel(*refs):
    refs[-2][...], refs[-1][...] = row_sums(refs[:-2])


def block_masks(total, tokens, wanted):
    i = lax.broadcasted_iota(jnp.int32, (total, total), 0)
    j = lax.broadcasted_iota(jnp.int32, (total, total), 1)
    last = tokens // BLK
    bi = jnp.minimum(lax.shift_right_logical(i, BLK.bit_length() - 1), last)
    bj = jnp.minimum(lax.shift_right_logical(j, BLK.bit_length() - 1), last)
    return wanted(i, j, bi, bj)


def project_kernel(count, tokens, heads, surveyed, *refs):
    pieces = refs[:count]
    mods = refs[count : count + count.bit_length()]
    refs = refs[count + count.bit_length() :]
    weights, early_sums, early_squares, spikes, gate_part = refs[:5]
    normed, keys, values, cum_f, cum_b, payload = refs[7:13]
    up_own, bias_own, sems = refs[13:]
    tp = lax.axis_index("tp")
    half = heads * DK
    first = pl.multiple_of(tp * half, half)
    sources = (refs[5].at[:, :, pl.ds(first, half)], refs[6].at[:, pl.ds(first, half)])
    copies = fetch(sources, (up_own, bias_own), sems)
    total, width = pieces[0].shape
    ctx = total - tokens
    features = width * count

    held = [[0]]
    for distance in mod_steps(count):
        held.append([k ^ distance for k in sum(held, [])])
    found = {k: (level, at) for level, ks in enumerate(held) for at, k in enumerate(ks)}

    def mod_row(k, row):
        level, at = found[k]
        return mods[level][4 * at + row : 4 * at + row + 1, :]

    sums, squares = row_sums([pieces[k] for k in range(count) if k not in surveyed])
    sums, squares = (sums + early_sums[...], squares + early_squares[...])
    mean = jnp.sum(sums, axis=1, keepdims=True) / features
    variance = jnp.sum(squares, axis=1, keepdims=True) / features - mean * mean
    inverse = lax.rsqrt(variance + epsilon)
    for k, piece in enumerate(pieces):
        column = pl.multiple_of(lax.bitwise_xor(tp, k) * width, width)
        scaled = (piece[...].astype(f32) - mean) * inverse
        ahead = scaled[:tokens] * (1.0 + mod_row(k, 2)) + mod_row(k, 0)
        context = scaled[tokens:] * (1.0 + mod_row(k, 3)) + mod_row(k, 1)
        normed[:tokens, pl.ds(column, width)] = ahead.astype(bf16)
        normed[tokens:, pl.ds(column, width)] = context.astype(bf16)
    products = matmul(weights[...], normed[...], NT).T
    key_all = products[:, :half].astype(bf16)
    value_all = products[:, half : half + values.shape[1]].astype(bf16)
    low_high, low_low = halves(products[:, half + values.shape[1] :])
    for copy in copies:
        copy.wait()
    blank = jnp.zeros((DECAY_RANK, half), bf16)
    up = jnp.concatenate(
        [
            jnp.concatenate([up_own[0], blank], axis=1),
            jnp.concatenate([blank, up_own[1]], axis=1),
        ],
        axis=0,
    )
    bias = jnp.concatenate([bias_own[0:1, :], bias_own[1:2, :]], axis=1)
    pre = matmul(low_high, up) + matmul(low_low, up) + bias
    decay = (jnp.minimum(pre, 0.0) - jnp.log1p(jnp.exp(-jnp.abs(pre)))) * (1.0 / gate_norm)
    row = lax.broadcasted_iota(jnp.int32, (spikes.shape[1], half), 0)
    head = lax.shift_right_logical(
        lax.broadcasted_iota(jnp.int32, (spikes.shape[1], half), 1), DK.bit_length() - 1
    )
    wanted = jnp.where(row == head + tp * heads, 1.0, 0.0).astype(bf16)
    marks = []
    for d in range(2):
        spike_high, spike_low = halves(spikes[d])
        added = matmul(spike_high, wanted, TN) + matmul(spike_low, wanted, TN)
        marks.append(decay[:tokens, d * half : (d + 1) * half] + added)
    decay = jnp.concatenate([jnp.concatenate(marks, axis=1), decay[tokens:]], axis=0)
    ones = jnp.ones((total, total), f32)
    zeros = jnp.zeros((total, total), f32)
    lower = block_masks(
        total, tokens, lambda i, j, bi, bj: jnp.where((bi == bj) & (i >= j), ones, zeros)
    ).astype(bf16)
    upper = block_masks(
        total, tokens, lambda i, j, bi, bj: jnp.where((bi == bj) & (i <= j), ones, zeros)
    ).astype(bf16)
    high, low = halves(decay)
    cf = matmul(lower, high[:, :half]) + matmul(lower, low[:, :half])
    cb = matmul(upper, high[:, half:]) + matmul(upper, low[:, half:])
    cum_f[...] = cf[:tokens]
    cum_b[...] = cb[:tokens]
    keys[...] = key_all[:tokens]
    values[...] = value_all[:tokens]
    wide = value_all.shape[1] // heads
    blocks = tokens // BLK
    size = heads * wide
    growth = [[], [], [], []]
    start = 2 * size + growth_rows(heads)
    for h in range(heads):
        own = slice(h * DK, (h + 1) * DK)
        kh = key_all[:, own].astype(f32)
        vh = value_all[:tokens, h * wide : (h + 1) * wide]
        cfh, cbh = (cf[:, own], cb[:, own])
        ends_f = [cfh[(b + 1) * BLK - 1 : (b + 1) * BLK] for b in range(blocks)]
        ends_b = [cbh[b * BLK : b * BLK + 1] for b in range(blocks)]
        weighted_f, weighted_b = ([], [])
        for b in range(blocks):
            rows = slice(b * BLK, (b + 1) * BLK)
            weighted_f.append(kh[rows] * jnp.exp(sum(ends_f[b + 1 :], ends_f[b]) - cfh[rows]))
            weighted_b.append(kh[rows] * jnp.exp(sum(ends_b[:b], ends_b[b]) - cbh[rows]))
        kf = jnp.concatenate(weighted_f, axis=0).astype(bf16)
        kb = jnp.concatenate(weighted_b, axis=0).astype(bf16)
        payload[h * wide : (h + 1) * wide, :] = matmul(vh, kf, TN).astype(bf16)
        payload[size + h * wide : size + (h + 1) * wide, :] = matmul(vh, kb, TN).astype(bf16)
        growth[0].append(jnp.exp(sum(ends_f[1:], ends_f[0])))
        growth[1].append(jnp.exp(sum(ends_b[1:], ends_b[0])))
        end_f, end_b = (cfh[total - 1 : total], cbh[tokens : tokens + 1])
        growth[2].append(jnp.exp(end_f))
        growth[3].append(jnp.exp(end_b))
        at = start + h * ctx
        payload[at : at + ctx, :] = (kh[tokens:] * jnp.exp(end_f - cfh[tokens:])).astype(bf16)
        at = at + heads * ctx
        payload[at : at + ctx, :] = (kh[tokens:] * jnp.exp(end_b - cbh[tokens:])).astype(bf16)
    for c in range(size // DK):
        at = start + (2 * heads + c) * ctx
        payload[at : at + ctx, :] = value_all[tokens:, c * DK : (c + 1) * DK]
    payload[2 * size : start, :] = growth_block(growth, heads)
    payload[start + 4 * heads * ctx :, :] = gate_part[...]


def growth_rows(heads):
    return -(-4 * heads // 16) * 16


def growth_block(growth, heads):
    rows = [row for kind in growth for row in kind]
    blank = jnp.zeros((growth_rows(heads) - len(rows), DK), f32)
    return jnp.concatenate([*rows, blank], axis=0).astype(bf16)


def growth_of(ref, at, kind, h, heads):
    block = ref[at : at + growth_rows(heads), :].astype(f32)
    return block[kind * heads + h : kind * heads + h + 1]


def within_kernel(
    heads,
    normed,
    query_w,
    gate_w,
    keys,
    values,
    cum_f,
    cum_b,
    gain,
    inside,
    reach_f,
    reach_b,
    gated,
):
    tokens = keys.shape[0]
    rows_in = normed[:tokens, :]
    query_all = matmul(rows_in, query_w[...], NT).astype(bf16).astype(f32) * DK ** (-0.5)
    wide = values.shape[1] // heads
    blocks = tokens // BLK

    def choose(i, j, bi, bj):
        same = bi == bj
        return (same & (i >= j), same & (i <= j), bi > bj, bi < bj)

    forward, backward, later, sooner = block_masks(tokens, tokens, choose)
    for h in range(heads):
        own = slice(h * DK, (h + 1) * DK)
        qh = query_all[:, own]
        kh = keys[:, own].astype(f32)
        cf, cb = (cum_f[:, own], cum_b[:, own])
        ends_f = [cf[(b + 1) * BLK - 1 : (b + 1) * BLK] for b in range(blocks)]
        ends_b = [cb[b * BLK : b * BLK + 1] for b in range(blocks)]
        spread = (BLK, DK)
        end_f = jnp.concatenate([jnp.broadcast_to(e, spread) for e in ends_f], axis=0)
        end_b = jnp.concatenate([jnp.broadcast_to(e, spread) for e in ends_b], axis=0)
        qf, qb = (qh * jnp.exp(cf), qh * jnp.exp(cb))
        qf_b, qb_b = (qf.astype(bf16), qb.astype(bf16))
        scores = (
            jnp.where(forward, matmul(qf_b, (kh * jnp.exp(-cf)).astype(bf16), NT), 0.0)
            + jnp.where(backward, matmul(qb_b, (kh * jnp.exp(-cb)).astype(bf16), NT), 0.0)
            + jnp.where(later, matmul(qf_b, (kh * jnp.exp(end_f - cf)).astype(bf16), NT), 0.0)
            + jnp.where(sooner, matmul(qb_b, (kh * jnp.exp(end_b - cb)).astype(bf16), NT), 0.0)
        )
        vh = values[:, h * wide : (h + 1) * wide]
        inside[:, h * wide : (h + 1) * wide] = matmul(scores.astype(bf16), vh)
        for b in range(blocks):
            rows = slice(b * BLK, (b + 1) * BLK)
            before = sum(ends_f[:b], jnp.zeros_like(ends_f[0]))
            after = sum(ends_b[b + 1 :], jnp.zeros_like(ends_b[0]))
            reach_f[rows, own] = (qf[rows] * jnp.exp(before)).astype(bf16)
            reach_b[rows, own] = (qb[rows] * jnp.exp(after)).astype(bf16)
    gates = matmul(rows_in, gate_w[...], NT).astype(bf16).astype(f32)
    gated[...] = gains_of(gates, gain[...])


def gains_of(gates, gain):
    return gates * jax.nn.sigmoid(gates) * gain


def merge_kernel(bit, final, heads, ctx, width, own, partner, out):
    gate_rows = gate_rows_of(width)
    size = (own.shape[0] - growth_rows(heads) - 4 * heads * ctx - gate_rows) // 2
    lift = growth_rows(heads)
    states = 1 if final else 2
    sp = lax.axis_index("sp")
    side = lax.bitwise_and(lax.shift_right_logical(sp, bit), 1)
    onward = lax.bitwise_and(lax.shift_right_logical(sp, bit + 1), 1)

    def emit(low, up):
        wide = size // heads

        def forward(at):
            for h in range(heads):
                rows = slice(h * wide, (h + 1) * wide)
                decayed = growth_of(up, 2 * size, 0, h, heads) * low[rows, :].astype(f32)
                out[at + h * wide : at + (h + 1) * wide, :] = (
                    decayed + up[rows, :].astype(f32)
                ).astype(bf16)

        def backward(at):
            for h in range(heads):
                rows = slice(size + h * wide, size + (h + 1) * wide)
                decayed = growth_of(low, 2 * size, 1, h, heads) * up[rows, :].astype(f32)
                out[at + h * wide : at + (h + 1) * wide, :] = (
                    decayed + low[rows, :].astype(f32)
                ).astype(bf16)

        if final:
            pl.when(onward == 0)(lambda: forward(0))
            pl.when(onward == 1)(lambda: backward(0))
        else:
            forward(0)
            backward(size)
        out[states * size : states * size + lift, :] = (
            low[2 * size : 2 * size + lift, :].astype(f32)
            * up[2 * size : 2 * size + lift, :].astype(f32)
        ).astype(bf16)
        base_in, base_out = (2 * size + lift, states * size + lift)
        count = out.shape[0]
        mine = joined_row(low[low.shape[0] - gate_rows :, :], width)
        theirs = joined_row(up[up.shape[0] - gate_rows :, :], width)
        out[count - gate_rows :, :] = split_row(mine + theirs)
        for section in range(4 * heads):
            before = low[base_in + section * ctx : base_in + (section + 1) * ctx, :]
            after = up[base_in + section * ctx : base_in + (section + 1) * ctx, :]
            if section < heads:
                before = before.astype(f32) * growth_of(up, 2 * size, 2, section, heads)
            elif section < 2 * heads:
                after = after.astype(f32) * growth_of(low, 2 * size, 3, section - heads, heads)
            at = base_out + 2 * section * ctx
            out[at : at + ctx, :] = before.astype(bf16)
            out[at + ctx : at + 2 * ctx, :] = after.astype(bf16)

    pl.when(side == 0)(lambda: emit(own, partner))
    pl.when(side == 1)(lambda: emit(partner, own))


def finish_kernel(steps, heads, ctx, *refs):
    own = refs[0]
    partners = refs[1 : 1 + steps]
    inside, reach_f, reach_b, gated, out, gates, start_f, start_b, grow_f, grow_b = refs[1 + steps :]
    sp = lax.axis_index("sp")
    size = start_f.shape[0]
    wide = size // heads
    start_f[...] = jnp.zeros(start_f.shape, f32)
    start_b[...] = jnp.zeros(start_b.shape, f32)
    grow_f[...] = jnp.ones(grow_f.shape, f32)
    grow_b[...] = jnp.ones(grow_b.shape, f32)

    def take(start, grow, partner, at, kind, states):
        for h in range(heads):
            rows = slice(h * wide, (h + 1) * wide)
            one = slice(h, h + 1)
            theirs = partner[at + h * wide : at + (h + 1) * wide, :].astype(f32)
            start[rows, :] = start[rows, :] + grow[one, :] * theirs
            grow[one, :] = grow[one, :] * growth_of(partner, states * size, kind, h, heads)

    for step in range(steps):
        side = lax.bitwise_and(lax.shift_right_logical(sp, step), 1)
        states = 1 if step == steps - 1 and steps > 1 else 2
        partner = partners[step]
        back = size if states == 2 else 0
        pl.when(side == 1)(functools.partial(take, start_f, grow_f, partner, 0, 0, states))
        pl.when(side == 0)(functools.partial(take, start_b, grow_b, partner, back, 1, states))

    states = 1 if steps > 1 else 2
    lift = growth_rows(heads)
    base = states * size + lift
    rows_each = ctx << (steps - 1)

    def context(low, up):
        def part(ref, section):
            return ref[base + section * rows_each : base + (section + 1) * rows_each, :]

        for h in range(heads):
            one = slice(h, h + 1)
            grow_up = growth_of(up, states * size, 2, h, heads)
            grow_low = growth_of(low, states * size, 3, h, heads)
            kf = [(part(low, h).astype(f32) * grow_up).astype(bf16), part(up, h)]
            kb = [part(low, heads + h), (part(up, heads + h).astype(f32) * grow_low).astype(bf16)]
            first = 2 * heads + h * (wide // DK)
            for c in range(wide // DK):
                vs = jnp.concatenate([part(low, first + c), part(up, first + c)], axis=0)
                at = slice(h * wide + c * DK, h * wide + (c + 1) * DK)
                start_f[at, :] += grow_f[one, :] * matmul(vs, jnp.concatenate(kf, axis=0), TN)
                start_b[at, :] += grow_b[one, :] * matmul(vs, jnp.concatenate(kb, axis=0), TN)

    side = lax.bitwise_and(lax.shift_right_logical(sp, steps - 1), 1)
    pl.when(side == 0)(lambda: context(own, partners[-1]))
    pl.when(side == 1)(lambda: context(partners[-1], own))
    width = gates.shape[1]
    last = own.shape[0] - gate_rows_of(width)
    gates[...] = joined_row(own[last:, :], width) + joined_row(partners[-1][last:, :], width)
    i = lax.broadcasted_iota(jnp.int32, (DK, DK), 0)
    j = lax.broadcasted_iota(jnp.int32, (DK, DK), 1)
    shift = VGROUP.bit_length() - 1
    alike = lax.shift_right_logical(i, shift) == lax.shift_right_logical(j, shift)
    averaging = jnp.where(alike, 1.0 / VGROUP, 0.0).astype(bf16)
    for h in range(heads):
        own_rows = slice(h * wide, (h + 1) * wide)
        lanes = slice(h * DK, (h + 1) * DK)
        result = (
            inside[:, own_rows]
            + matmul(reach_f[:, lanes], start_f[own_rows, :].astype(bf16), NT)
            + matmul(reach_b[:, lanes], start_b[own_rows, :].astype(bf16), NT)
        )
        for c in range(wide // DK):
            x = result[:, c * DK : (c + 1) * DK]
            high, low = halves(x * x)
            power = matmul(high, averaging) + matmul(low, averaging)
            at = slice(h * wide + c * DK, h * wide + (c + 1) * DK)
            out[:, at] = (x * lax.rsqrt(power + epsilon) * gated[:, at]).astype(bf16)


def branch_of(order, pieces, weight):
    width = pieces[0].shape[1]
    branch = None
    for k, piece in zip(order, pieces):
        column = pl.multiple_of(lax.bitwise_xor(lax.axis_index("tp"), k) * width, width)
        part = matmul(piece[...], weight[:, pl.ds(column, width)], NT)
        branch = part if branch is None else branch + part
    return branch


def early_kernel(order, *refs):
    weight, out = refs[-2:]
    out[...] = branch_of(order, refs[:-2], weight)


def output_kernel(order, *refs):
    weight, early, latent, gates, out = refs[-5:]
    branch = early[...] + branch_of(order, refs[:-5], weight)
    out[...] = (latent[...].astype(f32) + gates[...] * branch).astype(bf16)


def local_direct(*args):
    return direct_plan(*args)


def direct_plan(
    latent,
    context,
    conditioning,
    context_prompt_vector,
    shift_matrix,
    scale_matrix,
    residual_gate_matrix,
    query_matrix,
    key_matrix,
    value_matrix,
    gate_matrix,
    decay_down_factor,
    decay_up_factor,
    decay_key_bias,
    spike_log_decay,
    output_gain,
    output_matrix,
):
    tp_count, sp_count = (lax.axis_size("tp"), lax.axis_size("sp"))
    heads = HEADS // tp_count
    tokens, width = latent.shape
    ctx = context.shape[0]
    total = tokens + ctx
    features = width * tp_count
    steps = sp_count.bit_length() - 1
    shape = jax.ShapeDtypeStruct

    inner = conditioning.shape[0]
    rows_in = (inner // 128, 128)
    mod, joined = call(
        modulation_kernel,
        [shape((8, width), f32), shape((total, width), bf16)],
        [HBM_SPEC] * 6,
        (
            conditioning.reshape(rows_in),
            context_prompt_vector.reshape(rows_in),
            shift_matrix,
            scale_matrix,
            latent,
            context,
        ),
        4 * 8 * width * inner,
        4 * width * inner,
        [pltpu.VMEM(rows_in, bf16)] * 2
        + [pltpu.VMEM(shift_matrix.shape, bf16)] * 2
        + [pltpu.SemaphoreType.DMA((6,))],
        WIDE_GRANT,
    )
    gate_part = call(
        gating_kernel,
        shape((gate_rows_of(width), DK), bf16),
        [VMEM_SPEC] * 2,
        (conditioning.reshape(rows_in), residual_gate_matrix),
        16 * width * inner,
        2 * width * inner,
    )
    pieces = gathered_pieces(joined, "tp", "lat")
    for bit in range(steps):
        theirs = exchange(mod, "sp", 1 << bit)
        rows = [8] if bit < steps - 1 else [4]
        sums = call(
            add_kernel,
            [shape((r, width), f32) for r in rows],
            [VMEM_SPEC] * 2,
            (mod, theirs),
            8 * width,
            64 * width,
        )
        mod = sums[0]
    mods = [mod]
    for distance in mod_steps(tp_count):
        joint = mods[0]
        if len(mods) > 1:
            joint = call(
                join_kernel,
                shape((2 * mods[-1].shape[0], width), f32),
                [VMEM_SPEC] * len(mods),
                mods,
                8 * width,
                64 * width,
            )
        mods = mods + [exchange(joint, "tp", distance)]

    half = heads * DK
    down = jnp.transpose(decay_down_factor, (0, 2, 1)).reshape(2 * DECAY_RANK, features)
    vdim = value_matrix.shape[0]
    lift = growth_rows(heads)
    surveyed = sorted({k for k, _ in gather_plan(tp_count, "lat")} & {1, 2, 3})
    streamed = (key_matrix, value_matrix, down)
    staged = call(
        stage_kernel,
        shape((half + vdim + 2 * DECAY_RANK, features), bf16),
        [HBM_SPEC] * 3,
        streamed,
        0,
        4 * features * (half + vdim),
        [pltpu.SemaphoreType.DMA((3,))],
        STAGE_GRANT,
    )
    early = call(
        survey_kernel,
        [shape((total, 128), f32)] * 2,
        [VMEM_SPEC] * len(surveyed),
        [pieces[k] for k in surveyed],
        SURVEY_FLOPS,
        SURVEY_BYTES,
    )
    normed, keys, values, cum_f, cum_b, payload = call(
        functools.partial(project_kernel, tp_count, tokens, heads, surveyed),
        [
            shape((total, features), bf16),
            shape((tokens, half), bf16),
            shape((tokens, vdim), bf16),
            shape((tokens, half), f32),
            shape((tokens, half), f32),
            shape((2 * vdim + lift + 4 * heads * ctx + gate_rows_of(width), DK), bf16),
        ],
        [VMEM_SPEC] * (tp_count + len(mods) + 5) + [HBM_SPEC] * 2,
        (
            *pieces,
            *mods,
            staged,
            *early,
            jnp.transpose(spike_log_decay, (0, 2, 1)),
            gate_part,
            decay_up_factor,
            decay_key_bias,
        ),
        2 * total * features * (half + vdim),
        2 * features * (half + vdim),
        [
            pltpu.VMEM((2, DECAY_RANK, half), bf16),
            pltpu.VMEM((2, half), f32),
            pltpu.SemaphoreType.DMA((2,)),
        ],
    )
    partners = [exchange(payload, "sp", 1)]
    rows = ctx
    for bit in range(steps - 1):
        final = bit == steps - 2
        states = 1 if final else 2
        payload = call(
            functools.partial(merge_kernel, bit, final, heads, rows, width),
            shape((states * vdim + lift + 8 * heads * rows + gate_rows_of(width), DK), bf16),
            [VMEM_SPEC, VMEM_SPEC],
            (payload, partners[-1]),
            4 * vdim * DK,
            8 * vdim * DK,
        )
        rows = 2 * rows
        partners.append(exchange(payload, "sp", 2 << bit))
    inside, reach_f, reach_b, gated = call(
        functools.partial(within_kernel, heads),
        [
            shape((tokens, vdim), f32),
            shape((tokens, half), bf16),
            shape((tokens, half), bf16),
            shape((tokens, vdim), f32),
        ],
        [VMEM_SPEC] * 8,
        (
            normed,
            query_matrix,
            gate_matrix,
            keys,
            values,
            cum_f,
            cum_b,
            output_gain[None],
        ),
        2 * tokens * features * (half + vdim),
        2 * features * (half + vdim),
    )
    heads_out, gates = call(
        functools.partial(finish_kernel, steps, heads, ctx),
        [shape((tokens, vdim), bf16), shape((1, width), f32)],
        [VMEM_SPEC] * (5 + steps),
        (payload, *partners, inside, reach_f, reach_b, gated),
        8 * tokens * vdim * DK,
        8 * tokens * vdim,
        [
            pltpu.VMEM((vdim, DK), f32),
            pltpu.VMEM((vdim, DK), f32),
            pltpu.VMEM((8 * -(-heads // 8), DK), f32),
            pltpu.VMEM((8 * -(-heads // 8), DK), f32),
        ],
    )
    branches = gathered_pieces(heads_out, "tp", "out")
    late = [k for k in range(1, tp_count) if k >= tp_count - 3]
    soon = [k for k in range(tp_count) if k not in late]
    cost = 2 * width * vdim
    early = call(
        functools.partial(early_kernel, soon),
        shape((tokens, width), f32),
        [VMEM_SPEC] * (len(soon) + 1),
        (*(branches[k] for k in soon), output_matrix),
        tokens * cost * len(soon),
        cost * len(soon),
    )
    return call(
        functools.partial(output_kernel, late),
        shape((tokens, width), bf16),
        [VMEM_SPEC] * (len(late) + 4),
        (*(branches[k] for k in late), output_matrix, early, latent, gates),
        tokens * cost * len(late),
        cost * len(late),
    )


def solution(mesh):
    placed = (
        P("sp", "tp"),
        P("sp", "tp"),
        P("sp"),
        P("sp"),
        P("tp", "sp"),
        P("tp", "sp"),
        P("tp", "sp"),
        P("tp", None),
        P("tp", None),
        P("tp", None),
        P("tp", None),
        P(),
        P(),
        P(),
        P(None, "sp", None),
        P("tp"),
        P("tp", None),
    )
    tp_count, sp_count = (mesh.shape["tp"], mesh.shape["sp"])
    powers = tp_count & tp_count - 1 == 0 and sp_count & sp_count - 1 == 0
    direct = 2 <= tp_count <= HEADS and sp_count >= 2 and powers
    return jax.shard_map(
        local_direct if direct else local_general, mesh=mesh, in_specs=placed, out_specs=P("sp", "tp"), check_vma=False
    )
```

```python
import functools

import jax
import jax.numpy as jnp
from jax import lax
from jax.experimental import pallas as pl
from jax.experimental.pallas import tpu as pltpu
from jax.sharding import PartitionSpec as P


D = 4096
HEADS = 16
DK = 128
DECAY_RANK = 16
BLK = 64
VGROUP = 64


epsilon = 1e-05
gate_norm = 16.0
precise = lax.Precision.HIGHEST


def for_sending(value):

    def short(part):
        return part.astype(jnp.bfloat16) if part.dtype == jnp.float32 else part

    return jax.tree.map(short, value)


def from_partner(value, axis, distance):
    return lax.ppermute(value, axis, [(i, i ^ 1 << distance) for i in range(lax.axis_size(axis))])


def carried_in(value, axis, combine, identity, reverse):
    peers, index = (lax.axis_size(axis), lax.axis_index(axis))
    everything = jax.tree.map(
        lambda part, kind: lax.all_gather(part.astype(kind), axis),
        value,
        (jnp.bfloat16, jnp.bfloat16),
    )
    start = jax.tree.map(
        lambda part, zero: jnp.broadcast_to(jnp.asarray(zero, part.dtype), part.shape),
        value,
        identity,
    )

    def turn(k, before):
        at = peers - 1 - k if reverse else k
        reached = at > index if reverse else at < index
        new = combine(
            before, jax.tree.map(lambda part, own: part[at].astype(own.dtype), everything, value)
        )
        return jax.tree.map(lambda a, b: jnp.where(reached, a, b), new, before)

    return lax.fori_loop(0, peers, turn, start)


def linear(rows, weight):
    return lax.dot_general(
        rows, weight, (((1,), (1,)), ((), ())), preferred_element_type=jnp.float32
    )


def modulated(rows, row_sum, row_squares, shift_vec, scale_vec):
    rows_f = rows.astype(jnp.float32)
    mean_val = row_sum / D
    variance = row_squares / D - mean_val * mean_val
    return (
        (rows_f - mean_val) * lax.rsqrt(variance + epsilon) * (1.0 + scale_vec) + shift_vec
    ).astype(jnp.bfloat16)


def reverse_rows(array):
    return jnp.flip(array, axis=0)


def end_state(key_rows, value_rows, log_decay):
    cumulative = jnp.cumsum(log_decay, axis=0)
    totals = cumulative[-1]
    weighted = key_rows * jnp.exp(totals - cumulative)
    return (jnp.exp(totals), jnp.einsum("nhd,nhe->hde", weighted, value_rows, precision=precise))


def combine(earlier, later):
    return (earlier[0] * later[0], later[0][..., None] * earlier[1] + later[1])


def blockwise(queries, key_rows, value_rows, log_decay, carried, block_len):
    length, head_count, _ = queries.shape
    value_width = value_rows.shape[-1]
    blocks = length // block_len

    def shaped(array):
        return array.reshape(blocks, block_len, head_count, array.shape[-1])

    triangle = jnp.tril(jnp.ones((block_len, block_len), jnp.float32))

    def advance(state_now, inputs):
        block_q, block_k, block_v, block_a = inputs
        cumulative = jnp.cumsum(block_a, axis=0)
        block_end = cumulative[-1]
        query_dec = block_q * jnp.exp(cumulative)
        scores = (
            jnp.einsum("ihd,jhd->hij", query_dec, block_k * jnp.exp(-cumulative), precision=precise)
            * triangle
        )
        result = jnp.einsum("hij,jhe->ihe", scores, block_v, precision=precise)
        result = result + jnp.einsum("ihd,hde->ihe", query_dec, state_now, precision=precise)
        state_next = state_now * jnp.exp(block_end)[:, :, None] + jnp.einsum(
            "jhd,jhe->hde", block_k * jnp.exp(block_end - cumulative), block_v, precision=precise
        )
        return (state_next, result)

    _, outputs = lax.scan(
        advance, carried, (shaped(queries), shaped(key_rows), shaped(value_rows), shaped(log_decay))
    )
    return outputs.reshape(length, head_count, value_width)


def head_channels(pieces, per_head, tp_index):
    for bit_number in range(per_head.bit_length() - 1):
        partner = from_partner(
            (for_sending(pieces[0]), for_sending(pieces[1]), for_sending(pieces[2])),
            "tp",
            bit_number,
        )
        upper = tp_index // (1 << bit_number) % 2 == 1
        pieces = tuple(
            (
                jnp.where(
                    upper,
                    jnp.concatenate([theirs, mine], axis=1),
                    jnp.concatenate([mine, theirs], axis=1),
                )
                for mine, theirs in zip(pieces, partner)
            )
        )
    return pieces


def context_totals(fwd_growth, fwd_state, bwd_growth, bwd_state, identity):

    def absorb(carried, piece):
        return (combine(carried, piece), None)

    total_fwd, _ = lax.scan(absorb, identity, (fwd_growth, fwd_state))
    total_bwd, _ = lax.scan(absorb, identity, (bwd_growth, bwd_state), reverse=True)
    return (total_fwd, total_bwd)


def stored(array):
    return lax.optimization_barrier(array.astype(jnp.bfloat16))


def local_general(
    latent,
    context,
    conditioning,
    context_prompt_vector,
    shift_matrix,
    scale_matrix,
    residual_gate_matrix,
    query_matrix,
    key_matrix,
    value_matrix,
    gate_matrix,
    decay_down_factor,
    decay_up_factor,
    decay_key_bias,
    spike_log_decay,
    output_gain,
    output_matrix,
):
    tp_count = lax.axis_size("tp")
    tp_index = lax.axis_index("tp")
    per_head = max(tp_count // HEADS, 1)
    heads_per_shard = max(HEADS // tp_count, 1)
    leading_head = tp_index // per_head * heads_per_shard
    tok_rows = latent.shape[0]
    conds = jax.nn.silu(
        jnp.stack([conditioning, context_prompt_vector]).astype(jnp.float32)
    ).astype(jnp.bfloat16)
    shifts, scales, gates = lax.psum(
        (
            linear(conds, shift_matrix),
            linear(conds, scale_matrix),
            linear(conds, residual_gate_matrix),
        ),
        "sp",
    )
    down_both = jnp.concatenate([decay_down_factor[0].T, decay_down_factor[1].T], axis=0)
    lat_weights = (query_matrix, key_matrix, value_matrix, gate_matrix, down_both)
    ctx_weights = (key_matrix, value_matrix, down_both)
    lat_f = latent.astype(jnp.float32)
    ctx_f = context.astype(jnp.float32)
    lat_sum, lat_squares, ctx_sum, ctx_squares = lax.psum(
        (
            jnp.sum(lat_f, axis=1, keepdims=True),
            jnp.sum(lat_f * lat_f, axis=1, keepdims=True),
            jnp.sum(ctx_f, axis=1, keepdims=True),
            jnp.sum(ctx_f * ctx_f, axis=1, keepdims=True),
        ),
        "tp",
    )
    latent_normalized = modulated(latent, lat_sum, lat_squares, shifts[0], scales[0])
    normed_ctx = modulated(context, ctx_sum, ctx_squares, shifts[1], scales[1])
    lat_piece = lax.all_gather(latent_normalized, "tp", axis=1, tiled=True)
    ctx_piece = lax.all_gather(normed_ctx, "tp", axis=1, tiled=True)
    lat_new = tuple((linear(lat_piece, weight) for weight in lat_weights))
    ctx_new = tuple((linear(ctx_piece, weight) for weight in ctx_weights))
    query_part, key_part, value_part, gate_part, low_rank_part = lat_new
    ctx_key_part, ctx_value_part, ctx_low = ctx_new
    query_full, key_full, ctx_key_full = head_channels(
        (stored(query_part), stored(key_part), stored(ctx_key_part)), per_head, tp_index
    )

    def split_heads(rows, width):
        return rows.astype(jnp.float32).reshape(rows.shape[0], heads_per_shard, width)

    value_cols = value_part.shape[1] // heads_per_shard
    queries = split_heads(query_full, DK) * DK ** (-0.5)
    key_rows = split_heads(key_full, DK)
    ctx_keys = split_heads(ctx_key_full, DK)
    values_lat = split_heads(stored(value_part), value_cols)
    values_ctx = split_heads(stored(ctx_value_part), value_cols)
    gate_rows = stored(gate_part).astype(jnp.float32)

    def per_head_decay(low_rows, direction):
        up_part = lax.dynamic_slice_in_dim(
            decay_up_factor[direction], leading_head * DK, heads_per_shard * DK, 1
        ).astype(jnp.float32)
        bias_part = lax.dynamic_slice_in_dim(
            decay_key_bias[direction], leading_head * DK, heads_per_shard * DK, 0
        )
        pre_act = jnp.dot(low_rows, up_part, precision=precise) + bias_part
        return (jax.nn.log_sigmoid(pre_act) / gate_norm).reshape(
            low_rows.shape[0], heads_per_shard, DK
        )

    decay_spikes = lax.dynamic_slice_in_dim(spike_log_decay, leading_head, heads_per_shard, 2)
    latent_forward = per_head_decay(low_rank_part[:, :DECAY_RANK], 0) + decay_spikes[0][:, :, None]
    latent_backward = per_head_decay(low_rank_part[:, DECAY_RANK:], 1) + decay_spikes[1][:, :, None]
    ctx_fwd = per_head_decay(ctx_low[:, :DECAY_RANK], 0)
    ctx_bwd = per_head_decay(ctx_low[:, DECAY_RANK:], 1)
    cf_growth, cf_state = end_state(ctx_keys, values_ctx, ctx_fwd)
    cb_growth, cb_state = end_state(
        reverse_rows(ctx_keys), reverse_rows(values_ctx), reverse_rows(ctx_bwd)
    )
    lf_growth, lf_state = end_state(key_rows, values_lat, latent_forward)
    lb_growth, lb_state = end_state(
        reverse_rows(key_rows), reverse_rows(values_lat), reverse_rows(latent_backward)
    )
    identity = (
        jnp.ones((heads_per_shard, DK), jnp.float32),
        jnp.zeros((heads_per_shard, DK, value_cols), jnp.float32),
    )
    ctx_gathered = (
        lax.all_gather(cf_growth[None].astype(jnp.bfloat16), "sp", axis=0, tiled=True).astype(
            jnp.float32
        ),
        lax.all_gather(cf_state[None].astype(jnp.bfloat16), "sp", axis=0, tiled=True).astype(
            jnp.float32
        ),
        lax.all_gather(cb_growth[None].astype(jnp.bfloat16), "sp", axis=0, tiled=True).astype(
            jnp.float32
        ),
        lax.all_gather(cb_state[None].astype(jnp.bfloat16), "sp", axis=0, tiled=True).astype(
            jnp.float32
        ),
    )
    total_fwd, total_bwd = context_totals(
        ctx_gathered[0], ctx_gathered[1], ctx_gathered[2], ctx_gathered[3], identity
    )
    prefix = carried_in((lf_growth, lf_state), "sp", combine, identity, False)
    suffix = carried_in((lb_growth, lb_state), "sp", combine, identity, True)
    start_fwd = combine(total_fwd, prefix)[1]
    start_bwd = combine(total_bwd, suffix)[1]
    zero_state = jnp.zeros((heads_per_shard, DK, value_cols), jnp.float32)

    def direction_out(query_rows, key_list, value_list, log_decay, start_state):
        local_part = blockwise(query_rows, key_list, value_list, log_decay, zero_state, BLK)
        reach = query_rows * jnp.exp(jnp.cumsum(log_decay, axis=0))
        return local_part + jnp.einsum("nhd,hde->nhe", reach, start_state, precision=precise)

    out_fwd = direction_out(queries, key_rows, values_lat, latent_forward, start_fwd)
    out_bwd = reverse_rows(
        direction_out(
            reverse_rows(queries),
            reverse_rows(key_rows),
            reverse_rows(values_lat),
            reverse_rows(latent_backward),
            start_bwd,
        )
    )
    grouped = (out_fwd + out_bwd).reshape(tok_rows, -1, VGROUP)
    grouped = grouped * lax.rsqrt(jnp.mean(grouped * grouped, axis=-1, keepdims=True) + epsilon)
    heads_out = (grouped.reshape(tok_rows, -1) * output_gain * jax.nn.silu(gate_rows)).astype(
        jnp.bfloat16
    )
    branch = linear(lax.all_gather(heads_out, "tp", axis=1, tiled=True), output_matrix)
    return (latent.astype(jnp.float32) + gates[0] * branch).astype(jnp.bfloat16)


VMEM_SPEC = pl.BlockSpec(memory_space=pltpu.VMEM)
HBM_SPEC = pl.BlockSpec(memory_space=pltpu.HBM)
NT = (((1,), (1,)), ((), ()))
NN = (((1,), (0,)), ((), ()))
TN = (((0,), (0,)), ((), ()))
f32 = jnp.float32
bf16 = jnp.bfloat16


def matmul(a, b, dims=NN):
    return lax.dot_general(a, b, dims, preferred_element_type=f32)


def halves(value):
    high = value.astype(bf16)
    return (high, (value - high.astype(f32)).astype(bf16))


def exchange(value, axis, distance):
    return lax.ppermute(value, axis, [(i, i ^ distance) for i in range(lax.axis_size(axis))])


def gather_plan(count, label):
    if count == 8:
        return PLANS[label]
    half = count // 2
    direct = dict.fromkeys(k for k in (half, 2, 1, count - 1) if k < count)
    plan = [(k, 0) for k in direct]
    for k in range(3, count):
        if k not in direct:
            plan.append((k, half if k & half else 2 if k == 3 else 0))
    return plan


def gathered_pieces(value, axis, label):
    pieces = {0: value}
    for k, source in gather_plan(lax.axis_size(axis), label):
        pieces[k] = exchange(pieces[source], axis, k ^ source)
    return [pieces[k] for k in sorted(pieces)]


def mod_steps(count):
    return MOD_STEPS if count == 8 else tuple(1 << bit for bit in range(count.bit_length() - 1))


WIDE_GRANT = 60000
STAGE_GRANT = 2 << 10
SURVEY_FLOPS = 15 * 10**9
SURVEY_BYTES = 40 * 10**6
MOD_STEPS = (1, 2, 4)
PLANS = {
    "lat": ((4, 0), (2, 0), (1, 0), (7, 0), (3, 2), (5, 4), (6, 4)),
    "out": ((2, 0), (4, 0), (1, 0), (3, 2), (7, 0), (5, 4), (6, 4)),
}


def call(kernel, out_shapes, in_specs, args, flops, traffic, scratch=(), grant=24 << 10):
    single = not isinstance(out_shapes, (tuple, list))
    return pl.pallas_call(
        kernel,
        out_shape=out_shapes,
        in_specs=in_specs,
        out_specs=VMEM_SPEC if single else [VMEM_SPEC] * len(out_shapes),
        scratch_shapes=list(scratch),
        compiler_params=pltpu.CompilerParams(vmem_limit_bytes=grant << 10),
        cost_estimate=pl.CostEstimate(flops=flops, bytes_accessed=traffic, transcendentals=0),
    )(*args)


def fetch(sources, targets, sems):
    copies = [
        pltpu.make_async_copy(source, target, sems.at[n])
        for n, (source, target) in enumerate(zip(sources, targets))
    ]
    for copy in copies:
        copy.start()
    return copies


def in_one_row(ref):
    block = ref[...].astype(f32)
    return jnp.concatenate([block[r : r + 1] for r in range(block.shape[0])], axis=1)


def modulation_kernel(*refs):
    sources = refs[:6]
    out, joined = refs[6:8]
    cond_ref, prompt_ref, *weights = refs[8:12]
    tokens = sources[4].shape[0]
    rows = (joined.at[pl.ds(0, tokens)], joined.at[pl.ds(tokens, sources[5].shape[0])])
    copies = fetch(sources, (cond_ref, prompt_ref, *weights, *rows), refs[12])
    copies[0].wait()
    cond = in_one_row(cond_ref)
    copies[1].wait()
    row = lax.broadcasted_iota(jnp.int32, (8, cond.shape[1]), 0)
    both = jnp.where(row % 2 == 0, cond, in_one_row(prompt_ref))
    conds = (both * jax.nn.sigmoid(both)).astype(bf16)
    row_out = lax.broadcasted_iota(jnp.int32, out.shape, 0)
    copies[2].wait()
    shifts = matmul(conds, weights[0][...], NT)
    copies[3].wait()
    scales = matmul(conds, weights[1][...], NT)
    out[...] = jnp.where(row_out < 2, shifts, scales)
    copies[4].wait()
    copies[5].wait()


def gate_rows_of(width):
    return -(-2 * (width // DK) // 16) * 16


def split_row(value):
    count = value.shape[1] // DK
    rows = [value[:, c * DK : (c + 1) * DK] for c in range(count)]
    blank = jnp.zeros((gate_rows_of(value.shape[1]) - 2 * count, DK), bf16)
    parts = [halves(row) for row in rows]
    return jnp.concatenate([p[0] for p in parts] + [p[1] for p in parts] + [blank], axis=0)


def joined_row(block, width):
    count = width // DK
    value = block.astype(f32)
    value = value[:count] + value[count : 2 * count]
    return jnp.concatenate([value[c : c + 1] for c in range(count)], axis=1)


def gating_kernel(cond_ref, weight, out):
    cond = in_one_row(cond_ref)
    cond = jnp.broadcast_to(cond, (8, cond.shape[1]))
    conds = (cond * jax.nn.sigmoid(cond)).astype(bf16)
    out[...] = split_row(matmul(conds, weight[...], NT)[:1])


def row_sums(pieces):
    total, width = pieces[0].shape
    sums = jnp.zeros((total, 128), f32)
    squares = jnp.zeros((total, 128), f32)
    for piece in pieces:
        for c in range(width // 128):
            x = piece[:, c * 128 : (c + 1) * 128].astype(f32)
            sums = sums + x
            squares = squares + x * x
    return (sums, squares)


def add_kernel(mine, theirs, *outs):
    total = mine[...] + theirs[...]
    for out in outs:
        out[...] = total[: out.shape[0]]


def join_kernel(*refs):
    at = 0
    for ref in refs[:-1]:
        refs[-1][at : at + ref.shape[0], :] = ref[...]
        at += ref.shape[0]


def stage_kernel(*refs):
    sources = refs[:-2]
    targets, at = ([], 0)
    for source in sources:
        targets.append(refs[-2].at[pl.ds(at, source.shape[0])])
        at += source.shape[0]
    for copy in fetch(sources, targets, refs[-1]):
        copy.wait()


def survey_kernel(*refs):
    refs[-2][...], refs[-1][...] = row_sums(refs[:-2])


def block_masks(total, tokens, wanted):
    i = lax.broadcasted_iota(jnp.int32, (total, total), 0)
    j = lax.broadcasted_iota(jnp.int32, (total, total), 1)
    last = tokens // BLK
    bi = jnp.minimum(lax.shift_right_logical(i, BLK.bit_length() - 1), last)
    bj = jnp.minimum(lax.shift_right_logical(j, BLK.bit_length() - 1), last)
    return wanted(i, j, bi, bj)


def project_kernel(count, tokens, heads, surveyed, *refs):
    pieces = refs[:count]
    mods = refs[count : count + count.bit_length()]
    refs = refs[count + count.bit_length() :]
    weights, early_sums, early_squares, spikes, gate_part = refs[:5]
    normed, keys, values, cum_f, cum_b, payload, extra = refs[7:14]
    up_own, bias_own, sems = refs[14:]
    tp = lax.axis_index("tp")
    half = heads * DK
    first = pl.multiple_of(tp * half, half)
    sources = (refs[5].at[:, :, pl.ds(first, half)], refs[6].at[:, pl.ds(first, half)])
    copies = fetch(sources, (up_own, bias_own), sems)
    total, width = pieces[0].shape
    ctx = total - tokens
    features = width * count

    held = [[0]]
    for distance in mod_steps(count):
        held.append([k ^ distance for k in sum(held, [])])
    found = {k: (level, at) for level, ks in enumerate(held) for at, k in enumerate(ks)}

    def mod_row(k, row):
        level, at = found[k]
        return mods[level][4 * at + row : 4 * at + row + 1, :]

    sums, squares = row_sums([pieces[k] for k in range(count) if k not in surveyed])
    sums, squares = (sums + early_sums[...], squares + early_squares[...])
    mean = jnp.sum(sums, axis=1, keepdims=True) / features
    variance = jnp.sum(squares, axis=1, keepdims=True) / features - mean * mean
    inverse = lax.rsqrt(variance + epsilon)
    for k, piece in enumerate(pieces):
        column = pl.multiple_of(lax.bitwise_xor(tp, k) * width, width)
        scaled = (piece[...].astype(f32) - mean) * inverse
        ahead = scaled[:tokens] * (1.0 + mod_row(k, 2)) + mod_row(k, 0)
        context = scaled[tokens:] * (1.0 + mod_row(k, 3)) + mod_row(k, 1)
        normed[:tokens, pl.ds(column, width)] = ahead.astype(bf16)
        normed[tokens:, pl.ds(column, width)] = context.astype(bf16)
    products = matmul(weights[...], normed[...], NT).T
    key_all = products[:, :half].astype(bf16)
    value_all = products[:, half : half + values.shape[1]].astype(bf16)
    low_high, low_low = halves(products[:, half + values.shape[1] :])
    for copy in copies:
        copy.wait()
    blank = jnp.zeros((DECAY_RANK, half), bf16)
    up = jnp.concatenate(
        [
            jnp.concatenate([up_own[0], blank], axis=1),
            jnp.concatenate([blank, up_own[1]], axis=1),
        ],
        axis=0,
    )
    bias = jnp.concatenate([bias_own[0:1, :], bias_own[1:2, :]], axis=1)
    pre = matmul(low_high, up) + matmul(low_low, up) + bias
    decay = (jnp.minimum(pre, 0.0) - jnp.log1p(jnp.exp(-jnp.abs(pre)))) * (1.0 / gate_norm)
    row = lax.broadcasted_iota(jnp.int32, (spikes.shape[1], half), 0)
    head = lax.shift_right_logical(
        lax.broadcasted_iota(jnp.int32, (spikes.shape[1], half), 1), DK.bit_length() - 1
    )
    wanted = jnp.where(row == head + tp * heads, 1.0, 0.0).astype(bf16)
    marks = []
    for d in range(2):
        spike_high, spike_low = halves(spikes[d])
        added = matmul(spike_high, wanted, TN) + matmul(spike_low, wanted, TN)
        marks.append(decay[:tokens, d * half : (d + 1) * half] + added)
    decay = jnp.concatenate([jnp.concatenate(marks, axis=1), decay[tokens:]], axis=0)
    ones = jnp.ones((total, total), f32)
    zeros = jnp.zeros((total, total), f32)
    lower = block_masks(
        total, tokens, lambda i, j, bi, bj: jnp.where((bi == bj) & (i >= j), ones, zeros)
    ).astype(bf16)
    upper = block_masks(
        total, tokens, lambda i, j, bi, bj: jnp.where((bi == bj) & (i <= j), ones, zeros)
    ).astype(bf16)
    high, low = halves(decay)
    cf = matmul(lower, high[:, :half]) + matmul(lower, low[:, :half])
    cb = matmul(upper, high[:, half:]) + matmul(upper, low[:, half:])
    cum_f[...] = cf[:tokens]
    cum_b[...] = cb[:tokens]
    keys[...] = key_all[:tokens]
    values[...] = value_all[:tokens]
    wide = value_all.shape[1] // heads
    blocks = tokens // BLK
    size = heads * wide
    growth = [[], [], [], []]
    start = 2 * size + growth_rows(heads)
    for h in range(heads):
        own = slice(h * DK, (h + 1) * DK)
        kh = key_all[:, own].astype(f32)
        vh = value_all[:tokens, h * wide : (h + 1) * wide]
        cfh, cbh = (cf[:, own], cb[:, own])
        ends_f = [cfh[(b + 1) * BLK - 1 : (b + 1) * BLK] for b in range(blocks)]
        ends_b = [cbh[b * BLK : b * BLK + 1] for b in range(blocks)]
        weighted_f, weighted_b = ([], [])
        for b in range(blocks):
            rows = slice(b * BLK, (b + 1) * BLK)
            weighted_f.append(kh[rows] * jnp.exp(sum(ends_f[b + 1 :], ends_f[b]) - cfh[rows]))
            weighted_b.append(kh[rows] * jnp.exp(sum(ends_b[:b], ends_b[b]) - cbh[rows]))
        kf = jnp.concatenate(weighted_f, axis=0).astype(bf16)
        kb = jnp.concatenate(weighted_b, axis=0).astype(bf16)
        payload[h * wide : (h + 1) * wide, :] = matmul(vh, kf, TN).astype(bf16)
        payload[size + h * wide : size + (h + 1) * wide, :] = matmul(vh, kb, TN).astype(bf16)
        growth[0].append(jnp.exp(sum(ends_f[1:], ends_f[0])))
        growth[1].append(jnp.exp(sum(ends_b[1:], ends_b[0])))
        end_f, end_b = (cfh[total - 1 : total], cbh[tokens : tokens + 1])
        growth[2].append(jnp.exp(end_f))
        growth[3].append(jnp.exp(end_b))
        at = start + h * ctx
        payload[at : at + ctx, :] = (kh[tokens:] * jnp.exp(end_f - cfh[tokens:])).astype(bf16)
        at = at + heads * ctx
        payload[at : at + ctx, :] = (kh[tokens:] * jnp.exp(end_b - cbh[tokens:])).astype(bf16)
    for c in range(size // DK):
        at = start + (2 * heads + c) * ctx
        payload[at : at + ctx, :] = value_all[tokens:, c * DK : (c + 1) * DK]
    payload[2 * size : start, :] = growth_block(growth, heads)
    payload[start + 4 * heads * ctx :, :] = gate_part[...]
    extra[...] = payload[2 * size :, :]


def growth_rows(heads):
    return -(-4 * heads // 16) * 16


def growth_block(growth, heads):
    rows = [row for kind in growth for row in kind]
    blank = jnp.zeros((growth_rows(heads) - len(rows), DK), f32)
    return jnp.concatenate([*rows, blank], axis=0).astype(bf16)


def growth_of(ref, at, kind, h, heads):
    block = ref[at : at + growth_rows(heads), :].astype(f32)
    return block[kind * heads + h : kind * heads + h + 1]


def gated_kernel(normed, gate_w, gain, gated):
    products = matmul(gate_w[...], normed[: gated.shape[0], :], NT).T
    gates = products.astype(bf16).astype(f32)
    gated[...] = gates * jax.nn.sigmoid(gates) * gain[...]


def within_kernel(heads, normed, query_w, keys, values, cum_f, cum_b, inside, reach_f, reach_b):
    tokens = keys.shape[0]
    rows_in = normed[:tokens, :]
    query_all = matmul(rows_in, query_w[...], NT).astype(bf16).astype(f32) * DK ** (-0.5)
    wide = values.shape[1] // heads
    blocks = tokens // BLK

    def choose(i, j, bi, bj):
        same = bi == bj
        return (same & (i >= j), same & (i <= j), bi > bj, bi < bj)

    forward, backward, later, sooner = block_masks(tokens, tokens, choose)
    for h in range(heads):
        own = slice(h * DK, (h + 1) * DK)
        qh = query_all[:, own]
        kh = keys[:, own].astype(f32)
        cf, cb = (cum_f[:, own], cum_b[:, own])
        ends_f = [cf[(b + 1) * BLK - 1 : (b + 1) * BLK] for b in range(blocks)]
        ends_b = [cb[b * BLK : b * BLK + 1] for b in range(blocks)]
        spread = (BLK, DK)
        end_f = jnp.concatenate([jnp.broadcast_to(e, spread) for e in ends_f], axis=0)
        end_b = jnp.concatenate([jnp.broadcast_to(e, spread) for e in ends_b], axis=0)
        qf, qb = (qh * jnp.exp(cf), qh * jnp.exp(cb))
        qf_b, qb_b = (qf.astype(bf16), qb.astype(bf16))
        scores = (
            jnp.where(forward, matmul(qf_b, (kh * jnp.exp(-cf)).astype(bf16), NT), 0.0)
            + jnp.where(backward, matmul(qb_b, (kh * jnp.exp(-cb)).astype(bf16), NT), 0.0)
            + jnp.where(later, matmul(qf_b, (kh * jnp.exp(end_f - cf)).astype(bf16), NT), 0.0)
            + jnp.where(sooner, matmul(qb_b, (kh * jnp.exp(end_b - cb)).astype(bf16), NT), 0.0)
        )
        vh = values[:, h * wide : (h + 1) * wide]
        inside[:, h * wide : (h + 1) * wide] = matmul(scores.astype(bf16), vh)
        for b in range(blocks):
            rows = slice(b * BLK, (b + 1) * BLK)
            before = sum(ends_f[:b], jnp.zeros_like(ends_f[0]))
            after = sum(ends_b[b + 1 :], jnp.zeros_like(ends_b[0]))
            reach_f[rows, own] = (qf[rows] * jnp.exp(before)).astype(bf16)
            reach_b[rows, own] = (qb[rows] * jnp.exp(after)).astype(bf16)


def merge_kernel(heads, own, partner, out):
    lift = growth_rows(heads)
    size = out.shape[0] - lift
    wide = size // heads
    sp = lax.axis_index("sp")

    def emit(low, up):
        def forward():
            for h in range(heads):
                rows = slice(h * wide, (h + 1) * wide)
                decayed = growth_of(up, 2 * size, 0, h, heads) * low[rows, :].astype(f32)
                out[rows, :] = (decayed + up[rows, :].astype(f32)).astype(bf16)

        def backward():
            for h in range(heads):
                rows = slice(size + h * wide, size + (h + 1) * wide)
                decayed = growth_of(low, 2 * size, 1, h, heads) * up[rows, :].astype(f32)
                out[h * wide : (h + 1) * wide, :] = (
                    decayed + low[rows, :].astype(f32)
                ).astype(bf16)

        pl.when(sp < 2)(forward)
        pl.when(sp >= 2)(backward)
        rates = slice(2 * size, 2 * size + lift)
        out[size:, :] = (low[rates, :].astype(f32) * up[rates, :].astype(f32)).astype(bf16)

    pl.when(sp % 2 == 0)(lambda: emit(own, partner))
    pl.when(sp % 2 == 1)(lambda: emit(partner, own))


def finish_kernel(heads, ctx, *refs):
    own, partner, other, far, pair = refs[:5]
    inside, reach_f, reach_b, gated, out, gates = refs[5:11]
    start_f, start_b, grow_f, grow_b, shared = refs[11:]
    sp = lax.axis_index("sp")
    size = start_f.shape[0]
    wide = size // heads
    lift = growth_rows(heads)
    devices, rows_shared, _ = shared.shape
    start_f[...] = jnp.zeros(start_f.shape, f32)
    start_b[...] = jnp.zeros(start_b.shape, f32)
    grow_f[...] = jnp.ones(grow_f.shape, f32)
    grow_b[...] = jnp.ones(grow_b.shape, f32)

    def take(start, grow, source, at, kind, rates):
        for h in range(heads):
            rows = slice(h * wide, (h + 1) * wide)
            one = slice(h, h + 1)
            theirs = source[at + h * wide : at + (h + 1) * wide, :].astype(f32)
            start[rows, :] = start[rows, :] + grow[one, :] * theirs
            grow[one, :] = grow[one, :] * growth_of(source, rates, kind, h, heads)

    pl.when(sp % 2 == 1)(functools.partial(take, start_f, grow_f, partner, 0, 0, 2 * size))
    pl.when(sp % 2 == 0)(functools.partial(take, start_b, grow_b, partner, size, 1, 2 * size))
    pl.when(sp >= 2)(functools.partial(take, start_f, grow_f, pair, 0, 0, size))
    pl.when(sp < 2)(functools.partial(take, start_b, grow_b, pair, 0, 1, size))
    shared[sp] = own[:rows_shared, :]
    shared[lax.bitwise_xor(sp, 1)] = partner[2 * size : 2 * size + rows_shared, :]
    shared[lax.bitwise_xor(sp, 2)] = other[:rows_shared, :]
    shared[lax.bitwise_xor(sp, 3)] = far[:rows_shared, :]

    def part(d, section):
        return shared[d, lift + section * ctx : lift + (section + 1) * ctx, :]

    def rate(d, kind, h):
        return shared[d, :lift, :].astype(f32)[kind * heads + h : kind * heads + h + 1]

    def chained(order, kind, h, section):
        rows, running = ({}, None)
        for d in order:
            rows[d] = part(d, section)
            if running is not None:
                rows[d] = (rows[d].astype(f32) * running).astype(bf16)
            running = rate(d, kind, h) if running is None else running * rate(d, kind, h)
        return jnp.concatenate([rows[d] for d in range(devices)], axis=0)

    for h in range(heads):
        one = slice(h, h + 1)
        kf = chained(range(devices - 1, -1, -1), 2, h, h)
        kb = chained(range(devices), 3, h, heads + h)
        first = 2 * heads + h * (wide // DK)
        for c in range(wide // DK):
            vs = jnp.concatenate([part(d, first + c) for d in range(devices)], axis=0)
            at = slice(h * wide + c * DK, h * wide + (c + 1) * DK)
            start_f[at, :] += grow_f[one, :] * matmul(vs, kf, TN)
            start_b[at, :] += grow_b[one, :] * matmul(vs, kb, TN)
    width = gates.shape[1]
    total = None
    for ref in (own, partner, other, far):
        row = joined_row(ref[ref.shape[0] - gate_rows_of(width) :, :], width)
        total = row if total is None else total + row
    gates[...] = total
    i = lax.broadcasted_iota(jnp.int32, (DK, DK), 0)
    j = lax.broadcasted_iota(jnp.int32, (DK, DK), 1)
    shift = VGROUP.bit_length() - 1
    alike = lax.shift_right_logical(i, shift) == lax.shift_right_logical(j, shift)
    averaging = jnp.where(alike, 1.0 / VGROUP, 0.0).astype(bf16)
    for h in range(heads):
        own_rows = slice(h * wide, (h + 1) * wide)
        lanes = slice(h * DK, (h + 1) * DK)
        result = (
            inside[:, own_rows]
            + matmul(reach_f[:, lanes], start_f[own_rows, :].astype(bf16), NT)
            + matmul(reach_b[:, lanes], start_b[own_rows, :].astype(bf16), NT)
        )
        for c in range(wide // DK):
            x = result[:, c * DK : (c + 1) * DK]
            high, low = halves(x * x)
            power = matmul(high, averaging) + matmul(low, averaging)
            at = slice(h * wide + c * DK, h * wide + (c + 1) * DK)
            out[:, at] = (x * lax.rsqrt(power + epsilon) * gated[:, at]).astype(bf16)


def branch_of(order, pieces, weight):
    width = pieces[0].shape[1]
    branch = None
    for k, piece in zip(order, pieces):
        column = pl.multiple_of(lax.bitwise_xor(lax.axis_index("tp"), k) * width, width)
        part = matmul(piece[...], weight[:, pl.ds(column, width)], NT)
        branch = part if branch is None else branch + part
    return branch


def early_kernel(order, *refs):
    weight, out = refs[-2:]
    out[...] = branch_of(order, refs[:-2], weight)


def output_kernel(order, *refs):
    weight, early, latent, gates, out = refs[-5:]
    branch = early[...] + branch_of(order, refs[:-5], weight)
    out[...] = (latent[...].astype(f32) + gates[...] * branch).astype(bf16)


def local_direct(*args):
    return direct_plan(*args)


def direct_plan(
    latent,
    context,
    conditioning,
    context_prompt_vector,
    shift_matrix,
    scale_matrix,
    residual_gate_matrix,
    query_matrix,
    key_matrix,
    value_matrix,
    gate_matrix,
    decay_down_factor,
    decay_up_factor,
    decay_key_bias,
    spike_log_decay,
    output_gain,
    output_matrix,
):
    tp_count, sp_count = (lax.axis_size("tp"), lax.axis_size("sp"))
    heads = HEADS // tp_count
    tokens, width = latent.shape
    ctx = context.shape[0]
    total = tokens + ctx
    features = width * tp_count
    steps = sp_count.bit_length() - 1
    shape = jax.ShapeDtypeStruct

    inner = conditioning.shape[0]
    rows_in = (inner // 128, 128)
    mod, joined = call(
        modulation_kernel,
        [shape((8, width), f32), shape((total, width), bf16)],
        [HBM_SPEC] * 6,
        (
            conditioning.reshape(rows_in),
            context_prompt_vector.reshape(rows_in),
            shift_matrix,
            scale_matrix,
            latent,
            context,
        ),
        4 * 8 * width * inner,
        4 * width * inner,
        [pltpu.VMEM(rows_in, bf16)] * 2
        + [pltpu.VMEM(shift_matrix.shape, bf16)] * 2
        + [pltpu.SemaphoreType.DMA((6,))],
        WIDE_GRANT,
    )
    gate_part = call(
        gating_kernel,
        shape((gate_rows_of(width), DK), bf16),
        [VMEM_SPEC] * 2,
        (conditioning.reshape(rows_in), residual_gate_matrix),
        16 * width * inner,
        2 * width * inner,
    )
    pieces = gathered_pieces(joined, "tp", "lat")
    for bit in range(steps):
        theirs = exchange(mod, "sp", 1 << bit)
        rows = [8] if bit < steps - 1 else [4]
        sums = call(
            add_kernel,
            [shape((r, width), f32) for r in rows],
            [VMEM_SPEC] * 2,
            (mod, theirs),
            8 * width,
            64 * width,
        )
        mod = sums[0]
    mods = [mod]
    for distance in mod_steps(tp_count):
        joint = mods[0]
        if len(mods) > 1:
            joint = call(
                join_kernel,
                shape((2 * mods[-1].shape[0], width), f32),
                [VMEM_SPEC] * len(mods),
                mods,
                8 * width,
                64 * width,
            )
        mods = mods + [exchange(joint, "tp", distance)]

    half = heads * DK
    down = jnp.transpose(decay_down_factor, (0, 2, 1)).reshape(2 * DECAY_RANK, features)
    vdim = value_matrix.shape[0]
    lift = growth_rows(heads)
    surveyed = sorted({k for k, _ in gather_plan(tp_count, "lat")} & {1, 2, 3})
    streamed = (key_matrix, value_matrix, down)
    staged = call(
        stage_kernel,
        shape((half + vdim + 2 * DECAY_RANK, features), bf16),
        [HBM_SPEC] * 3,
        streamed,
        0,
        4 * features * (half + vdim),
        [pltpu.SemaphoreType.DMA((3,))],
        STAGE_GRANT,
    )
    early = call(
        survey_kernel,
        [shape((total, 128), f32)] * 2,
        [VMEM_SPEC] * len(surveyed),
        [pieces[k] for k in surveyed],
        SURVEY_FLOPS,
        SURVEY_BYTES,
    )
    extra_rows = lift + 4 * heads * ctx + gate_rows_of(width)
    normed, keys, values, cum_f, cum_b, payload, extra = call(
        functools.partial(project_kernel, tp_count, tokens, heads, surveyed),
        [
            shape((total, features), bf16),
            shape((tokens, half), bf16),
            shape((tokens, vdim), bf16),
            shape((tokens, half), f32),
            shape((tokens, half), f32),
            shape((2 * vdim + extra_rows, DK), bf16),
            shape((extra_rows, DK), bf16),
        ],
        [VMEM_SPEC] * (tp_count + len(mods) + 5) + [HBM_SPEC] * 2,
        (
            *pieces,
            *mods,
            staged,
            *early,
            jnp.transpose(spike_log_decay, (0, 2, 1)),
            gate_part,
            decay_up_factor,
            decay_key_bias,
        ),
        2 * total * features * (half + vdim),
        2 * features * (half + vdim),
        [
            pltpu.VMEM((2, DECAY_RANK, half), bf16),
            pltpu.VMEM((2, half), f32),
            pltpu.SemaphoreType.DMA((2,)),
        ],
    )
    partner = exchange(payload, "sp", 1)
    other = exchange(extra, "sp", 2)
    pair = call(
        functools.partial(merge_kernel, heads),
        shape((vdim + lift, DK), bf16),
        [VMEM_SPEC, VMEM_SPEC],
        (payload, partner),
        4 * vdim * DK,
        8 * vdim * DK,
    )
    pair = exchange(pair, "sp", 2)
    inside, reach_f, reach_b = call(
        functools.partial(within_kernel, heads),
        [
            shape((tokens, vdim), f32),
            shape((tokens, half), bf16),
            shape((tokens, half), bf16),
        ],
        [VMEM_SPEC] * 6,
        (normed, query_matrix, keys, values, cum_f, cum_b),
        2 * tokens * features * half,
        2 * features * half,
    )
    far = exchange(other, "sp", 1)
    gated = call(
        gated_kernel,
        shape((tokens, vdim), f32),
        [VMEM_SPEC] * 3,
        (normed, gate_matrix, output_gain[None]),
        2 * tokens * features * vdim,
        2 * features * vdim,
    )
    heads_out, gates = call(
        functools.partial(finish_kernel, heads, ctx),
        [shape((tokens, vdim), bf16), shape((1, width), f32)],
        [VMEM_SPEC] * 9,
        (extra, partner, other, far, pair, inside, reach_f, reach_b, gated),
        8 * tokens * vdim * DK,
        8 * tokens * vdim,
        [
            pltpu.VMEM((vdim, DK), f32),
            pltpu.VMEM((vdim, DK), f32),
            pltpu.VMEM((8 * -(-heads // 8), DK), f32),
            pltpu.VMEM((8 * -(-heads // 8), DK), f32),
            pltpu.VMEM((sp_count, lift + 4 * heads * ctx, DK), bf16),
        ],
    )
    branches = gathered_pieces(heads_out, "tp", "out")
    late = [k for k in range(1, tp_count) if k >= tp_count - 3]
    soon = [k for k in range(tp_count) if k not in late]
    cost = 2 * width * vdim
    early = call(
        functools.partial(early_kernel, soon),
        shape((tokens, width), f32),
        [VMEM_SPEC] * (len(soon) + 1),
        (*(branches[k] for k in soon), output_matrix),
        tokens * cost * len(soon),
        cost * len(soon),
    )
    return call(
        functools.partial(output_kernel, late),
        shape((tokens, width), bf16),
        [VMEM_SPEC] * (len(late) + 4),
        (*(branches[k] for k in late), output_matrix, early, latent, gates),
        tokens * cost * len(late),
        cost * len(late),
    )


def solution(mesh):
    placed = (
        P("sp", "tp"),
        P("sp", "tp"),
        P("sp"),
        P("sp"),
        P("tp", "sp"),
        P("tp", "sp"),
        P("tp", "sp"),
        P("tp", None),
        P("tp", None),
        P("tp", None),
        P("tp", None),
        P(),
        P(),
        P(),
        P(None, "sp", None),
        P("tp"),
        P("tp", None),
    )
    tp_count, sp_count = (mesh.shape["tp"], mesh.shape["sp"])
    powers = tp_count & tp_count - 1 == 0
    direct = 2 <= tp_count <= HEADS and sp_count == 4 and powers
    return jax.shard_map(
        local_direct if direct else local_general, mesh=mesh, in_specs=placed, out_specs=P("sp", "tp"), check_vma=False
    )
```

```python
import functools

import jax
import jax.numpy as jnp
from jax import lax
from jax.experimental import pallas as pl
from jax.experimental.pallas import tpu as pltpu
from jax.sharding import PartitionSpec as P


D = 4096
HEADS = 16
DK = 128
DECAY_RANK = 16
BLK = 64
VGROUP = 64


epsilon = 1e-05
gate_norm = 16.0
precise = lax.Precision.HIGHEST


def for_sending(value):

    def short(part):
        return part.astype(jnp.bfloat16) if part.dtype == jnp.float32 else part

    return jax.tree.map(short, value)


def from_partner(value, axis, distance):
    return lax.ppermute(value, axis, [(i, i ^ 1 << distance) for i in range(lax.axis_size(axis))])


def carried_in(value, axis, combine, identity, reverse):
    peers, index = (lax.axis_size(axis), lax.axis_index(axis))
    everything = jax.tree.map(
        lambda part, kind: lax.all_gather(part.astype(kind), axis),
        value,
        (jnp.bfloat16, jnp.bfloat16),
    )
    start = jax.tree.map(
        lambda part, zero: jnp.broadcast_to(jnp.asarray(zero, part.dtype), part.shape),
        value,
        identity,
    )

    def turn(k, before):
        at = peers - 1 - k if reverse else k
        reached = at > index if reverse else at < index
        new = combine(
            before, jax.tree.map(lambda part, own: part[at].astype(own.dtype), everything, value)
        )
        return jax.tree.map(lambda a, b: jnp.where(reached, a, b), new, before)

    return lax.fori_loop(0, peers, turn, start)


def linear(rows, weight):
    return lax.dot_general(
        rows, weight, (((1,), (1,)), ((), ())), preferred_element_type=jnp.float32
    )


def modulated(rows, row_sum, row_squares, shift_vec, scale_vec):
    rows_f = rows.astype(jnp.float32)
    mean_val = row_sum / D
    variance = row_squares / D - mean_val * mean_val
    return (
        (rows_f - mean_val) * lax.rsqrt(variance + epsilon) * (1.0 + scale_vec) + shift_vec
    ).astype(jnp.bfloat16)


def reverse_rows(array):
    return jnp.flip(array, axis=0)


def end_state(key_rows, value_rows, log_decay):
    cumulative = jnp.cumsum(log_decay, axis=0)
    totals = cumulative[-1]
    weighted = key_rows * jnp.exp(totals - cumulative)
    return (jnp.exp(totals), jnp.einsum("nhd,nhe->hde", weighted, value_rows, precision=precise))


def combine(earlier, later):
    return (earlier[0] * later[0], later[0][..., None] * earlier[1] + later[1])


def blockwise(queries, key_rows, value_rows, log_decay, carried, block_len):
    length, head_count, _ = queries.shape
    value_width = value_rows.shape[-1]
    blocks = length // block_len

    def shaped(array):
        return array.reshape(blocks, block_len, head_count, array.shape[-1])

    triangle = jnp.tril(jnp.ones((block_len, block_len), jnp.float32))

    def advance(state_now, inputs):
        block_q, block_k, block_v, block_a = inputs
        cumulative = jnp.cumsum(block_a, axis=0)
        block_end = cumulative[-1]
        query_dec = block_q * jnp.exp(cumulative)
        scores = (
            jnp.einsum("ihd,jhd->hij", query_dec, block_k * jnp.exp(-cumulative), precision=precise)
            * triangle
        )
        result = jnp.einsum("hij,jhe->ihe", scores, block_v, precision=precise)
        result = result + jnp.einsum("ihd,hde->ihe", query_dec, state_now, precision=precise)
        state_next = state_now * jnp.exp(block_end)[:, :, None] + jnp.einsum(
            "jhd,jhe->hde", block_k * jnp.exp(block_end - cumulative), block_v, precision=precise
        )
        return (state_next, result)

    _, outputs = lax.scan(
        advance, carried, (shaped(queries), shaped(key_rows), shaped(value_rows), shaped(log_decay))
    )
    return outputs.reshape(length, head_count, value_width)


def head_channels(pieces, per_head, tp_index):
    for bit_number in range(per_head.bit_length() - 1):
        partner = from_partner(
            (for_sending(pieces[0]), for_sending(pieces[1]), for_sending(pieces[2])),
            "tp",
            bit_number,
        )
        upper = tp_index // (1 << bit_number) % 2 == 1
        pieces = tuple(
            (
                jnp.where(
                    upper,
                    jnp.concatenate([theirs, mine], axis=1),
                    jnp.concatenate([mine, theirs], axis=1),
                )
                for mine, theirs in zip(pieces, partner)
            )
        )
    return pieces


def context_totals(fwd_growth, fwd_state, bwd_growth, bwd_state, identity):

    def absorb(carried, piece):
        return (combine(carried, piece), None)

    total_fwd, _ = lax.scan(absorb, identity, (fwd_growth, fwd_state))
    total_bwd, _ = lax.scan(absorb, identity, (bwd_growth, bwd_state), reverse=True)
    return (total_fwd, total_bwd)


def stored(array):
    return lax.optimization_barrier(array.astype(jnp.bfloat16))


def local_general(
    latent,
    context,
    conditioning,
    context_prompt_vector,
    shift_matrix,
    scale_matrix,
    residual_gate_matrix,
    query_matrix,
    key_matrix,
    value_matrix,
    gate_matrix,
    decay_down_factor,
    decay_up_factor,
    decay_key_bias,
    spike_log_decay,
    output_gain,
    output_matrix,
):
    tp_count = lax.axis_size("tp")
    tp_index = lax.axis_index("tp")
    per_head = max(tp_count // HEADS, 1)
    heads_per_shard = max(HEADS // tp_count, 1)
    leading_head = tp_index // per_head * heads_per_shard
    tok_rows = latent.shape[0]
    conds = jax.nn.silu(
        jnp.stack([conditioning, context_prompt_vector]).astype(jnp.float32)
    ).astype(jnp.bfloat16)
    shifts, scales, gates = lax.psum(
        (
            linear(conds, shift_matrix),
            linear(conds, scale_matrix),
            linear(conds, residual_gate_matrix),
        ),
        "sp",
    )
    down_both = jnp.concatenate([decay_down_factor[0].T, decay_down_factor[1].T], axis=0)
    lat_weights = (query_matrix, key_matrix, value_matrix, gate_matrix, down_both)
    ctx_weights = (key_matrix, value_matrix, down_both)
    lat_f = latent.astype(jnp.float32)
    ctx_f = context.astype(jnp.float32)
    lat_sum, lat_squares, ctx_sum, ctx_squares = lax.psum(
        (
            jnp.sum(lat_f, axis=1, keepdims=True),
            jnp.sum(lat_f * lat_f, axis=1, keepdims=True),
            jnp.sum(ctx_f, axis=1, keepdims=True),
            jnp.sum(ctx_f * ctx_f, axis=1, keepdims=True),
        ),
        "tp",
    )
    latent_normalized = modulated(latent, lat_sum, lat_squares, shifts[0], scales[0])
    normed_ctx = modulated(context, ctx_sum, ctx_squares, shifts[1], scales[1])
    lat_piece = lax.all_gather(latent_normalized, "tp", axis=1, tiled=True)
    ctx_piece = lax.all_gather(normed_ctx, "tp", axis=1, tiled=True)
    lat_new = tuple((linear(lat_piece, weight) for weight in lat_weights))
    ctx_new = tuple((linear(ctx_piece, weight) for weight in ctx_weights))
    query_part, key_part, value_part, gate_part, low_rank_part = lat_new
    ctx_key_part, ctx_value_part, ctx_low = ctx_new
    query_full, key_full, ctx_key_full = head_channels(
        (stored(query_part), stored(key_part), stored(ctx_key_part)), per_head, tp_index
    )

    def split_heads(rows, width):
        return rows.astype(jnp.float32).reshape(rows.shape[0], heads_per_shard, width)

    value_cols = value_part.shape[1] // heads_per_shard
    queries = split_heads(query_full, DK) * DK ** (-0.5)
    key_rows = split_heads(key_full, DK)
    ctx_keys = split_heads(ctx_key_full, DK)
    values_lat = split_heads(stored(value_part), value_cols)
    values_ctx = split_heads(stored(ctx_value_part), value_cols)
    gate_rows = stored(gate_part).astype(jnp.float32)

    def per_head_decay(low_rows, direction):
        up_part = lax.dynamic_slice_in_dim(
            decay_up_factor[direction], leading_head * DK, heads_per_shard * DK, 1
        ).astype(jnp.float32)
        bias_part = lax.dynamic_slice_in_dim(
            decay_key_bias[direction], leading_head * DK, heads_per_shard * DK, 0
        )
        pre_act = jnp.dot(low_rows, up_part, precision=precise) + bias_part
        return (jax.nn.log_sigmoid(pre_act) / gate_norm).reshape(
            low_rows.shape[0], heads_per_shard, DK
        )

    decay_spikes = lax.dynamic_slice_in_dim(spike_log_decay, leading_head, heads_per_shard, 2)
    latent_forward = per_head_decay(low_rank_part[:, :DECAY_RANK], 0) + decay_spikes[0][:, :, None]
    latent_backward = per_head_decay(low_rank_part[:, DECAY_RANK:], 1) + decay_spikes[1][:, :, None]
    ctx_fwd = per_head_decay(ctx_low[:, :DECAY_RANK], 0)
    ctx_bwd = per_head_decay(ctx_low[:, DECAY_RANK:], 1)
    cf_growth, cf_state = end_state(ctx_keys, values_ctx, ctx_fwd)
    cb_growth, cb_state = end_state(
        reverse_rows(ctx_keys), reverse_rows(values_ctx), reverse_rows(ctx_bwd)
    )
    lf_growth, lf_state = end_state(key_rows, values_lat, latent_forward)
    lb_growth, lb_state = end_state(
        reverse_rows(key_rows), reverse_rows(values_lat), reverse_rows(latent_backward)
    )
    identity = (
        jnp.ones((heads_per_shard, DK), jnp.float32),
        jnp.zeros((heads_per_shard, DK, value_cols), jnp.float32),
    )
    ctx_gathered = (
        lax.all_gather(cf_growth[None].astype(jnp.bfloat16), "sp", axis=0, tiled=True).astype(
            jnp.float32
        ),
        lax.all_gather(cf_state[None].astype(jnp.bfloat16), "sp", axis=0, tiled=True).astype(
            jnp.float32
        ),
        lax.all_gather(cb_growth[None].astype(jnp.bfloat16), "sp", axis=0, tiled=True).astype(
            jnp.float32
        ),
        lax.all_gather(cb_state[None].astype(jnp.bfloat16), "sp", axis=0, tiled=True).astype(
            jnp.float32
        ),
    )
    total_fwd, total_bwd = context_totals(
        ctx_gathered[0], ctx_gathered[1], ctx_gathered[2], ctx_gathered[3], identity
    )
    prefix = carried_in((lf_growth, lf_state), "sp", combine, identity, False)
    suffix = carried_in((lb_growth, lb_state), "sp", combine, identity, True)
    start_fwd = combine(total_fwd, prefix)[1]
    start_bwd = combine(total_bwd, suffix)[1]
    zero_state = jnp.zeros((heads_per_shard, DK, value_cols), jnp.float32)

    def direction_out(query_rows, key_list, value_list, log_decay, start_state):
        local_part = blockwise(query_rows, key_list, value_list, log_decay, zero_state, BLK)
        reach = query_rows * jnp.exp(jnp.cumsum(log_decay, axis=0))
        return local_part + jnp.einsum("nhd,hde->nhe", reach, start_state, precision=precise)

    out_fwd = direction_out(queries, key_rows, values_lat, latent_forward, start_fwd)
    out_bwd = reverse_rows(
        direction_out(
            reverse_rows(queries),
            reverse_rows(key_rows),
            reverse_rows(values_lat),
            reverse_rows(latent_backward),
            start_bwd,
        )
    )
    grouped = (out_fwd + out_bwd).reshape(tok_rows, -1, VGROUP)
    grouped = grouped * lax.rsqrt(jnp.mean(grouped * grouped, axis=-1, keepdims=True) + epsilon)
    heads_out = (grouped.reshape(tok_rows, -1) * output_gain * jax.nn.silu(gate_rows)).astype(
        jnp.bfloat16
    )
    branch = linear(lax.all_gather(heads_out, "tp", axis=1, tiled=True), output_matrix)
    return (latent.astype(jnp.float32) + gates[0] * branch).astype(jnp.bfloat16)


VMEM_SPEC = pl.BlockSpec(memory_space=pltpu.VMEM)
HBM_SPEC = pl.BlockSpec(memory_space=pltpu.HBM)
NT = (((1,), (1,)), ((), ()))
NN = (((1,), (0,)), ((), ()))
TN = (((0,), (0,)), ((), ()))
f32 = jnp.float32
bf16 = jnp.bfloat16


def matmul(a, b, dims=NN):
    return lax.dot_general(a, b, dims, preferred_element_type=f32)


def halves(value):
    high = value.astype(bf16)
    return (high, (value - high.astype(f32)).astype(bf16))


def exchange(value, axis, distance):
    return lax.ppermute(value, axis, [(i, i ^ distance) for i in range(lax.axis_size(axis))])


def gather_plan(count, label):
    if count == 8:
        return PLANS[label]
    half = count // 2
    direct = dict.fromkeys(k for k in (half, 2, 1, count - 1) if k < count)
    plan = [(k, 0) for k in direct]
    for k in range(3, count):
        if k not in direct:
            plan.append((k, half if k & half else 2 if k == 3 else 0))
    return plan


def gathered_pieces(value, axis, label):
    pieces = {0: value}
    for k, source in gather_plan(lax.axis_size(axis), label):
        pieces[k] = exchange(pieces[source], axis, k ^ source)
    return [pieces[k] for k in sorted(pieces)]


def mod_steps(count):
    return MOD_STEPS if count == 8 else tuple(1 << bit for bit in range(count.bit_length() - 1))


WIDE_GRANT = 60000
STAGE_GRANT = 2 << 10
SURVEY_FLOPS = 15 * 10**9
SURVEY_BYTES = 40 * 10**6
MOD_STEPS = (1, 2, 4)
LATE = (5, 6)
MIDDLE = (7,)
PLANS = {
    "lat": ((4, 0), (2, 0), (1, 0), (7, 0), (3, 2), (5, 4), (6, 4)),
    "out": ((2, 0), (4, 0), (1, 0), (3, 2), (7, 0), (5, 4), (6, 4)),
}


def call(kernel, out_shapes, in_specs, args, flops, traffic, scratch=(), grant=24 << 10):
    single = not isinstance(out_shapes, (tuple, list))
    return pl.pallas_call(
        kernel,
        out_shape=out_shapes,
        in_specs=in_specs,
        out_specs=VMEM_SPEC if single else [VMEM_SPEC] * len(out_shapes),
        scratch_shapes=list(scratch),
        compiler_params=pltpu.CompilerParams(vmem_limit_bytes=grant << 10),
        cost_estimate=pl.CostEstimate(flops=flops, bytes_accessed=traffic, transcendentals=0),
    )(*args)


def fetch(sources, targets, sems):
    copies = [
        pltpu.make_async_copy(source, target, sems.at[n])
        for n, (source, target) in enumerate(zip(sources, targets))
    ]
    for copy in copies:
        copy.start()
    return copies


def in_one_row(ref):
    block = ref[...].astype(f32)
    return jnp.concatenate([block[r : r + 1] for r in range(block.shape[0])], axis=1)


def modulation_kernel(*refs):
    sources = refs[:6]
    out, joined = refs[6:8]
    cond_ref, prompt_ref, *weights = refs[8:12]
    tokens = sources[4].shape[0]
    rows = (joined.at[pl.ds(0, tokens)], joined.at[pl.ds(tokens, sources[5].shape[0])])
    copies = fetch(sources, (cond_ref, prompt_ref, *weights, *rows), refs[12])
    copies[0].wait()
    cond = in_one_row(cond_ref)
    copies[1].wait()
    row = lax.broadcasted_iota(jnp.int32, (8, cond.shape[1]), 0)
    both = jnp.where(row % 2 == 0, cond, in_one_row(prompt_ref))
    conds = (both * jax.nn.sigmoid(both)).astype(bf16)
    row_out = lax.broadcasted_iota(jnp.int32, out.shape, 0)
    copies[2].wait()
    shifts = matmul(conds, weights[0][...], NT)
    copies[3].wait()
    scales = matmul(conds, weights[1][...], NT)
    out[...] = jnp.where(row_out < 2, shifts, scales)
    copies[4].wait()
    copies[5].wait()


def gate_rows_of(width):
    return -(-2 * (width // DK) // 16) * 16


def split_row(value):
    count = value.shape[1] // DK
    rows = [value[:, c * DK : (c + 1) * DK] for c in range(count)]
    blank = jnp.zeros((gate_rows_of(value.shape[1]) - 2 * count, DK), bf16)
    parts = [halves(row) for row in rows]
    return jnp.concatenate([p[0] for p in parts] + [p[1] for p in parts] + [blank], axis=0)


def joined_row(block, width):
    count = width // DK
    value = block.astype(f32)
    value = value[:count] + value[count : 2 * count]
    return jnp.concatenate([value[c : c + 1] for c in range(count)], axis=1)


def gating_kernel(cond_ref, weight, out):
    cond = in_one_row(cond_ref)
    cond = jnp.broadcast_to(cond, (8, cond.shape[1]))
    conds = (cond * jax.nn.sigmoid(cond)).astype(bf16)
    out[...] = split_row(matmul(conds, weight[...], NT)[:1])


def row_sums(pieces):
    total, width = pieces[0].shape
    sums = jnp.zeros((total, 128), f32)
    squares = jnp.zeros((total, 128), f32)
    for piece in pieces:
        for c in range(width // 128):
            x = piece[:, c * 128 : (c + 1) * 128].astype(f32)
            sums = sums + x
            squares = squares + x * x
    return (sums, squares)


def add_kernel(mine, theirs, *outs):
    total = mine[...] + theirs[...]
    for out in outs:
        out[...] = total[: out.shape[0]]


def join_kernel(*refs):
    at = 0
    for ref in refs[:-1]:
        refs[-1][at : at + ref.shape[0], :] = ref[...]
        at += ref.shape[0]


def stage_kernel(*refs):
    sources = refs[:-2]
    targets, at = ([], 0)
    for source in sources:
        targets.append(refs[-2].at[pl.ds(at, source.shape[0])])
        at += source.shape[0]
    for copy in fetch(sources, targets, refs[-1]):
        copy.wait()


def survey_kernel(*refs):
    refs[-2][...], refs[-1][...] = row_sums(refs[:-2])


def block_masks(total, tokens, wanted):
    i = lax.broadcasted_iota(jnp.int32, (total, total), 0)
    j = lax.broadcasted_iota(jnp.int32, (total, total), 1)
    last = tokens // BLK
    bi = jnp.minimum(lax.shift_right_logical(i, BLK.bit_length() - 1), last)
    bj = jnp.minimum(lax.shift_right_logical(j, BLK.bit_length() - 1), last)
    return wanted(i, j, bi, bj)


def project_kernel(count, tokens, heads, surveyed, *refs):
    pieces = refs[:count]
    mods = refs[count : count + count.bit_length()]
    refs = refs[count + count.bit_length() :]
    weights, early_sums, early_squares, spikes, gate_part = refs[:5]
    normed, keys, values, cum_f, cum_b, payload, extra = refs[7:14]
    up_own, bias_own, sems = refs[14:]
    tp = lax.axis_index("tp")
    half = heads * DK
    first = pl.multiple_of(tp * half, half)
    sources = (refs[5].at[:, :, pl.ds(first, half)], refs[6].at[:, pl.ds(first, half)])
    copies = fetch(sources, (up_own, bias_own), sems)
    total, width = pieces[0].shape
    ctx = total - tokens
    features = width * count

    held = [[0]]
    for distance in mod_steps(count):
        held.append([k ^ distance for k in sum(held, [])])
    found = {k: (level, at) for level, ks in enumerate(held) for at, k in enumerate(ks)}

    def mod_row(k, row):
        level, at = found[k]
        return mods[level][4 * at + row : 4 * at + row + 1, :]

    sums, squares = row_sums([pieces[k] for k in range(count) if k not in surveyed])
    sums, squares = (sums + early_sums[...], squares + early_squares[...])
    mean = jnp.sum(sums, axis=1, keepdims=True) / features
    variance = jnp.sum(squares, axis=1, keepdims=True) / features - mean * mean
    inverse = lax.rsqrt(variance + epsilon)
    for k, piece in enumerate(pieces):
        column = pl.multiple_of(lax.bitwise_xor(tp, k) * width, width)
        scaled = (piece[...].astype(f32) - mean) * inverse
        ahead = scaled[:tokens] * (1.0 + mod_row(k, 2)) + mod_row(k, 0)
        context = scaled[tokens:] * (1.0 + mod_row(k, 3)) + mod_row(k, 1)
        normed[:tokens, pl.ds(column, width)] = ahead.astype(bf16)
        normed[tokens:, pl.ds(column, width)] = context.astype(bf16)
    products = matmul(weights[...], normed[...], NT).T
    key_all = products[:, :half].astype(bf16)
    value_all = products[:, half : half + values.shape[1]].astype(bf16)
    low_high, low_low = halves(products[:, half + values.shape[1] :])
    for copy in copies:
        copy.wait()
    blank = jnp.zeros((DECAY_RANK, half), bf16)
    up = jnp.concatenate(
        [
            jnp.concatenate([up_own[0], blank], axis=1),
            jnp.concatenate([blank, up_own[1]], axis=1),
        ],
        axis=0,
    )
    bias = jnp.concatenate([bias_own[0:1, :], bias_own[1:2, :]], axis=1)
    pre = matmul(low_high, up) + matmul(low_low, up) + bias
    decay = (jnp.minimum(pre, 0.0) - jnp.log1p(jnp.exp(-jnp.abs(pre)))) * (1.0 / gate_norm)
    row = lax.broadcasted_iota(jnp.int32, (spikes.shape[1], half), 0)
    head = lax.shift_right_logical(
        lax.broadcasted_iota(jnp.int32, (spikes.shape[1], half), 1), DK.bit_length() - 1
    )
    wanted = jnp.where(row == head + tp * heads, 1.0, 0.0).astype(bf16)
    marks = []
    for d in range(2):
        spike_high, spike_low = halves(spikes[d])
        added = matmul(spike_high, wanted, TN) + matmul(spike_low, wanted, TN)
        marks.append(decay[:tokens, d * half : (d + 1) * half] + added)
    decay = jnp.concatenate([jnp.concatenate(marks, axis=1), decay[tokens:]], axis=0)
    ones = jnp.ones((total, total), f32)
    zeros = jnp.zeros((total, total), f32)
    lower = block_masks(
        total, tokens, lambda i, j, bi, bj: jnp.where((bi == bj) & (i >= j), ones, zeros)
    ).astype(bf16)
    upper = block_masks(
        total, tokens, lambda i, j, bi, bj: jnp.where((bi == bj) & (i <= j), ones, zeros)
    ).astype(bf16)
    high, low = halves(decay)
    cf = matmul(lower, high[:, :half]) + matmul(lower, low[:, :half])
    cb = matmul(upper, high[:, half:]) + matmul(upper, low[:, half:])
    cum_f[...] = cf[:tokens]
    cum_b[...] = cb[:tokens]
    keys[...] = key_all[:tokens]
    values[...] = value_all[:tokens]
    wide = value_all.shape[1] // heads
    blocks = tokens // BLK
    size = heads * wide
    growth = [[], [], [], []]
    start = 2 * size + growth_rows(heads)
    for h in range(heads):
        own = slice(h * DK, (h + 1) * DK)
        kh = key_all[:, own].astype(f32)
        vh = value_all[:tokens, h * wide : (h + 1) * wide]
        cfh, cbh = (cf[:, own], cb[:, own])
        ends_f = [cfh[(b + 1) * BLK - 1 : (b + 1) * BLK] for b in range(blocks)]
        ends_b = [cbh[b * BLK : b * BLK + 1] for b in range(blocks)]
        weighted_f, weighted_b = ([], [])
        for b in range(blocks):
            rows = slice(b * BLK, (b + 1) * BLK)
            weighted_f.append(kh[rows] * jnp.exp(sum(ends_f[b + 1 :], ends_f[b]) - cfh[rows]))
            weighted_b.append(kh[rows] * jnp.exp(sum(ends_b[:b], ends_b[b]) - cbh[rows]))
        kf = jnp.concatenate(weighted_f, axis=0).astype(bf16)
        kb = jnp.concatenate(weighted_b, axis=0).astype(bf16)
        payload[h * wide : (h + 1) * wide, :] = matmul(vh, kf, TN).astype(bf16)
        payload[size + h * wide : size + (h + 1) * wide, :] = matmul(vh, kb, TN).astype(bf16)
        growth[0].append(jnp.exp(sum(ends_f[1:], ends_f[0])))
        growth[1].append(jnp.exp(sum(ends_b[1:], ends_b[0])))
        end_f, end_b = (cfh[total - 1 : total], cbh[tokens : tokens + 1])
        growth[2].append(jnp.exp(end_f))
        growth[3].append(jnp.exp(end_b))
        at = start + h * ctx
        payload[at : at + ctx, :] = (kh[tokens:] * jnp.exp(end_f - cfh[tokens:])).astype(bf16)
        at = at + heads * ctx
        payload[at : at + ctx, :] = (kh[tokens:] * jnp.exp(end_b - cbh[tokens:])).astype(bf16)
    for c in range(size // DK):
        at = start + (2 * heads + c) * ctx
        payload[at : at + ctx, :] = value_all[tokens:, c * DK : (c + 1) * DK]
    payload[2 * size : start, :] = growth_block(growth, heads)
    payload[start + 4 * heads * ctx :, :] = gate_part[...]
    extra[...] = payload[2 * size :, :]


def growth_rows(heads):
    return -(-4 * heads // 16) * 16


def growth_block(growth, heads):
    rows = [row for kind in growth for row in kind]
    blank = jnp.zeros((growth_rows(heads) - len(rows), DK), f32)
    return jnp.concatenate([*rows, blank], axis=0).astype(bf16)


def growth_of(ref, at, kind, h, heads):
    block = ref[at : at + growth_rows(heads), :].astype(f32)
    return block[kind * heads + h : kind * heads + h + 1]


def gated_kernel(normed, gate_w, gain, gated):
    products = matmul(gate_w[...], normed[: gated.shape[0], :], NT).T
    gates = products.astype(bf16).astype(f32)
    gated[...] = gates * jax.nn.sigmoid(gates) * gain[...]


def within_kernel(heads, normed, query_w, keys, values, cum_f, cum_b, inside, reach_f, reach_b):
    tokens = keys.shape[0]
    rows_in = normed[:tokens, :]
    query_all = matmul(rows_in, query_w[...], NT).astype(bf16).astype(f32) * DK ** (-0.5)
    wide = values.shape[1] // heads
    blocks = tokens // BLK

    def choose(i, j, bi, bj):
        same = bi == bj
        return (same & (i >= j), same & (i <= j), bi > bj, bi < bj)

    forward, backward, later, sooner = block_masks(tokens, tokens, choose)
    for h in range(heads):
        own = slice(h * DK, (h + 1) * DK)
        qh = query_all[:, own]
        kh = keys[:, own].astype(f32)
        cf, cb = (cum_f[:, own], cum_b[:, own])
        ends_f = [cf[(b + 1) * BLK - 1 : (b + 1) * BLK] for b in range(blocks)]
        ends_b = [cb[b * BLK : b * BLK + 1] for b in range(blocks)]
        spread = (BLK, DK)
        end_f = jnp.concatenate([jnp.broadcast_to(e, spread) for e in ends_f], axis=0)
        end_b = jnp.concatenate([jnp.broadcast_to(e, spread) for e in ends_b], axis=0)
        qf, qb = (qh * jnp.exp(cf), qh * jnp.exp(cb))
        qf_b, qb_b = (qf.astype(bf16), qb.astype(bf16))
        scores = (
            jnp.where(forward, matmul(qf_b, (kh * jnp.exp(-cf)).astype(bf16), NT), 0.0)
            + jnp.where(backward, matmul(qb_b, (kh * jnp.exp(-cb)).astype(bf16), NT), 0.0)
            + jnp.where(later, matmul(qf_b, (kh * jnp.exp(end_f - cf)).astype(bf16), NT), 0.0)
            + jnp.where(sooner, matmul(qb_b, (kh * jnp.exp(end_b - cb)).astype(bf16), NT), 0.0)
        )
        vh = values[:, h * wide : (h + 1) * wide]
        inside[:, h * wide : (h + 1) * wide] = matmul(scores.astype(bf16), vh)
        for b in range(blocks):
            rows = slice(b * BLK, (b + 1) * BLK)
            before = sum(ends_f[:b], jnp.zeros_like(ends_f[0]))
            after = sum(ends_b[b + 1 :], jnp.zeros_like(ends_b[0]))
            reach_f[rows, own] = (qf[rows] * jnp.exp(before)).astype(bf16)
            reach_b[rows, own] = (qb[rows] * jnp.exp(after)).astype(bf16)


def merge_kernel(heads, own, partner, out):
    lift = growth_rows(heads)
    size = out.shape[0] - lift
    wide = size // heads
    sp = lax.axis_index("sp")

    def emit(low, up):
        def forward():
            for h in range(heads):
                rows = slice(h * wide, (h + 1) * wide)
                decayed = growth_of(up, 2 * size, 0, h, heads) * low[rows, :].astype(f32)
                out[rows, :] = (decayed + up[rows, :].astype(f32)).astype(bf16)

        def backward():
            for h in range(heads):
                rows = slice(size + h * wide, size + (h + 1) * wide)
                decayed = growth_of(low, 2 * size, 1, h, heads) * up[rows, :].astype(f32)
                out[h * wide : (h + 1) * wide, :] = (
                    decayed + low[rows, :].astype(f32)
                ).astype(bf16)

        pl.when(sp < 2)(forward)
        pl.when(sp >= 2)(backward)
        rates = slice(2 * size, 2 * size + lift)
        out[size:, :] = (low[rates, :].astype(f32) * up[rates, :].astype(f32)).astype(bf16)

    pl.when(sp % 2 == 0)(lambda: emit(own, partner))
    pl.when(sp % 2 == 1)(lambda: emit(partner, own))


def finish_kernel(heads, ctx, *refs):
    own, partner, other, far, pair = refs[:5]
    inside, reach_f, reach_b, gated, out, gates = refs[5:11]
    start_f, start_b, grow_f, grow_b, shared = refs[11:]
    sp = lax.axis_index("sp")
    size = start_f.shape[0]
    wide = size // heads
    lift = growth_rows(heads)
    devices, rows_shared, _ = shared.shape
    start_f[...] = jnp.zeros(start_f.shape, f32)
    start_b[...] = jnp.zeros(start_b.shape, f32)
    grow_f[...] = jnp.ones(grow_f.shape, f32)
    grow_b[...] = jnp.ones(grow_b.shape, f32)

    def take(start, grow, source, at, kind, rates):
        for h in range(heads):
            rows = slice(h * wide, (h + 1) * wide)
            one = slice(h, h + 1)
            theirs = source[at + h * wide : at + (h + 1) * wide, :].astype(f32)
            start[rows, :] = start[rows, :] + grow[one, :] * theirs
            grow[one, :] = grow[one, :] * growth_of(source, rates, kind, h, heads)

    pl.when(sp % 2 == 1)(functools.partial(take, start_f, grow_f, partner, 0, 0, 2 * size))
    pl.when(sp % 2 == 0)(functools.partial(take, start_b, grow_b, partner, size, 1, 2 * size))
    pl.when(sp >= 2)(functools.partial(take, start_f, grow_f, pair, 0, 0, size))
    pl.when(sp < 2)(functools.partial(take, start_b, grow_b, pair, 0, 1, size))
    shared[sp] = own[:rows_shared, :]
    shared[lax.bitwise_xor(sp, 1)] = partner[2 * size : 2 * size + rows_shared, :]
    shared[lax.bitwise_xor(sp, 2)] = other[:rows_shared, :]
    shared[lax.bitwise_xor(sp, 3)] = far[:rows_shared, :]

    def part(d, section):
        return shared[d, lift + section * ctx : lift + (section + 1) * ctx, :]

    def rate(d, kind, h):
        return shared[d, :lift, :].astype(f32)[kind * heads + h : kind * heads + h + 1]

    def chained(order, kind, h, section):
        rows, running = ({}, None)
        for d in order:
            rows[d] = part(d, section)
            if running is not None:
                rows[d] = (rows[d].astype(f32) * running).astype(bf16)
            running = rate(d, kind, h) if running is None else running * rate(d, kind, h)
        return jnp.concatenate([rows[d] for d in range(devices)], axis=0)

    for h in range(heads):
        one = slice(h, h + 1)
        kf = chained(range(devices - 1, -1, -1), 2, h, h)
        kb = chained(range(devices), 3, h, heads + h)
        first = 2 * heads + h * (wide // DK)
        for c in range(wide // DK):
            vs = jnp.concatenate([part(d, first + c) for d in range(devices)], axis=0)
            at = slice(h * wide + c * DK, h * wide + (c + 1) * DK)
            start_f[at, :] += grow_f[one, :] * matmul(vs, kf, TN)
            start_b[at, :] += grow_b[one, :] * matmul(vs, kb, TN)
    width = gates.shape[1]
    total = None
    for ref in (own, partner, other, far):
        row = joined_row(ref[ref.shape[0] - gate_rows_of(width) :, :], width)
        total = row if total is None else total + row
    gates[...] = total
    i = lax.broadcasted_iota(jnp.int32, (DK, DK), 0)
    j = lax.broadcasted_iota(jnp.int32, (DK, DK), 1)
    shift = VGROUP.bit_length() - 1
    alike = lax.shift_right_logical(i, shift) == lax.shift_right_logical(j, shift)
    averaging = jnp.where(alike, 1.0 / VGROUP, 0.0).astype(bf16)
    for h in range(heads):
        own_rows = slice(h * wide, (h + 1) * wide)
        lanes = slice(h * DK, (h + 1) * DK)
        result = (
            inside[:, own_rows]
            + matmul(reach_f[:, lanes], start_f[own_rows, :].astype(bf16), NT)
            + matmul(reach_b[:, lanes], start_b[own_rows, :].astype(bf16), NT)
        )
        for c in range(wide // DK):
            x = result[:, c * DK : (c + 1) * DK]
            high, low = halves(x * x)
            power = matmul(high, averaging) + matmul(low, averaging)
            at = slice(h * wide + c * DK, h * wide + (c + 1) * DK)
            out[:, at] = (x * lax.rsqrt(power + epsilon) * gated[:, at]).astype(bf16)


def branch_of(order, pieces, weight):
    width = pieces[0].shape[1]
    branch = None
    for k, piece in zip(order, pieces):
        column = pl.multiple_of(lax.bitwise_xor(lax.axis_index("tp"), k) * width, width)
        part = matmul(piece[...], weight[:, pl.ds(column, width)], NT)
        branch = part if branch is None else branch + part
    return branch


def early_kernel(order, *refs):
    weight, out = refs[-2:]
    out[...] = branch_of(order, refs[:-2], weight)


def middle_kernel(order, *refs):
    weight, early, out = refs[-3:]
    out[...] = early[...] + branch_of(order, refs[:-3], weight)


def output_kernel(order, *refs):
    weight, early, latent, gates, out = refs[-5:]
    branch = early[...] + branch_of(order, refs[:-5], weight)
    out[...] = (latent[...].astype(f32) + gates[...] * branch).astype(bf16)


def local_direct(*args):
    return direct_plan(*args)


def direct_plan(
    latent,
    context,
    conditioning,
    context_prompt_vector,
    shift_matrix,
    scale_matrix,
    residual_gate_matrix,
    query_matrix,
    key_matrix,
    value_matrix,
    gate_matrix,
    decay_down_factor,
    decay_up_factor,
    decay_key_bias,
    spike_log_decay,
    output_gain,
    output_matrix,
):
    tp_count, sp_count = (lax.axis_size("tp"), lax.axis_size("sp"))
    heads = HEADS // tp_count
    tokens, width = latent.shape
    ctx = context.shape[0]
    total = tokens + ctx
    features = width * tp_count
    steps = sp_count.bit_length() - 1
    shape = jax.ShapeDtypeStruct

    inner = conditioning.shape[0]
    rows_in = (inner // 128, 128)
    mod, joined = call(
        modulation_kernel,
        [shape((8, width), f32), shape((total, width), bf16)],
        [HBM_SPEC] * 6,
        (
            conditioning.reshape(rows_in),
            context_prompt_vector.reshape(rows_in),
            shift_matrix,
            scale_matrix,
            latent,
            context,
        ),
        4 * 8 * width * inner,
        4 * width * inner,
        [pltpu.VMEM(rows_in, bf16)] * 2
        + [pltpu.VMEM(shift_matrix.shape, bf16)] * 2
        + [pltpu.SemaphoreType.DMA((6,))],
        WIDE_GRANT,
    )
    gate_part = call(
        gating_kernel,
        shape((gate_rows_of(width), DK), bf16),
        [VMEM_SPEC] * 2,
        (conditioning.reshape(rows_in), residual_gate_matrix),
        16 * width * inner,
        2 * width * inner,
    )
    pieces = gathered_pieces(joined, "tp", "lat")
    for bit in range(steps):
        theirs = exchange(mod, "sp", 1 << bit)
        rows = [8] if bit < steps - 1 else [4]
        sums = call(
            add_kernel,
            [shape((r, width), f32) for r in rows],
            [VMEM_SPEC] * 2,
            (mod, theirs),
            8 * width,
            64 * width,
        )
        mod = sums[0]
    mods = [mod]
    for distance in mod_steps(tp_count):
        joint = mods[0]
        if len(mods) > 1:
            joint = call(
                join_kernel,
                shape((2 * mods[-1].shape[0], width), f32),
                [VMEM_SPEC] * len(mods),
                mods,
                8 * width,
                64 * width,
            )
        mods = mods + [exchange(joint, "tp", distance)]

    half = heads * DK
    down = jnp.transpose(decay_down_factor, (0, 2, 1)).reshape(2 * DECAY_RANK, features)
    vdim = value_matrix.shape[0]
    lift = growth_rows(heads)
    surveyed = sorted({k for k, _ in gather_plan(tp_count, "lat")} & {1, 2, 3})
    streamed = (key_matrix, value_matrix, down)
    staged = call(
        stage_kernel,
        shape((half + vdim + 2 * DECAY_RANK, features), bf16),
        [HBM_SPEC] * 3,
        streamed,
        0,
        4 * features * (half + vdim),
        [pltpu.SemaphoreType.DMA((3,))],
        STAGE_GRANT,
    )
    early = call(
        survey_kernel,
        [shape((total, 128), f32)] * 2,
        [VMEM_SPEC] * len(surveyed),
        [pieces[k] for k in surveyed],
        SURVEY_FLOPS,
        SURVEY_BYTES,
    )
    extra_rows = lift + 4 * heads * ctx + gate_rows_of(width)
    normed, keys, values, cum_f, cum_b, payload, extra = call(
        functools.partial(project_kernel, tp_count, tokens, heads, surveyed),
        [
            shape((total, features), bf16),
            shape((tokens, half), bf16),
            shape((tokens, vdim), bf16),
            shape((tokens, half), f32),
            shape((tokens, half), f32),
            shape((2 * vdim + extra_rows, DK), bf16),
            shape((extra_rows, DK), bf16),
        ],
        [VMEM_SPEC] * (tp_count + len(mods) + 5) + [HBM_SPEC] * 2,
        (
            *pieces,
            *mods,
            staged,
            *early,
            jnp.transpose(spike_log_decay, (0, 2, 1)),
            gate_part,
            decay_up_factor,
            decay_key_bias,
        ),
        2 * total * features * (half + vdim),
        2 * features * (half + vdim),
        [
            pltpu.VMEM((2, DECAY_RANK, half), bf16),
            pltpu.VMEM((2, half), f32),
            pltpu.SemaphoreType.DMA((2,)),
        ],
    )
    partner = exchange(payload, "sp", 1)
    other = exchange(extra, "sp", 2)
    pair = call(
        functools.partial(merge_kernel, heads),
        shape((vdim + lift, DK), bf16),
        [VMEM_SPEC, VMEM_SPEC],
        (payload, partner),
        4 * vdim * DK,
        8 * vdim * DK,
    )
    pair = exchange(pair, "sp", 2)
    inside, reach_f, reach_b = call(
        functools.partial(within_kernel, heads),
        [
            shape((tokens, vdim), f32),
            shape((tokens, half), bf16),
            shape((tokens, half), bf16),
        ],
        [VMEM_SPEC] * 6,
        (normed, query_matrix, keys, values, cum_f, cum_b),
        2 * tokens * features * half,
        2 * features * half,
    )
    far = exchange(other, "sp", 1)
    gated = call(
        gated_kernel,
        shape((tokens, vdim), f32),
        [VMEM_SPEC] * 3,
        (normed, gate_matrix, output_gain[None]),
        2 * tokens * features * vdim,
        2 * features * vdim,
    )
    heads_out, gates = call(
        functools.partial(finish_kernel, heads, ctx),
        [shape((tokens, vdim), bf16), shape((1, width), f32)],
        [VMEM_SPEC] * 9,
        (extra, partner, other, far, pair, inside, reach_f, reach_b, gated),
        8 * tokens * vdim * DK,
        8 * tokens * vdim,
        [
            pltpu.VMEM((vdim, DK), f32),
            pltpu.VMEM((vdim, DK), f32),
            pltpu.VMEM((8 * -(-heads // 8), DK), f32),
            pltpu.VMEM((8 * -(-heads // 8), DK), f32),
            pltpu.VMEM((sp_count, lift + 4 * heads * ctx, DK), bf16),
        ],
    )
    branches = gathered_pieces(heads_out, "tp", "out")
    late = LATE if tp_count == 8 else list(range(max(1, tp_count - 2), tp_count))
    middle = MIDDLE if tp_count == 8 else []
    soon = [k for k in range(tp_count) if k not in late and k not in middle]
    cost = 2 * width * vdim
    early = call(
        functools.partial(early_kernel, soon),
        shape((tokens, width), f32),
        [VMEM_SPEC] * (len(soon) + 1),
        (*(branches[k] for k in soon), output_matrix),
        tokens * cost * len(soon),
        cost * len(soon),
    )
    if middle:
        early = call(
            functools.partial(middle_kernel, middle),
            shape((tokens, width), f32),
            [VMEM_SPEC] * (len(middle) + 2),
            (*(branches[k] for k in middle), output_matrix, early),
            tokens * cost * len(middle),
            cost * len(middle),
        )
    return call(
        functools.partial(output_kernel, late),
        shape((tokens, width), bf16),
        [VMEM_SPEC] * (len(late) + 4),
        (*(branches[k] for k in late), output_matrix, early, latent, gates),
        tokens * cost * len(late),
        cost * len(late),
    )


def solution(mesh):
    placed = (
        P("sp", "tp"),
        P("sp", "tp"),
        P("sp"),
        P("sp"),
        P("tp", "sp"),
        P("tp", "sp"),
        P("tp", "sp"),
        P("tp", None),
        P("tp", None),
        P("tp", None),
        P("tp", None),
        P(),
        P(),
        P(),
        P(None, "sp", None),
        P("tp"),
        P("tp", None),
    )
    tp_count, sp_count = (mesh.shape["tp"], mesh.shape["sp"])
    powers = tp_count & tp_count - 1 == 0
    direct = 2 <= tp_count <= HEADS and sp_count == 4 and powers
    return jax.shard_map(
        local_direct if direct else local_general, mesh=mesh, in_specs=placed, out_specs=P("sp", "tp"), check_vma=False
    )
```
